128 devices in a mesh: sp: 16 (over z, x), tp: 8 (over y, core).
Axes of the slice: x: 4, y: 4, z: 4, core: 2. Of those that a mesh axis runs over, the one named last changes fastest.
Arguments:
- hidden_states: bfloat16 [12288, 4096], P('sp'), may hold values from -60 to 60
- w_conv_b: bfloat16 [4096, 2048], P(None, 'tp'), may hold values from -0.09375 to 0.09375
- w_conv_c: bfloat16 [4096, 2048], P(None, 'tp'), may hold values from -0.09375 to 0.09375
- w_conv_h: bfloat16 [4096, 2048], P(None, 'tp'), may hold values from -0.09375 to 0.09375
- conv_taps: bfloat16 [3, 2048], P(None, 'tp'), may hold values from -3.5 to 3.5
- w_query: bfloat16 [4096, 2048], P(None, 'tp'), may hold values from -0.15625 to 0.15625
- w_key: bfloat16 [4096, 2048], P(None, 'tp'), may hold values from -0.09375 to 0.09375
- w_value: bfloat16 [4096, 2048], P(None, 'tp'), may hold values from -0.09375 to 0.09375
- lambdas: float32 [16], P('tp'), may hold values from 0.3 to 0.8
- head_gain: bfloat16 [128], replicated, may hold values from 0.099609375 to 1.8984375
- w_out_conv: bfloat16 [2048, 4096], P('tp'), may hold values from -1 to 1
- w_out_attn: bfloat16 [2048, 4096], P('tp'), may hold values from -1 to 1
- out_gain: bfloat16 [4096], replicated, may hold values from 0.099609375 to 1.8984375
Outputs:
- mixed: bfloat16 [12288, 4096], P('sp', 'tp')
The draws below stay inside these ranges and needn't reach their ends.
All inputs are finite; a program needn't handle non-finite values.
Results may differ from the reference program's by a relative error of at most 0.023.
Values may be sent and summed in bfloat16 or wider, within the bound.
A program may use at most 192 MiB of HBM per device.

```python
import jax
import jax.numpy as jnp
from jax import lax

D = 4096
HEADS = 16
QK = 64
CONV = 2048
TAPS = 3
TOK_DEV = 768
VD = 128
TOKENS = 12288
N_TP = 8


def draw_hidden_states(key, part):
    values = jnp.clip(jax.random.normal(key, (TOKENS, D), jnp.float32), -6.0, 6.0)
    return jnp.clip(values, -60.0, 60.0).astype(jnp.bfloat16)


def rising_columns(key, row_count):
    columns = jnp.arange(D, dtype=jnp.float32) / D
    base = jnp.clip(jax.random.normal(key, (row_count, D), jnp.float32), -6.0, 6.0)
    ramp = 3.0 ** columns
    values = base * ramp[None, :] * (CONV + HEADS * VD) ** (-0.5)
    return jnp.clip(values, -1.0, 1.0).astype(jnp.bfloat16)


def draw_w_out_conv(key, part):
    return rising_columns(jax.random.fold_in(key, 11), CONV)


def draw_w_out_attn(key, part):
    return rising_columns(jax.random.fold_in(key, 13), HEADS * VD)


def block_scale(own_key, shape, cuts, smallest, high):
    gain = 1.0
    for position, shards_of in cuts:
        draws = jax.random.uniform(jax.random.fold_in(jax.random.fold_in(own_key, 6), position), (shards_of,), jnp.float32, smallest / len(cuts), high / len(cuts))
        gain = gain * jnp.repeat(jnp.exp(draws), shape[position] // shards_of).reshape((-1,) + (1,) * (len(shape) - 1 - position))
    return gain


def normal_values(key, shape, width, most, cuts=(), kind=jnp.bfloat16):
    values = width * jax.random.normal(key, shape, jnp.float32)
    if cuts:
        values = values * block_scale(key, shape, cuts, -0.22, 0.18)
    return jnp.clip(values, -most, most).astype(kind)


def setup_inputs(seed: int = 0) -> dict:
    splits = jax.random.split(jax.random.key(seed), 14)
    return {
        "hidden_states": draw_hidden_states(jax.random.fold_in(splits[13], 71), 0),
        "w_conv_b": normal_values(splits[1], (D, CONV), D ** -0.5, 0.09375, ((1, 8),)),
        "w_conv_c": normal_values(splits[2], (D, CONV), D ** -0.5, 0.09375, ((1, 8),)),
        "w_conv_h": normal_values(splits[3], (D, CONV), D ** -0.5, 0.09375, ((1, 8),)),
        "conv_taps": normal_values(splits[4], (TAPS, CONV), TAPS ** -0.5, 3.5, ((1, 8),)),
        "w_query": normal_values(splits[5], (D, HEADS * 2 * QK), (D // 3) ** -0.5, 0.15625, ((1, 8),)),
        "w_key": normal_values(splits[6], (D, HEADS * 2 * QK), D ** -0.5, 0.09375, ((1, 8),)),
        "w_value": normal_values(splits[7], (D, HEADS * VD), D ** -0.5, 0.09375, ((1, 8),)),
        "lambdas": jnp.clip(0.3 + 0.5 * jax.random.uniform(splits[8], (HEADS,), jnp.float32) ** block_scale(splits[8], (HEADS,), ((0, 8),), -0.2, 0.2), 0.3, 0.8),
        "head_gain": jnp.clip(1.0 + 0.18 * jax.random.normal(splits[9], (VD,), jnp.float32), 0.099609375, 1.8984375).astype(jnp.bfloat16),
        "w_out_conv": draw_w_out_conv(jax.random.fold_in(splits[13], 71), 0),
        "w_out_attn": draw_w_out_attn(jax.random.fold_in(splits[13], 71), 0),
        "out_gain": jnp.clip(1.0 + 0.18 * jax.random.normal(splits[12], (D,), jnp.float32), 0.099609375, 1.8984375).astype(jnp.bfloat16),
    }


def rotate(values, positions):
    inverse = 1.0 / 10000.0 ** (jnp.arange(0, QK, 2, dtype=jnp.float32) / QK)
    angles = positions[:, None] * inverse[None, :]
    angles = jnp.concatenate([angles, angles], axis=-1)
    cosine = jnp.cos(angles)[:, None, None, :]
    sine = jnp.sin(angles)[:, None, None, :]
    first_half, second_half = jnp.split(values, 2, axis=-1)
    return values * cosine + jnp.concatenate([-second_half, first_half], axis=-1) * sine

def reference(hidden_states, w_conv_b, w_conv_c, w_conv_h, conv_taps, w_query, w_key, w_value, lambdas, head_gain, w_out_conv, w_out_attn, out_gain):

    def project(weight):
        return jnp.dot(hidden_states, weight, preferred_element_type=jnp.float32).astype(jnp.bfloat16)
    u_b = project(w_conv_b)
    u_c = project(w_conv_c)
    u_h = project(w_conv_h)
    gated = u_c.astype(jnp.float32) * u_h.astype(jnp.float32)
    padded = jnp.concatenate([jnp.zeros((TAPS - 1, CONV), jnp.float32), gated], axis=0)
    taps_f = conv_taps.astype(jnp.float32)
    convolved = jnp.zeros((TOKENS, CONV), jnp.float32)
    for tap in range(TAPS):
        convolved = convolved + taps_f[tap][None, :] * padded[tap:tap + TOKENS]
    conv_out = (u_b.astype(jnp.float32) * convolved).astype(jnp.bfloat16)
    positions = jnp.arange(TOKENS, dtype=jnp.float32)
    query = rotate(project(w_query).reshape(TOKENS, HEADS, 2, QK).astype(jnp.float32), positions).astype(jnp.bfloat16)
    keys = rotate(project(w_key).reshape(TOKENS, HEADS, 2, QK).astype(jnp.float32), positions).astype(jnp.bfloat16)
    values = project(w_value).reshape(TOKENS, HEADS, VD)
    gain_f = head_gain.astype(jnp.float32)
    key_pos = jnp.arange(TOKENS, dtype=jnp.int32)

    def one_head(args):
        head_query, head_keys, head_values, weight_two = args
        keys_f = head_keys.astype(jnp.float32)
        values_f = head_values.astype(jnp.float32)

        def one_block(block_index):
            first = (block_index * TOK_DEV).astype(jnp.int32)
            block_query = lax.dynamic_slice_in_dim(head_query, first, TOK_DEV, 0).astype(jnp.float32)
            scores = jnp.einsum('qcd,kcd->cqk', block_query, keys_f) * QK ** (-0.5)
            query_pos = first + jnp.arange(TOK_DEV, dtype=jnp.int32)
            visible = key_pos[None, :] <= query_pos[:, None]
            scores = jnp.where(visible[None], scores, -jnp.inf)
            top = lax.optimization_barrier(jnp.max(scores, axis=-1, keepdims=True))
            weights = jnp.exp(scores - top)
            denom = lax.optimization_barrier(jnp.sum(weights, axis=-1))
            rounded = lax.optimization_barrier(weights.astype(jnp.bfloat16)).astype(jnp.float32)
            numer = jnp.einsum('cqk,ke->cqe', rounded, values_f)
            diff = numer[0] / denom[0][:, None] - weight_two * numer[1] / denom[1][:, None]
            normed = diff * lax.rsqrt(lax.optimization_barrier(jnp.mean(diff * diff, axis=-1, keepdims=True)) + 1e-05) * gain_f[None, :]
            return normed.astype(jnp.bfloat16)
        blocks = lax.map(one_block, jnp.arange(TOKENS // TOK_DEV, dtype=jnp.int32))
        return blocks.reshape(TOKENS, VD)
    per_head = lax.map(one_head, (query.transpose(1, 0, 2, 3), keys.transpose(1, 0, 2, 3), values.transpose(1, 0, 2), lambdas))
    attn_out = per_head.transpose(1, 0, 2).reshape(TOKENS, HEADS * VD)
    conv_width = CONV // N_TP
    attn_width = HEADS * VD // N_TP
    total = jnp.zeros((TOKENS, D), jnp.float32)
    for block in range(N_TP):
        term = jnp.dot(conv_out[:, block * conv_width:(block + 1) * conv_width], w_out_conv[block * conv_width:(block + 1) * conv_width], preferred_element_type=jnp.float32)
        term = term + jnp.dot(attn_out[:, block * attn_width:(block + 1) * attn_width], w_out_attn[block * attn_width:(block + 1) * attn_width], preferred_element_type=jnp.float32)
        total = total + lax.optimization_barrier(term.astype(jnp.bfloat16)).astype(jnp.float32)
    mix = total.astype(jnp.bfloat16).astype(jnp.float32)
    mean_value = lax.optimization_barrier(jnp.mean(mix, axis=-1, keepdims=True))
    variance = lax.optimization_barrier(jnp.mean(mix * mix, axis=-1, keepdims=True)) - mean_value * mean_value
    normed = (mix - mean_value) * lax.rsqrt(variance + 1e-05) * out_gain.astype(jnp.float32)[None, :]
    return normed.astype(jnp.bfloat16)
```

```python
import functools

import jax
import jax.numpy as jnp
from jax import lax
from jax.experimental import pallas as pl
from jax.experimental.pallas import tpu as pltpu
from jax.sharding import PartitionSpec as P

D = 4096
QK = 64
TAPS = 3
VD = 128
TB = 768
NB = 16
TQ = 256
NT = TB // TQ
VA = 144
LOG2E = 1.4426950408889634
NEG_LARGE = -1e30
BF16 = jnp.bfloat16
F32 = jnp.float32


def attention_kernel(
    k_in, v_in, q_in, lam_in, gain_ref, o_hbm,
    k_all, v_all, q_own, qa, lam_own, s0, s1, s2, acc, m_ref, o_stage,
    k_recv, v_recv, q_recv, l_recv, o_recv,
    q_send, l_send, p1k_send, p1v_send, rk_send, rv_send, lk_send, lv_send,
    dk_send, dv_send, o_send,
):
    sp = lax.axis_index("sp")
    tp = lax.axis_index("tp")
    z, x = sp // 4, sp % 4
    y, c = tp // 2, tp % 2
    own_pair = 2 * x + c

    def device(zz, xx, cc):
        return {"sp": zz * 4 + xx, "tp": y * 2 + cc}

    def send(src, dst, send_sem, recv_sem, zz, xx, cc):
        same = (zz == z) & (xx == x) & (cc == c)

        @pl.when(same)
        def _():
            pltpu.make_async_copy(src, dst, recv_sem).start()

        @pl.when(jnp.logical_not(same))
        def _():
            remote(src, dst, send_sem, recv_sem, zz, xx, cc).start()

    def remote(src, dst, send_sem, recv_sem, zz, xx, cc):
        return pltpu.make_async_remote_copy(
            src_ref=src, dst_ref=dst, send_sem=send_sem, recv_sem=recv_sem,
            device_id=device(zz, xx, cc), device_id_type=pl.DeviceIdType.MESH,
        )

    def wait_sent(src, dst, send_sem, recv_sem, zz, xx, cc):
        same = (zz == z) & (xx == x) & (cc == c)

        @pl.when(jnp.logical_not(same))
        def _():
            remote(src, dst, send_sem, recv_sem, zz, xx, cc).wait_send()

    barrier = pltpu.get_barrier_semaphore()
    me = sp * 2 + c

    def greet(i, carry):
        other = (me + i) % 32
        pl.semaphore_signal(
            barrier, inc=1, device_id={"sp": other // 2, "tp": y * 2 + other % 2},
            device_id_type=pl.DeviceIdType.MESH,
        )
        return carry

    lax.fori_loop(1, 32, greet, 0)
    pl.semaphore_wait(barrier, 31)

    pair_of_sp = jnp.where(sp < 8, sp, 15 - sp)
    slot_of_sp = jnp.where(sp < 8, 0, 1)
    first = []
    for e in range(2):
        head = 2 * c + e
        first.append((k_in.at[:, e * 128 : (e + 1) * 128], k_all.at[sp], p1k_send.at[e], k_recv.at[sp], head, x, z % 2))
        first.append((q_in.at[e * 128 : (e + 1) * 128], q_own.at[slot_of_sp], q_send.at[e], q_recv.at[slot_of_sp], head, pair_of_sp // 2, pair_of_sp % 2))
        first.append((v_in.at[e * 128 : (e + 1) * 128], v_all.at[sp, pl.ds(0, 128)], p1v_send.at[e], v_recv.at[sp], head, x, z % 2))
        first.append((lam_in.at[e], lam_own.at[slot_of_sp], l_send.at[e], l_recv.at[slot_of_sp], head, pair_of_sp // 2, pair_of_sp % 2))
    for one in first:
        send(*one)

    def ones(j, carry):
        v_all[j, 128:VA, :] = jnp.ones((VA - 128, TB), BF16)
        return carry

    lax.fori_loop(0, NB, ones, 0)
    acc[...] = jnp.zeros(acc.shape, F32)
    m_ref[...] = jnp.full(m_ref.shape, NEG_LARGE, F32)
    zero = jnp.zeros((QK, TQ), BF16)
    for qb in range(2):
        remote(q_in.at[0:128], q_own.at[qb], q_send.at[0], q_recv.at[qb], z, x, c).wait_recv()
        remote(lam_in.at[0], lam_own.at[qb], l_send.at[0], l_recv.at[qb], z, x, c).wait_recv()
        for t in range(NT):
            qt = q_own[qb, :, t * TQ : (t + 1) * TQ]
            qa[qb * NT + t, 0:QK, 0:TQ] = qt[0:QK]
            qa[qb * NT + t, QK:128, 0:TQ] = zero
            qa[qb * NT + t, 0:QK, TQ : 2 * TQ] = zero
            qa[qb * NT + t, QK:128, TQ : 2 * TQ] = qt[QK:128]

    scores = (s0, s1, s2)

    def unit(qb, j, diagonal):
        tops = [None] * NT

        def produce(t):
            rows = TQ * (t + 1) if diagonal else TB
            s = jnp.dot(k_all[j, 0:rows, :], qa[qb * NT + t], preferred_element_type=F32)
            if diagonal:
                key = lax.broadcasted_iota(jnp.int32, (rows, 2 * TQ), 0)
                query = lax.broadcasted_iota(jnp.int32, (rows, 2 * TQ), 1)
                query = jnp.where(query >= TQ, query - TQ, query) + t * TQ
                s = jnp.where(key <= query, s, NEG_LARGE)
            scores[t][0:rows, :] = s
            tops[t] = jnp.max(s, axis=0, keepdims=True)

        def consume(t):
            rows = TQ * (t + 1) if diagonal else TB
            at = qb * NT + t
            before = m_ref[at]
            after = jnp.maximum(before, tops[t])
            w = jnp.exp2(scores[t][0:rows, :] - after).astype(BF16)
            factor = jnp.exp2(before - after)
            acc[at] = acc[at] * factor + jnp.dot(
                v_all[j, :, 0:rows], w, preferred_element_type=F32
            )
            m_ref[at] = after

        produce(0)
        produce(1)
        consume(0)
        produce(2)
        consume(1)
        consume(2)

    def block_of(i):
        w, u = i // 4, i % 4
        side = jnp.where(u < 2, x + 3, x + 1) % 4
        col = jnp.where(w == 0, x, jnp.where(w == 3, (x + 2) % 4, side))
        row = jnp.where(w == 2, (u + 2) % 4, u)
        return w, u, row * 4 + col

    left, right = (x + 3) % 4, (x + 1) % 4

    def k_copy(blk, sems, n, zz, xx, cc):
        return remote(k_all.at[blk], k_all.at[blk], sems.at[n], k_recv.at[blk], zz, xx, cc)

    def v_copy(blk, sems, n, zz, xx, cc):
        part = v_all.at[blk, pl.ds(0, 128)]
        return remote(part, part, sems.at[n], v_recv.at[blk], zz, xx, cc)

    def step(i, carry):
        w, u, blk = block_of(i)
        k_copy(blk, dk_send, 0, z, x, 1 - c).wait_recv()
        v_copy(blk, dv_send, 0, z, x, 1 - c).wait_recv()

        @pl.when(u % 2 == c)
        def _():
            @pl.when((w == 0) & (u < 2))
            def _():
                k_copy(blk, rk_send, 0, z, right, c).start()
                v_copy(blk, rv_send, 0, z, right, c).start()

            @pl.when((w == 0) & (u >= 2))
            def _():
                k_copy(blk, lk_send, 0, z, left, c).start()
                v_copy(blk, lv_send, 0, z, left, c).start()
                k_copy(blk, rk_send, 1, z, right, c).start()
                v_copy(blk, rv_send, 1, z, right, c).start()
                k_copy(blk - 8, lk_send, 1, z, left, c).start()
                v_copy(blk - 8, lv_send, 1, z, left, c).start()

            @pl.when((w == 1) & (u < 2))
            def _():
                k_copy(blk, rk_send, 2, z, right, c).start()
                v_copy(blk, rv_send, 2, z, right, c).start()

            @pl.when((w == 1) & (u >= 2))
            def _():
                k_copy(blk, lk_send, 2, z, left, c).start()
                v_copy(blk, lv_send, 2, z, left, c).start()

            k_copy(blk, dk_send, i // 2, z, x, 1 - c).start()
            v_copy(blk, dv_send, i // 2, z, x, 1 - c).start()

        def for_queries(qb, carry):
            q_blk = jnp.where(qb == 0, own_pair, 15 - own_pair)

            @pl.when(blk < q_blk)
            def _():
                unit(qb, blk, False)

            @pl.when(blk == q_blk)
            def _():
                unit(qb, blk, True)

            return carry

        lax.fori_loop(0, 2, for_queries, 0)
        return carry

    lax.fori_loop(0, NB, step, 0)

    out = []
    for qb in range(2):
        lam = lam_own[qb, 0:1, 0:1]
        for t in range(NT):
            at = qb * NT + t
            n1 = acc[at, 0:128, 0:TQ] / acc[at, 128:129, 0:TQ]
            n2 = acc[at, 0:128, TQ : 2 * TQ] / acc[at, 128:129, TQ : 2 * TQ]
            diff = n1 - lam * n2
            mean = jnp.mean(diff * diff, axis=0, keepdims=True)
            o_stage[qb, :, t * TQ : (t + 1) * TQ] = (
                diff * lax.rsqrt(mean + 1e-05) * gain_ref[...]
            ).astype(BF16)
        q_blk = own_pair if qb == 0 else 15 - own_pair
        e = z % 2
        one = (o_stage.at[qb], o_hbm.at[e], o_send.at[qb], o_recv.at[e], q_blk // 4, q_blk % 4, z // 2)
        send(*one)
        out.append(one)

    for one in first + out:
        wait_sent(*one)
    for n in range(3):
        k_copy(0, rk_send, n, z, right, c).wait_send()
        v_copy(0, rv_send, n, z, right, c).wait_send()
        k_copy(0, lk_send, n, z, left, c).wait_send()
        v_copy(0, lv_send, n, z, left, c).wait_send()
    for n in range(8):
        k_copy(0, dk_send, n, z, x, 1 - c).wait_send()
        v_copy(0, dv_send, n, z, x, 1 - c).wait_send()
    for e in range(2):
        remote(o_stage.at[e], o_hbm.at[e], o_send.at[e], o_recv.at[e], z, x, c).wait_recv()


def attention(keys, values_t, query_t, lam, gain):
    dma = pltpu.SemaphoreType.DMA
    hbm = pl.BlockSpec(memory_space=pl.ANY)
    return pl.pallas_call(
        attention_kernel,
        out_shape=jax.ShapeDtypeStruct((2, 128, TB), BF16),
        in_specs=[hbm, hbm, hbm, hbm, pl.BlockSpec(memory_space=pltpu.VMEM)],
        out_specs=hbm,
        scratch_shapes=[
            pltpu.VMEM((NB, TB, 128), BF16),
            pltpu.VMEM((NB, VA, TB), BF16),
            pltpu.VMEM((2, 128, TB), BF16),
            pltpu.VMEM((2 * NT, 128, 2 * TQ), BF16),
            pltpu.VMEM((2, 8, 128), F32),
            pltpu.VMEM((TB, 2 * TQ), F32),
            pltpu.VMEM((TB, 2 * TQ), F32),
            pltpu.VMEM((TB, 2 * TQ), F32),
            pltpu.VMEM((2 * NT, VA, 2 * TQ), F32),
            pltpu.VMEM((2 * NT, 1, 2 * TQ), F32),
            pltpu.VMEM((2, 128, TB), BF16),
            dma((NB,)), dma((NB,)), dma((2,)), dma((2,)), dma((2,)),
            dma((2,)), dma((2,)), dma((2,)), dma((2,)),
            dma((3,)), dma((3,)), dma((3,)), dma((3,)),
            dma((8,)), dma((8,)), dma((2,)),
        ],
        compiler_params=pltpu.CompilerParams(
            collective_id=0, has_side_effects=True, vmem_limit_bytes=48 << 20
        ),
        name="attention",
    )(keys, values_t, query_t, lam, gain)


def passed_along(block, axis, distance):
    devices = range(lax.axis_size(axis))
    route = [(i - distance, i) for i in devices if i - distance in devices]
    return lax.ppermute(block, axis, route)


def copy_for_each(value, axis):
    copies = jnp.broadcast_to(value, (lax.axis_size(axis), *value.shape))
    return lax.all_to_all(copies, axis, split_axis=0, concat_axis=0, tiled=True)


def per_device(
    hidden_states,
    w_conv_b,
    w_conv_c,
    w_conv_h,
    conv_taps,
    w_query,
    w_key,
    w_value,
    lambdas,
    head_gain,
    w_out_conv,
    w_out_attn,
    out_gain,
):
    tok_rows = hidden_states.shape[0]
    channels = w_conv_b.shape[1]
    offset = lax.axis_index("sp") * tok_rows
    positions = (offset + jnp.arange(tok_rows, dtype=jnp.int32)).astype(F32)
    inverse = 1.0 / 10000.0 ** (jnp.arange(0, QK, 2, dtype=F32) / QK)

    def project(weight):
        return jnp.dot(hidden_states, weight, preferred_element_type=F32).astype(BF16)

    def project_t(weight):
        return lax.dot_general(
            weight, hidden_states, (((0,), (1,)), ((), ())), preferred_element_type=F32
        ).astype(BF16)

    angles = positions[:, None] * inverse[None, :]
    cos, sin = jnp.cos(angles), jnp.sin(angles)

    k = project(w_key).astype(F32).reshape(tok_rows, 4, 2, QK // 2)
    k1, k2 = k[:, :, 0], k[:, :, 1]
    ck, sk = cos[:, None, :], sin[:, None, :]
    keys = jnp.stack([k1 * ck - k2 * sk, k2 * ck + k1 * sk], axis=2).reshape(tok_rows, 256).astype(BF16)

    scale = LOG2E * QK ** (-0.5)
    cq, sq = (cos.T * scale)[None], (sin.T * scale)[None]
    q = project_t(w_query).astype(F32).reshape(4, 2, QK // 2, tok_rows)
    q1, q2 = q[:, 0], q[:, 1]
    query_t = jnp.stack([q1 * cq - q2 * sq, q2 * cq + q1 * sq], axis=1).reshape(256, tok_rows).astype(BF16)
    values_t = project_t(w_value)

    lam = jnp.broadcast_to(lambdas[:, None, None], (2, 8, 128))
    gain = head_gain.astype(F32)[:, None]
    attn_t = attention(keys, values_t, query_t, lam, gain).reshape(256, tok_rows)

    u_b = project(w_conv_b)
    u_c = project(w_conv_c)
    u_h = project(w_conv_h)
    gated = u_c.astype(F32) * u_h.astype(F32)
    rim_rows = passed_along(gated[tok_rows - (TAPS - 1) :], "sp", 1)
    padded = jnp.concatenate([rim_rows, gated], axis=0)
    taps_f = conv_taps.astype(F32)
    convolved = jnp.zeros((tok_rows, channels), F32)
    for tap in range(TAPS):
        convolved = convolved + taps_f[tap][None, :] * padded[tap : tap + tok_rows]
    conv_out = (u_b.astype(F32) * convolved).astype(BF16)

    gain_f = out_gain.astype(F32)
    partial_value = jnp.dot(conv_out, w_out_conv, preferred_element_type=F32) + lax.dot_general(
        attn_t, w_out_attn, (((0,), (0,)), ((), ())), preferred_element_type=F32
    )
    summed = lax.psum_scatter(partial_value.astype(BF16), "tp", scatter_dimension=1, tiled=True)
    mix_f = summed.astype(F32)
    width = mix_f.shape[1]
    stats = jnp.concatenate([jnp.sum(mix_f, axis=-1), jnp.sum(mix_f * mix_f, axis=-1)])
    total = jnp.sum(copy_for_each(stats, "tp").reshape(lax.axis_size("tp"), -1), axis=0)
    mean_value = (total[:tok_rows] / D)[:, None]
    variance = (total[tok_rows:] / D)[:, None] - mean_value * mean_value
    own_gain = lax.dynamic_slice_in_dim(gain_f, lax.axis_index("tp") * width, width, 0)
    return ((mix_f - mean_value) * lax.rsqrt(variance + 1e-05) * own_gain[None, :]).astype(BF16)


def solution(mesh):
    return jax.shard_map(
        per_device,
        mesh=mesh,
        in_specs=(
            P("sp", None),
            P(None, "tp"),
            P(None, "tp"),
            P(None, "tp"),
            P(None, "tp"),
            P(None, "tp"),
            P(None, "tp"),
            P(None, "tp"),
            P("tp"),
            P(),
            P("tp", None),
            P("tp", None),
            P(),
        ),
        out_specs=P("sp", "tp"),
        check_vma=False,
    )
```

```python
import functools

import jax
import jax.numpy as jnp
from jax import lax
from jax.experimental import pallas as pl
from jax.experimental.pallas import tpu as pltpu
from jax.sharding import PartitionSpec as P

D = 4096
QK = 64
TAPS = 3
VD = 128
TB = 768
NB = 16
TQ = 256
NT = TB // TQ
VA = 144
LOG2E = 1.4426950408889634
NEG_LARGE = -1e30
BF16 = jnp.bfloat16
F32 = jnp.float32


def attention_kernel(
    k_in, v_in, q_in, lam_in, gain_ref, o_hbm,
    k_all, v_all, q_own, qa, lam_own, s0, s1, s2, acc, m_ref, o_stage,
    k_recv, v_recv, q_recv, l_recv, o_recv,
    q_send, l_send, p1k_send, p1v_send, rk_send, rv_send, lk_send, lv_send,
    dk_send, dv_send, o_send,
):
    sp = lax.axis_index("sp")
    tp = lax.axis_index("tp")
    z, x = sp // 4, sp % 4
    y, c = tp // 2, tp % 2
    own_pair = x + 4 * c

    def device(zz, xx, cc):
        return {"sp": zz * 4 + xx, "tp": y * 2 + cc}

    def send(src, dst, send_sem, recv_sem, zz, xx, cc):
        same = (zz == z) & (xx == x) & (cc == c)

        @pl.when(same)
        def _():
            pltpu.make_async_copy(src, dst, recv_sem).start()

        @pl.when(jnp.logical_not(same))
        def _():
            remote(src, dst, send_sem, recv_sem, zz, xx, cc).start()

    def remote(src, dst, send_sem, recv_sem, zz, xx, cc):
        return pltpu.make_async_remote_copy(
            src_ref=src, dst_ref=dst, send_sem=send_sem, recv_sem=recv_sem,
            device_id=device(zz, xx, cc), device_id_type=pl.DeviceIdType.MESH,
        )

    def wait_sent(src, dst, send_sem, recv_sem, zz, xx, cc):
        same = (zz == z) & (xx == x) & (cc == c)

        @pl.when(jnp.logical_not(same))
        def _():
            remote(src, dst, send_sem, recv_sem, zz, xx, cc).wait_send()

    barrier = pltpu.get_barrier_semaphore()
    me = sp * 2 + c

    def greet(i, carry):
        other = (me + i) % 32
        pl.semaphore_signal(
            barrier, inc=1, device_id={"sp": other // 2, "tp": y * 2 + other % 2},
            device_id_type=pl.DeviceIdType.MESH,
        )
        return carry

    lax.fori_loop(1, 32, greet, 0)
    pl.semaphore_wait(barrier, 31)

    pair_of_sp = jnp.where(sp < 8, sp, 15 - sp)
    slot_of_sp = jnp.where(sp < 8, 0, 1)
    first = []
    for e in range(2):
        head = 2 * c + e
        first.append((k_in.at[:, e * 128 : (e + 1) * 128], k_all.at[sp], p1k_send.at[e], k_recv.at[sp], head, x, z % 2))
        first.append((q_in.at[e * 128 : (e + 1) * 128], q_own.at[slot_of_sp], q_send.at[e], q_recv.at[slot_of_sp], head, pair_of_sp % 4, pair_of_sp // 4))
        first.append((v_in.at[e * 128 : (e + 1) * 128], v_all.at[sp, pl.ds(0, 128)], p1v_send.at[e], v_recv.at[sp], head, x, z % 2))
        first.append((lam_in.at[e], lam_own.at[slot_of_sp], l_send.at[e], l_recv.at[slot_of_sp], head, pair_of_sp % 4, pair_of_sp // 4))
    for one in first:
        send(*one)

    def ones(j, carry):
        v_all[j, 128:VA, :] = jnp.ones((VA - 128, TB), BF16)
        return carry

    lax.fori_loop(0, NB, ones, 0)
    acc[...] = jnp.zeros(acc.shape, F32)
    m_ref[...] = jnp.full(m_ref.shape, NEG_LARGE, F32)
    zero = jnp.zeros((QK, TQ), BF16)
    for qb in range(2):
        remote(q_in.at[0:128], q_own.at[qb], q_send.at[0], q_recv.at[qb], z, x, c).wait_recv()
        remote(lam_in.at[0], lam_own.at[qb], l_send.at[0], l_recv.at[qb], z, x, c).wait_recv()
        for t in range(NT):
            qt = q_own[qb, :, t * TQ : (t + 1) * TQ]
            qa[qb * NT + t, 0:QK, 0:TQ] = qt[0:QK]
            qa[qb * NT + t, QK:128, 0:TQ] = zero
            qa[qb * NT + t, 0:QK, TQ : 2 * TQ] = zero
            qa[qb * NT + t, QK:128, TQ : 2 * TQ] = qt[QK:128]

    scores = (s0, s1, s2)

    def unit(qb, j, diagonal):
        tops = [None] * NT

        def produce(t):
            rows = TQ * (t + 1) if diagonal else TB
            s = jnp.dot(k_all[j, 0:rows, :], qa[qb * NT + t], preferred_element_type=F32)
            if diagonal:
                key = lax.broadcasted_iota(jnp.int32, (rows, 2 * TQ), 0)
                query = lax.broadcasted_iota(jnp.int32, (rows, 2 * TQ), 1)
                query = jnp.where(query >= TQ, query - TQ, query) + t * TQ
                s = jnp.where(key <= query, s, NEG_LARGE)
            scores[t][0:rows, :] = s
            tops[t] = jnp.max(s, axis=0, keepdims=True)

        def consume(t):
            rows = TQ * (t + 1) if diagonal else TB
            at = qb * NT + t
            before = m_ref[at]
            after = jnp.maximum(before, tops[t])
            w = jnp.exp2(scores[t][0:rows, :] - after).astype(BF16)
            factor = jnp.exp2(before - after)
            acc[at] = acc[at] * factor + jnp.dot(
                v_all[j, :, 0:rows], w, preferred_element_type=F32
            )
            m_ref[at] = after

        produce(0)
        produce(1)
        consume(0)
        produce(2)
        consume(1)
        consume(2)

    def block_of(i):
        w, u = i // 4, i % 4
        side = jnp.where(u < 2, x + 3, x + 1) % 4
        col = jnp.where(w == 0, x, jnp.where(w == 3, (x + 2) % 4, side))
        row = jnp.where(w == 2, (u + 2) % 4, u)
        return w, u, row * 4 + col

    left, right = (x + 3) % 4, (x + 1) % 4

    def k_copy(blk, sems, n, zz, xx, cc):
        return remote(k_all.at[blk], k_all.at[blk], sems.at[n], k_recv.at[blk], zz, xx, cc)

    def v_copy(blk, sems, n, zz, xx, cc):
        part = v_all.at[blk, pl.ds(0, 128)]
        return remote(part, part, sems.at[n], v_recv.at[blk], zz, xx, cc)

    def step(i, carry):
        w, u, blk = block_of(i)
        k_copy(blk, dk_send, 0, z, x, 1 - c).wait_recv()
        v_copy(blk, dv_send, 0, z, x, 1 - c).wait_recv()

        @pl.when(u % 2 == c)
        def _():
            @pl.when((w == 0) & (u < 2))
            def _():
                k_copy(blk, rk_send, 0, z, right, c).start()
                v_copy(blk, rv_send, 0, z, right, c).start()

            @pl.when((w == 0) & (u >= 2))
            def _():
                k_copy(blk, lk_send, 0, z, left, c).start()
                v_copy(blk, lv_send, 0, z, left, c).start()
                k_copy(blk, rk_send, 1, z, right, c).start()
                v_copy(blk, rv_send, 1, z, right, c).start()
                k_copy(blk - 8, lk_send, 1, z, left, c).start()
                v_copy(blk - 8, lv_send, 1, z, left, c).start()

            @pl.when((w == 1) & (u < 2))
            def _():
                k_copy(blk, rk_send, 2, z, right, c).start()
                v_copy(blk, rv_send, 2, z, right, c).start()

            @pl.when((w == 1) & (u >= 2))
            def _():
                k_copy(blk, lk_send, 2, z, left, c).start()
                v_copy(blk, lv_send, 2, z, left, c).start()

            k_copy(blk, dk_send, i // 2, z, x, 1 - c).start()
            v_copy(blk, dv_send, i // 2, z, x, 1 - c).start()

        def for_queries(qb, carry):
            q_blk = jnp.where(qb == 0, own_pair, 15 - own_pair)

            @pl.when(blk < q_blk)
            def _():
                unit(qb, blk, False)

            @pl.when(blk == q_blk)
            def _():
                unit(qb, blk, True)

            return carry

        lax.fori_loop(0, 2, for_queries, 0)
        return carry

    lax.fori_loop(0, NB, step, 0)

    out = []
    for qb in range(2):
        lam = lam_own[qb, 0:1, 0:1]
        for t in range(NT):
            at = qb * NT + t
            n1 = acc[at, 0:128, 0:TQ] / acc[at, 128:129, 0:TQ]
            n2 = acc[at, 0:128, TQ : 2 * TQ] / acc[at, 128:129, TQ : 2 * TQ]
            diff = n1 - lam * n2
            mean = jnp.mean(diff * diff, axis=0, keepdims=True)
            normed = diff * lax.rsqrt(mean + 1e-05) * gain_ref[...]
            o_stage[qb, t * TQ : (t + 1) * TQ, :] = normed.T.astype(BF16)
        q_blk = own_pair if qb == 0 else 15 - own_pair
        e = z % 2
        one = (o_stage.at[qb], o_hbm.at[e], o_send.at[qb], o_recv.at[e], q_blk // 4, q_blk % 4, z // 2)
        send(*one)
        out.append(one)

    for one in first + out:
        wait_sent(*one)
    for n in range(3):
        k_copy(0, rk_send, n, z, right, c).wait_send()
        v_copy(0, rv_send, n, z, right, c).wait_send()
        k_copy(0, lk_send, n, z, left, c).wait_send()
        v_copy(0, lv_send, n, z, left, c).wait_send()
    for n in range(8):
        k_copy(0, dk_send, n, z, x, 1 - c).wait_send()
        v_copy(0, dv_send, n, z, x, 1 - c).wait_send()
    for e in range(2):
        remote(o_stage.at[e], o_hbm.at[e], o_send.at[e], o_recv.at[e], z, x, c).wait_recv()


def attention(keys, values_t, query_t, lam, gain):
    dma = pltpu.SemaphoreType.DMA
    hbm = pl.BlockSpec(memory_space=pl.ANY)
    return pl.pallas_call(
        attention_kernel,
        out_shape=jax.ShapeDtypeStruct((2, TB, 128), BF16),
        in_specs=[hbm, hbm, hbm, hbm, pl.BlockSpec(memory_space=pltpu.VMEM)],
        out_specs=hbm,
        scratch_shapes=[
            pltpu.VMEM((NB, TB, 128), BF16),
            pltpu.VMEM((NB, VA, TB), BF16),
            pltpu.VMEM((2, 128, TB), BF16),
            pltpu.VMEM((2 * NT, 128, 2 * TQ), BF16),
            pltpu.VMEM((2, 8, 128), F32),
            pltpu.VMEM((TB, 2 * TQ), F32),
            pltpu.VMEM((TB, 2 * TQ), F32),
            pltpu.VMEM((TB, 2 * TQ), F32),
            pltpu.VMEM((2 * NT, VA, 2 * TQ), F32),
            pltpu.VMEM((2 * NT, 1, 2 * TQ), F32),
            pltpu.VMEM((2, TB, 128), BF16),
            dma((NB,)), dma((NB,)), dma((2,)), dma((2,)), dma((2,)),
            dma((2,)), dma((2,)), dma((2,)), dma((2,)),
            dma((3,)), dma((3,)), dma((3,)), dma((3,)),
            dma((8,)), dma((8,)), dma((2,)),
        ],
        compiler_params=pltpu.CompilerParams(
            collective_id=0, has_side_effects=True, vmem_limit_bytes=48 << 20
        ),
        name="attention",
    )(keys, values_t, query_t, lam, gain)


SUB = 2
HALF = TB // 2
PR = HALF // SUB


def output_kernel(
    conv_in, attn_in, wc_in, wa_in, gain_ref, out_ref,
    act, wts, sbuf, rbuf, mix, stats,
    a_sem, a_recv, a_send, w_sem, w_recv, w_send, r_send, r_recv, t_send, t_recv,
):
    sp = lax.axis_index("sp")
    tp = lax.axis_index("tp")
    y, c = tp // 2, tp % 2

    def remote(src, dst, send_sem, recv_sem, other):
        return pltpu.make_async_remote_copy(
            src_ref=src, dst_ref=dst, send_sem=send_sem, recv_sem=recv_sem,
            device_id={"sp": sp, "tp": other}, device_id_type=pl.DeviceIdType.MESH,
        )

    barrier = pltpu.get_barrier_semaphore()

    def greet(i, carry):
        pl.semaphore_signal(
            barrier, inc=1, device_id={"sp": sp, "tp": (tp + i) % 8},
            device_id_type=pl.DeviceIdType.MESH,
        )
        return carry

    lax.fori_loop(1, 8, greet, 0)

    partner = y * 2 + (1 - c)
    local, pairs = [], []
    sources = [conv_in, attn_in.at[0], attn_in.at[1]]
    places = [pl.ds(c * 256, 256), pl.ds(512 + c * 256, 128), pl.ds(640 + c * 256, 128)]
    for n in range(3):
        dst = act.at[:, places[n]]
        local.append(pltpu.make_async_copy(sources[n], dst, a_sem.at[n]))
        pairs.append(remote(sources[n], dst, a_send.at[n], a_recv.at[n], partner))
    for chunk in range(4):
        for n, w_in in enumerate((wc_in, wa_in)):
            dst = wts.at[chunk, pl.ds(n * 512 + c * 256, 256)]
            k = chunk * 2 + n
            own = w_in.at[:, pl.ds(chunk * 1024 + c * 512, 512)]
            theirs = w_in.at[:, pl.ds(chunk * 1024 + (1 - c) * 512, 512)]
            local.append(pltpu.make_async_copy(own, dst, w_sem.at[k]))
            pairs.append(remote(theirs, dst, w_send.at[k], w_recv.at[k], partner))
    for one in local:
        one.start()
    pl.semaphore_wait(barrier, 7)
    for one in pairs:
        one.start()
    for one in local:
        one.wait()
    for one in pairs:
        one.wait_recv()

    up, down = ((y + 1) % 4) * 2 + c, ((y + 3) % 4) * 2 + c

    def ring(s, d, u):
        return remote(
            sbuf.at[s, d, u], rbuf.at[s, d, u], r_send.at[s, d, u], r_recv.at[s, d, u],
            up if d == 0 else down,
        )

    for s in range(4):
        for u in range(SUB):
            for d in range(2):
                chunk = (y + 3 - s) % 4 if d == 0 else (y + 1 + s) % 4
                first = d * HALF + u * PR
                part = jnp.dot(
                    act[first : first + PR, :], wts[chunk], preferred_element_type=F32
                )
                if s > 0:
                    ring(s - 1, d, u).wait_recv()
                    part = part + rbuf[s - 1, d, u].astype(F32)
                if s < 3:
                    sbuf[s, d, u] = part.astype(BF16)
                    ring(s, d, u).start()
                else:
                    mix[first : first + PR, :] = part.astype(BF16)

    ones = jnp.ones((8, 512), BF16)
    dims = (((1,), (1,)), ((), ()))
    m = mix[...]
    square = m.astype(F32) * m.astype(F32)
    high = square.astype(BF16)
    low = (square - high.astype(F32)).astype(BF16)
    total = lax.dot_general(ones, m, dims, preferred_element_type=F32)
    squares = lax.dot_general(ones, high, dims, preferred_element_type=F32)
    squares = squares + lax.dot_general(ones, low, dims, preferred_element_type=F32)
    row = lax.broadcasted_iota(jnp.int32, (8, TB), 0)
    stats[tp] = jnp.where(row == 0, total, squares)

    def tell(i):
        return remote(stats.at[tp], stats.at[tp], t_send.at[i - 1], t_recv.at[i - 1], (tp + i) % 8)

    for i in range(1, 8):
        tell(i).start()
    for i in range(1, 8):
        tell(i).wait_recv()
    everything = stats[0]
    for n in range(1, 8):
        everything = everything + stats[n]
    columns = everything.T
    mean = columns[:, 0:1] * (1.0 / D)
    variance = columns[:, 1:2] * (1.0 / D) - mean * mean
    out_ref[...] = (
        (mix[...].astype(F32) - mean) * lax.rsqrt(variance + 1e-05) * gain_ref[tp]
    ).astype(BF16)

    for one in pairs:
        one.wait_send()
    for s in range(3):
        for d in range(2):
            for u in range(SUB):
                ring(s, d, u).wait_send()
    for i in range(1, 8):
        tell(i).wait_send()


def output(conv_out, attn_out, w_conv, w_attn, gain):
    dma = pltpu.SemaphoreType.DMA
    hbm = pl.BlockSpec(memory_space=pl.ANY)
    vmem = pl.BlockSpec(memory_space=pltpu.VMEM)
    return pl.pallas_call(
        output_kernel,
        out_shape=jax.ShapeDtypeStruct((TB, 512), BF16),
        in_specs=[hbm, hbm, hbm, hbm, vmem],
        out_specs=vmem,
        scratch_shapes=[
            pltpu.VMEM((TB, 1024), BF16),
            pltpu.VMEM((4, 1024, 512), BF16),
            pltpu.VMEM((3, 2, SUB, PR, 512), BF16),
            pltpu.VMEM((3, 2, SUB, PR, 512), BF16),
            pltpu.VMEM((TB, 512), BF16),
            pltpu.VMEM((8, 8, TB), F32),
            dma((3,)), dma((3,)), dma((3,)), dma((8,)), dma((8,)), dma((8,)),
            dma((3, 2, SUB)), dma((3, 2, SUB)), dma((7,)), dma((7,)),
        ],
        compiler_params=pltpu.CompilerParams(
            collective_id=1, has_side_effects=True, vmem_limit_bytes=48 << 20
        ),
        name="output",
    )(conv_out, attn_out, w_conv, w_attn, gain)


def passed_along(block, axis, distance):
    devices = range(lax.axis_size(axis))
    route = [(i - distance, i) for i in devices if i - distance in devices]
    return lax.ppermute(block, axis, route)


def per_device(
    hidden_states,
    w_conv_b,
    w_conv_c,
    w_conv_h,
    conv_taps,
    w_query,
    w_key,
    w_value,
    lambdas,
    head_gain,
    w_out_conv,
    w_out_attn,
    out_gain,
):
    tok_rows = hidden_states.shape[0]
    channels = w_conv_b.shape[1]
    offset = lax.axis_index("sp") * tok_rows
    positions = (offset + jnp.arange(tok_rows, dtype=jnp.int32)).astype(F32)
    inverse = 1.0 / 10000.0 ** (jnp.arange(0, QK, 2, dtype=F32) / QK)

    def project(weight):
        return jnp.dot(hidden_states, weight, preferred_element_type=F32).astype(BF16)

    def project_t(weight):
        return lax.dot_general(
            weight, hidden_states, (((0,), (1,)), ((), ())), preferred_element_type=F32
        ).astype(BF16)

    angles = positions[:, None] * inverse[None, :]
    cos, sin = jnp.cos(angles), jnp.sin(angles)

    k = project(w_key).astype(F32).reshape(tok_rows, 4, 2, QK // 2)
    k1, k2 = k[:, :, 0], k[:, :, 1]
    ck, sk = cos[:, None, :], sin[:, None, :]
    keys = jnp.stack([k1 * ck - k2 * sk, k2 * ck + k1 * sk], axis=2).reshape(tok_rows, 256).astype(BF16)

    scale = LOG2E * QK ** (-0.5)
    cq, sq = (cos.T * scale)[None], (sin.T * scale)[None]
    q = project_t(w_query).astype(F32).reshape(4, 2, QK // 2, tok_rows)
    q1, q2 = q[:, 0], q[:, 1]
    query_t = jnp.stack([q1 * cq - q2 * sq, q2 * cq + q1 * sq], axis=1).reshape(256, tok_rows).astype(BF16)
    values_t = project_t(w_value)

    lam = jnp.broadcast_to(lambdas[:, None, None], (2, 8, 128))
    gain = head_gain.astype(F32)[:, None]
    attn_out = attention(keys, values_t, query_t, lam, gain)

    u_b = project(w_conv_b)
    u_c = project(w_conv_c)
    u_h = project(w_conv_h)
    gated = u_c.astype(F32) * u_h.astype(F32)
    rim_rows = passed_along(gated[tok_rows - (TAPS - 1) :], "sp", 1)
    padded = jnp.concatenate([rim_rows, gated], axis=0)
    taps_f = conv_taps.astype(F32)
    convolved = jnp.zeros((tok_rows, channels), F32)
    for tap in range(TAPS):
        convolved = convolved + taps_f[tap][None, :] * padded[tap : tap + tok_rows]
    conv_out = (u_b.astype(F32) * convolved).astype(BF16)

    return output(conv_out, attn_out, w_out_conv, w_out_attn, out_gain.astype(F32).reshape(8, 1, 512))


def solution(mesh):
    return jax.shard_map(
        per_device,
        mesh=mesh,
        in_specs=(
            P("sp", None),
            P(None, "tp"),
            P(None, "tp"),
            P(None, "tp"),
            P(None, "tp"),
            P(None, "tp"),
            P(None, "tp"),
            P(None, "tp"),
            P("tp"),
            P(),
            P("tp", None),
            P("tp", None),
            P(),
        ),
        out_specs=P("sp", "tp"),
        check_vma=False,
    )
```

```python
import jax
import jax.numpy as jnp
from jax import lax
from jax.experimental import pallas as pl
from jax.experimental.pallas import tpu as pltpu
from jax.sharding import PartitionSpec as P

D = 4096
QK = 64
TAPS = 3
TB = 768
NB = 16
TQ = 256
NT = TB // TQ
VA = 144
SUB = 2
HALF = TB // 2
PR = HALF // SUB
LOG2E = 1.4426950408889634
NEG_LARGE = -1e30
BF16 = jnp.bfloat16
F32 = jnp.float32


def mixer_kernel(
    hid_in, wk_in, wv_in, wq_in, wb_in, wc_in, wh_in, oc_in, oa_in,
    lam_in, hgain_ref, cs_ref, taps_ref, ogain_ref,
    out_ref,
    hid, wp, k_own, v_own, q_src, gated, rim, u_b,
    k_all, v_all, q_own, qa, lam_own, s0, s1, s2, acc, m_ref, o_stage,
    act, wts, sbuf, rbuf, mix, stats,
    h_sem, w_sem, ow_sem, ow_send, ow_recv, rim_send, rim_recv,
    k_recv, v_recv, q_recv, l_recv, o_recv,
    q_send, l_send, p1k_send, p1v_send, rk_send, rv_send, lk_send, lv_send,
    dk_send, dv_send, o_send,
    c_send, c_recv, f_send, f_recv, r_send, r_recv, t_send, t_recv,
):
    sp = lax.axis_index("sp")
    tp = lax.axis_index("tp")
    z, x = sp // 4, sp % 4
    y, c = tp // 2, tp % 2
    own_pair = x + 4 * c
    left, right = (x + 3) % 4, (x + 1) % 4

    def copy_to(src, dst, send_sem, recv_sem, at_sp, at_tp):
        return pltpu.make_async_remote_copy(
            src_ref=src, dst_ref=dst, send_sem=send_sem, recv_sem=recv_sem,
            device_id={"sp": at_sp, "tp": at_tp}, device_id_type=pl.DeviceIdType.MESH,
        )

    def remote(src, dst, send_sem, recv_sem, zz, xx, cc):
        return copy_to(src, dst, send_sem, recv_sem, zz * 4 + xx, y * 2 + cc)

    def partner(src, dst, send_sem, recv_sem):
        return copy_to(src, dst, send_sem, recv_sem, sp, y * 2 + (1 - c))

    loads = [pltpu.make_async_copy(wk_in, wp.at[0], w_sem.at[0])]
    for m in range(NT):
        loads.append(pltpu.make_async_copy(hid_in.at[m * TQ : (m + 1) * TQ], hid.at[m], h_sem.at[m]))
    for n, w_in in enumerate((wv_in, wq_in, wc_in, wh_in, wb_in)):
        loads.append(pltpu.make_async_copy(w_in, wp.at[n + 1], w_sem.at[n + 1]))
    own_out, pair_out = [], []
    for chunk in range(4):
        for n, w_in in enumerate((oc_in, oa_in)):
            dst = wts.at[chunk, pl.ds(n * 512 + c * 256, 256)]
            k = chunk * 2 + n
            own = w_in.at[:, pl.ds(chunk * 1024 + c * 512, 512)]
            theirs = w_in.at[:, pl.ds(chunk * 1024 + (1 - c) * 512, 512)]
            own_out.append(pltpu.make_async_copy(own, dst, ow_sem.at[k]))
            pair_out.append(partner(theirs, dst, ow_send.at[k], ow_recv.at[k]))
    for one in loads:
        one.start()

    barrier = pltpu.get_barrier_semaphore()
    me = sp * 2 + c

    def greet_plane(i, carry):
        other = (me + i) % 32
        pl.semaphore_signal(
            barrier, inc=1, device_id={"sp": other // 2, "tp": y * 2 + other % 2},
            device_id_type=pl.DeviceIdType.MESH,
        )
        return carry

    def greet_column(i, carry):
        pl.semaphore_signal(
            barrier, inc=1, device_id={"sp": sp, "tp": ((y + 1) * 2 + i) % 8},
            device_id_type=pl.DeviceIdType.MESH,
        )
        return carry

    lax.fori_loop(1, 32, greet_plane, 0)
    lax.fori_loop(0, 6, greet_column, 0)

    def project(m, n):
        r = jnp.dot(hid[m], wp[n], preferred_element_type=F32)
        return r.astype(BF16).astype(F32)

    def rotated(t, m, scale):
        cos, sin = cs_ref[0, m], cs_ref[1, m]
        if scale is not None:
            cos, sin = cos * scale, sin * scale
        parts = []
        for g in range(4):
            a, b = t[g * 64 : g * 64 + 32], t[g * 64 + 32 : g * 64 + 64]
            parts += [a * cos - b * sin, b * cos + a * sin]
        return jnp.concatenate(parts, axis=0)

    loads[0].wait()

    def key_rows(m, carry):
        pltpu.make_async_copy(hid_in.at[0:TQ], hid.at[m], h_sem.at[m]).wait()
        r = rotated(project(m, 0).T, m, None).T.astype(BF16)
        rows = pl.ds(pl.multiple_of(m * TQ, TQ), TQ)
        k_own[0, rows, :] = r[:, 0:128]
        k_own[1, rows, :] = r[:, 128:256]
        return carry

    lax.fori_loop(0, NT, key_rows, 0)
    pl.semaphore_wait(barrier, 37)
    for one in own_out + pair_out:
        one.start()

    pair_of_sp = jnp.where(sp < 8, sp, 15 - sp)
    slot_of_sp = jnp.where(sp < 8, 0, 1)

    def kv_same(e):
        return (2 * c + e == z) & (z % 2 == c)

    def q_same(e):
        return (2 * c + e == z) & (pair_of_sp % 4 == x) & (pair_of_sp // 4 == c)

    def key_first(e):
        return remote(k_own.at[e], k_all.at[sp], p1k_send.at[e], k_recv.at[sp], 2 * c + e, x, z % 2)

    def value_first(e):
        return remote(v_own.at[e], v_all.at[sp, pl.ds(0, 128)], p1v_send.at[e], v_recv.at[sp], 2 * c + e, x, z % 2)

    def query_first(e):
        return remote(q_src.at[e], q_own.at[slot_of_sp], q_send.at[e], q_recv.at[slot_of_sp], 2 * c + e, pair_of_sp % 4, pair_of_sp // 4)

    def lam_first(e):
        return remote(lam_in.at[e], lam_own.at[slot_of_sp], l_send.at[e], l_recv.at[slot_of_sp], 2 * c + e, pair_of_sp % 4, pair_of_sp // 4)

    def unless(same, action):
        @pl.when(jnp.logical_not(same))
        def _():
            action()

    for e in range(2):
        unless(kv_same(e), lambda: key_first(e).start())

        @pl.when(kv_same(e))
        def _():
            k_all[sp] = k_own[e]

    def column(m):
        return pl.ds(pl.multiple_of(m * TQ, TQ), TQ)

    loads[4].wait()

    def value_rows(m, carry):
        r = project(m, 1).T.astype(BF16)
        v_own[0, :, column(m)] = r[0:128]
        v_own[1, :, column(m)] = r[128:256]
        return carry

    lax.fori_loop(0, NT, value_rows, 0)
    for e in range(2):
        unless(kv_same(e), lambda: value_first(e).start())

        @pl.when(kv_same(e))
        def _():
            v_all[sp, 0:128, :] = v_own[e]

    loads[5].wait()

    def query_rows(m, carry):
        r = rotated(project(m, 2).T, m, LOG2E * QK ** (-0.5)).astype(BF16)
        q_src[0, :, column(m)] = r[0:128]
        q_src[1, :, column(m)] = r[128:256]
        return carry

    lax.fori_loop(0, NT, query_rows, 0)
    for e in range(2):
        unless(q_same(e), lambda: query_first(e).start())
        unless(q_same(e), lambda: lam_first(e).start())

        @pl.when(q_same(e))
        def _():
            q_own[slot_of_sp] = q_src[e]
            lam_own[slot_of_sp] = lam_in[e]

    for n in (6, 7, 8):
        loads[n].wait()

    def gated_rows(m, carry):
        gated[pl.ds(pl.multiple_of(8 + m * TQ, 8), TQ), :] = project(m, 3) * project(m, 4)
        return carry

    lax.fori_loop(0, NT, gated_rows, 0)

    def gate_rows(m, carry):
        u_b[m] = jnp.dot(hid[m], wp[5], preferred_element_type=F32).astype(BF16)
        return carry

    lax.fori_loop(0, NT, gate_rows, 0)

    rim_copy = copy_to(
        gated.at[pl.ds(TB, 8)], rim, rim_send, rim_recv, (sp + 1) % 16, tp
    )

    @pl.when(sp < 15)
    def _():
        rim_copy.start()

    def ones(j, carry):
        v_all[j, 128:VA, :] = jnp.ones((VA - 128, TB), BF16)
        return carry

    lax.fori_loop(0, NB, ones, 0)
    acc[...] = jnp.zeros(acc.shape, F32)
    m_ref[...] = jnp.full(m_ref.shape, NEG_LARGE, F32)

    @pl.when(sp > 0)
    def _():
        rim_copy.wait_recv()
        gated[0:8, :] = rim[...]

    @pl.when(sp == 0)
    def _():
        gated[0:8, :] = jnp.zeros((8, 256), F32)

    for m in range(NT):
        total = jnp.zeros((TQ, 256), F32)
        for tap in range(TAPS):
            first = 8 + m * TQ - (TAPS - 1) + tap
            total = total + taps_ref[tap : tap + 1, :] * gated[first : first + TQ, :]
        conv = (u_b[m].astype(F32) * total).astype(BF16)
        act[2 * c, m * TQ : (m + 1) * TQ, :] = conv[:, 0:128]
        act[2 * c + 1, m * TQ : (m + 1) * TQ, :] = conv[:, 128:256]

    zero = jnp.zeros((QK, TQ), BF16)
    for qb in range(2):
        q_blk = own_pair if qb == 0 else 15 - own_pair
        same = (q_blk == sp) & (z // 2 == c)
        unless(same, lambda: remote(q_src.at[0], q_own.at[qb], q_send.at[0], q_recv.at[qb], z, x, 1 - c).wait_recv())
        unless(same, lambda: remote(lam_in.at[0], lam_own.at[qb], l_send.at[0], l_recv.at[qb], z, x, 1 - c).wait_recv())
        for t in range(NT):
            qt = q_own[qb, :, t * TQ : (t + 1) * TQ]
            qa[qb * NT + t, 0:QK, 0:TQ] = qt[0:QK]
            qa[qb * NT + t, QK:128, 0:TQ] = zero
            qa[qb * NT + t, 0:QK, TQ : 2 * TQ] = zero
            qa[qb * NT + t, QK:128, TQ : 2 * TQ] = qt[QK:128]

    conv_sends = []
    for n in range(2):
        piece = act.at[2 * c + n]
        conv_sends.append(partner(piece, piece, c_send.at[n], c_recv.at[n]))
    for one in conv_sends:
        one.start()

    scores = (s0, s1, s2)

    def unit(qb, j, diagonal):
        tops = [None] * NT

        def produce(t):
            rows = TQ * (t + 1) if diagonal else TB
            s = jnp.dot(k_all[j, 0:rows, :], qa[qb * NT + t], preferred_element_type=F32)
            if diagonal:
                key = lax.broadcasted_iota(jnp.int32, (rows, 2 * TQ), 0)
                query = lax.broadcasted_iota(jnp.int32, (rows, 2 * TQ), 1)
                query = jnp.where(query >= TQ, query - TQ, query) + t * TQ
                s = jnp.where(key <= query, s, NEG_LARGE)
            scores[t][0:rows, :] = s
            tops[t] = jnp.max(s, axis=0, keepdims=True)

        def consume(t):
            rows = TQ * (t + 1) if diagonal else TB
            at = qb * NT + t
            before = m_ref[at]
            after = jnp.maximum(before, tops[t])
            w = jnp.exp2(scores[t][0:rows, :] - after).astype(BF16)
            factor = jnp.exp2(before - after)
            acc[at] = acc[at] * factor + jnp.dot(
                v_all[j, :, 0:rows], w, preferred_element_type=F32
            )
            m_ref[at] = after

        produce(0)
        produce(1)
        consume(0)
        produce(2)
        consume(1)
        consume(2)

    def k_copy(blk, sems, n, xx, cc):
        return remote(k_all.at[blk], k_all.at[blk], sems.at[n], k_recv.at[blk], z, xx, cc)

    def v_copy(blk, sems, n, xx, cc):
        part = v_all.at[blk, pl.ds(0, 128)]
        return remote(part, part, sems.at[n], v_recv.at[blk], z, xx, cc)

    def block_of(w, u):
        side = jnp.where(u < 2, left, right)
        col = jnp.where(w == 0, x, jnp.where(w == 3, (x + 2) % 4, side))
        row = jnp.where(w == 2, (u + 2) % 4, u)
        return row * 4 + col

    def arrived(blk):
        k_copy(blk, dk_send, 0, x, 1 - c).wait_recv()
        v_copy(blk, dv_send, 0, x, 1 - c).wait_recv()

    def pass_right(blk, n):
        k_copy(blk, rk_send, n, right, c).start()
        v_copy(blk, rv_send, n, right, c).start()

    def pass_left(blk, n):
        k_copy(blk, lk_send, n, left, c).start()
        v_copy(blk, lv_send, n, left, c).start()

    def pass_partner(blk, n):
        k_copy(blk, dk_send, n, x, 1 - c).start()
        v_copy(blk, dv_send, n, x, 1 - c).start()

    low, high = c * 4 + x, (c + 2) * 4 + x
    unless((low == sp) & (z // 2 == c), lambda: arrived(low))
    pass_right(low, 0)
    unless((high == sp) & (z // 2 == c), lambda: arrived(high))
    pass_left(high, 0)
    pass_right(high, 1)
    pass_left(low, 1)
    pass_partner(low, 0)
    pass_partner(high, 1)

    def exchange(w):
        from_left, from_right = block_of(w, c), block_of(w, c + 2)
        arrived(from_left)

        @pl.when(w == 1)
        def _():
            pass_right(from_left, 2)

        pass_partner(from_left, 2 * w)
        arrived(from_right)

        @pl.when(w == 1)
        def _():
            pass_left(from_right, 2)

        pass_partner(from_right, 2 * w + 1)

    def step(i, carry):
        w, k = i // 4, i % 4
        u = jnp.where(k < 2, c + 2 * k, 1 - c + 2 * (k - 2))
        blk = block_of(w, u)

        @pl.when((k == 3) & (w < 3))
        def _():
            exchange(w + 1)

        @pl.when(k >= 2)
        def _():
            arrived(blk)

        def for_queries(qb, carry):
            q_blk = jnp.where(qb == 0, own_pair, 15 - own_pair)

            @pl.when(blk < q_blk)
            def _():
                unit(qb, blk, False)

            @pl.when(blk == q_blk)
            def _():
                unit(qb, blk, True)

            return carry

        lax.fori_loop(0, 2, for_queries, 0)
        return carry

    lax.fori_loop(0, NB, step, 0)

    def out_same(q_blk):
        return (q_blk == sp) & (z // 2 == c)

    def out_copy(qb, q_blk):
        return remote(
            o_stage.at[qb], act.at[4 + z], o_send.at[qb], o_recv.at[z % 2],
            q_blk // 4, q_blk % 4, z // 2,
        )

    q_blks = (own_pair, 15 - own_pair)
    for qb in range(2):
        lam = lam_own[qb, 0:1, 0:1]
        for t in range(NT):
            at = qb * NT + t
            n1 = acc[at, 0:128, 0:TQ] / acc[at, 128:129, 0:TQ]
            n2 = acc[at, 0:128, TQ : 2 * TQ] / acc[at, 128:129, TQ : 2 * TQ]
            diff = n1 - lam * n2
            mean = jnp.mean(diff * diff, axis=0, keepdims=True)
            normed = diff * lax.rsqrt(mean + 1e-05) * hgain_ref[...]
            o_stage[qb, t * TQ : (t + 1) * TQ, :] = normed.T.astype(BF16)
        unless(out_same(q_blks[qb]), lambda: out_copy(qb, q_blks[qb]).start())

        @pl.when(out_same(q_blks[qb]))
        def _():
            act[4 + z] = o_stage[qb]

    forwards = []
    for e in range(2):
        head = 2 * c + e
        made_here = (head == z) & ((sp == own_pair) | (sp == 15 - own_pair))
        piece = act.at[4 + head]
        unless(made_here, lambda: remote(o_stage.at[0], piece, o_send.at[0], o_recv.at[e], z, x, 1 - c).wait_recv())
        forwards.append(partner(piece, piece, f_send.at[e], f_recv.at[e]))
        forwards[e].start()
    for one in own_out:
        one.wait()
    for one in pair_out + conv_sends + forwards:
        one.wait_recv()

    up, down = ((y + 1) % 4) * 2 + c, ((y + 3) % 4) * 2 + c

    def ring(s, d, u):
        return copy_to(
            sbuf.at[s, d, u], rbuf.at[s, d, u], r_send.at[s, d, u], r_recv.at[s, d, u],
            sp, up if d == 0 else down,
        )

    for s in range(4):
        for u in range(SUB):
            for d in range(2):
                chunk = (y + 3 - s) % 4 if d == 0 else (y + 1 + s) % 4
                first = d * HALF + u * PR
                rows = jnp.concatenate([act[n, first : first + PR, :] for n in range(8)], axis=1)
                part = jnp.dot(rows, wts[chunk], preferred_element_type=F32)
                if s > 0:
                    ring(s - 1, d, u).wait_recv()
                    part = part + rbuf[s - 1, d, u].astype(F32)
                if s < 3:
                    sbuf[s, d, u] = part.astype(BF16)
                    ring(s, d, u).start()
                else:
                    mix[first : first + PR, :] = part.astype(BF16)

    ones_row = jnp.ones((8, 512), BF16)
    dims = (((1,), (1,)), ((), ()))
    m = mix[...]
    square = m.astype(F32) * m.astype(F32)
    high = square.astype(BF16)
    low = (square - high.astype(F32)).astype(BF16)
    total = lax.dot_general(ones_row, m, dims, preferred_element_type=F32)
    squares = lax.dot_general(ones_row, high, dims, preferred_element_type=F32)
    squares = squares + lax.dot_general(ones_row, low, dims, preferred_element_type=F32)
    row = lax.broadcasted_iota(jnp.int32, (8, TB), 0)
    stats[tp] = jnp.where(row == 0, total, squares)

    def tell(i):
        return copy_to(stats.at[tp], stats.at[tp], t_send.at[i - 1], t_recv.at[i - 1], sp, (tp + i) % 8)

    for i in range(1, 8):
        tell(i).start()
    for i in range(1, 8):
        tell(i).wait_recv()
    everything = stats[0]
    for n in range(1, 8):
        everything = everything + stats[n]
    columns = everything.T
    mean = columns[:, 0:1] * (1.0 / D)
    variance = columns[:, 1:2] * (1.0 / D) - mean * mean
    out_ref[...] = (
        (mix[...].astype(F32) - mean) * lax.rsqrt(variance + 1e-05) * ogain_ref[tp]
    ).astype(BF16)


    for e in range(2):
        unless(kv_same(e), lambda: key_first(e).wait_send())
        unless(kv_same(e), lambda: value_first(e).wait_send())
        unless(q_same(e), lambda: query_first(e).wait_send())
        unless(q_same(e), lambda: lam_first(e).wait_send())
        unless(out_same(q_blks[e]), lambda: out_copy(e, q_blks[e]).wait_send())

    @pl.when(sp < 15)
    def _():
        rim_copy.wait_send()

    for n in range(3):
        k_copy(0, rk_send, n, right, c).wait_send()
        v_copy(0, rv_send, n, right, c).wait_send()
        k_copy(0, lk_send, n, left, c).wait_send()
        v_copy(0, lv_send, n, left, c).wait_send()
    for n in range(8):
        k_copy(0, dk_send, n, x, 1 - c).wait_send()
        v_copy(0, dv_send, n, x, 1 - c).wait_send()
    for one in pair_out + conv_sends + forwards:
        one.wait_send()
    for s in range(3):
        for d in range(2):
            for u in range(SUB):
                ring(s, d, u).wait_send()
    for i in range(1, 8):
        tell(i).wait_send()


def mixer(*arrays):
    dma = pltpu.SemaphoreType.DMA
    hbm = pl.BlockSpec(memory_space=pl.ANY)
    vmem = pl.BlockSpec(memory_space=pltpu.VMEM)
    return pl.pallas_call(
        mixer_kernel,
        out_shape=jax.ShapeDtypeStruct((TB, 512), BF16),
        in_specs=[hbm] * 9 + [vmem] * 5,
        out_specs=vmem,
        scratch_shapes=[
            pltpu.VMEM((NT, TQ, D), BF16),
            pltpu.VMEM((6, D, 256), BF16),
            pltpu.VMEM((2, TB, 128), BF16),
            pltpu.VMEM((2, 128, TB), BF16),
            pltpu.VMEM((2, 128, TB), BF16),
            pltpu.VMEM((TB + 8, 256), F32),
            pltpu.VMEM((8, 256), F32),
            pltpu.VMEM((NT, TQ, 256), BF16),
            pltpu.VMEM((NB, TB, 128), BF16),
            pltpu.VMEM((NB, VA, TB), BF16),
            pltpu.VMEM((2, 128, TB), BF16),
            pltpu.VMEM((2 * NT, 128, 2 * TQ), BF16),
            pltpu.VMEM((2, 8, 128), F32),
            pltpu.VMEM((TB, 2 * TQ), F32),
            pltpu.VMEM((TB, 2 * TQ), F32),
            pltpu.VMEM((TB, 2 * TQ), F32),
            pltpu.VMEM((2 * NT, VA, 2 * TQ), F32),
            pltpu.VMEM((2 * NT, 1, 2 * TQ), F32),
            pltpu.VMEM((2, TB, 128), BF16),
            pltpu.VMEM((8, TB, 128), BF16),
            pltpu.VMEM((4, 1024, 512), BF16),
            pltpu.VMEM((3, 2, SUB, PR, 512), BF16),
            pltpu.VMEM((3, 2, SUB, PR, 512), BF16),
            pltpu.VMEM((TB, 512), BF16),
            pltpu.VMEM((8, 8, TB), F32),
            dma((NT,)), dma((6,)), dma((8,)), dma((8,)), dma((8,)), dma, dma,
            dma((NB,)), dma((NB,)), dma((2,)), dma((2,)), dma((2,)),
            dma((2,)), dma((2,)), dma((2,)), dma((2,)),
            dma((3,)), dma((3,)), dma((3,)), dma((3,)),
            dma((8,)), dma((8,)), dma((2,)),
            dma((2,)), dma((2,)), dma((2,)), dma((2,)),
            dma((3, 2, SUB)), dma((3, 2, SUB)), dma((7,)), dma((7,)),
        ],
        compiler_params=pltpu.CompilerParams(
            collective_id=0, has_side_effects=True, vmem_limit_bytes=67043328
        ),
        name="mixer",
    )(*arrays)


def per_device(
    hidden_states,
    w_conv_b,
    w_conv_c,
    w_conv_h,
    conv_taps,
    w_query,
    w_key,
    w_value,
    lambdas,
    head_gain,
    w_out_conv,
    w_out_attn,
    out_gain,
):
    first = lax.axis_index("sp") * TB
    positions = (first + jnp.arange(TB, dtype=jnp.int32)).astype(F32).reshape(NT, 1, TQ)
    inverse = 1.0 / 10000.0 ** (jnp.arange(0, QK, 2, dtype=F32) / QK)
    angles = positions * inverse[None, :, None]
    table = jnp.stack([jnp.cos(angles), jnp.sin(angles)])
    return mixer(
        hidden_states, w_key, w_value, w_query, w_conv_b, w_conv_c, w_conv_h,
        w_out_conv, w_out_attn,
        jnp.broadcast_to(lambdas[:, None, None], (2, 8, 128)),
        head_gain.astype(F32)[:, None],
        table,
        conv_taps.astype(F32),
        out_gain.astype(F32).reshape(8, 1, 512),
    )


def solution(mesh):
    return jax.shard_map(
        per_device,
        mesh=mesh,
        in_specs=(
            P("sp", None),
            P(None, "tp"),
            P(None, "tp"),
            P(None, "tp"),
            P(None, "tp"),
            P(None, "tp"),
            P(None, "tp"),
            P(None, "tp"),
            P("tp"),
            P(),
            P("tp", None),
            P("tp", None),
            P(),
        ),
        out_specs=P("sp", "tp"),
        check_vma=False,
    )
```

```python
import jax
import jax.numpy as jnp
from jax import lax
from jax.experimental import pallas as pl
from jax.experimental.pallas import tpu as pltpu
from jax.sharding import PartitionSpec as P

D = 4096
QK = 64
TAPS = 3
TB = 768
NB = 16
TQ = 256
NT = TB // TQ
VA = 144
SUB = 2
HALF = TB // 2
PR = HALF // SUB
LOG2E = 1.4426950408889634
NEG_LARGE = -1e30
BF16 = jnp.bfloat16
F32 = jnp.float32


def mixer_kernel(
    hid_in, wk_in, wv_in, wq_in, wb_in, wc_in, wh_in, oc_in, oa_in,
    lam_ref, hgain_ref, cs_ref, taps_ref, ogain_ref,
    out_ref,
    hid, wp, k_own, v_own, q_src, lam_in, gated, rim, u_b,
    k_all, v_all, q_own, qa, lam_own, s0, s1, s2, acc, m_ref, o_stage,
    act, wts, sbuf, rbuf, mix, stats,
    h_sem, w_sem, ow_sem, ow_send, ow_recv, rim_send, rim_recv,
    k_recv, v_recv, q_recv, l_recv, o_recv,
    q_send, l_send, p1k_send, p1v_send, rk_send, rv_send, lk_send, lv_send,
    dk_send, dv_send, o_send,
    c_send, c_recv, f_send, f_recv, r_send, r_recv, t_send, t_recv,
):
    sp = lax.axis_index("sp")
    tp = lax.axis_index("tp")
    z, x = sp // 4, sp % 4
    y, c = tp // 2, tp % 2
    own_pair = x + 4 * c
    left, right = (x + 3) % 4, (x + 1) % 4

    def copy_to(src, dst, send_sem, recv_sem, at_sp, at_tp):
        return pltpu.make_async_remote_copy(
            src_ref=src, dst_ref=dst, send_sem=send_sem, recv_sem=recv_sem,
            device_id={"sp": at_sp, "tp": at_tp}, device_id_type=pl.DeviceIdType.MESH,
        )

    def remote(src, dst, send_sem, recv_sem, zz, xx, cc):
        return copy_to(src, dst, send_sem, recv_sem, zz * 4 + xx, y * 2 + cc)

    def partner(src, dst, send_sem, recv_sem):
        return copy_to(src, dst, send_sem, recv_sem, sp, y * 2 + (1 - c))

    loads = [pltpu.make_async_copy(wk_in, wp.at[0], w_sem.at[0])]
    for m in range(NT):
        loads.append(pltpu.make_async_copy(hid_in.at[m * TQ : (m + 1) * TQ], hid.at[m], h_sem.at[m]))
    for n, w_in in enumerate((wv_in, wq_in, wc_in, wh_in, wb_in)):
        loads.append(pltpu.make_async_copy(w_in, wp.at[n + 1], w_sem.at[n + 1]))
    own_out, pair_out = [], []
    for chunk in range(4):
        for n, w_in in enumerate((oc_in, oa_in)):
            dst = wts.at[chunk, pl.ds(n * 512 + c * 256, 256)]
            k = chunk * 2 + n
            own = w_in.at[:, pl.ds(chunk * 1024 + c * 512, 512)]
            theirs = w_in.at[:, pl.ds(chunk * 1024 + (1 - c) * 512, 512)]
            own_out.append(pltpu.make_async_copy(own, dst, ow_sem.at[k]))
            pair_out.append(partner(theirs, dst, ow_send.at[k], ow_recv.at[k]))
    for one in loads[:4]:
        one.start()

    barrier = pltpu.get_barrier_semaphore()
    me = sp * 2 + c

    def greet_plane(i, carry):
        other = (me + i) % 32
        pl.semaphore_signal(
            barrier, inc=1, device_id={"sp": other // 2, "tp": y * 2 + other % 2},
            device_id_type=pl.DeviceIdType.MESH,
        )
        return carry

    def greet_column(i, carry):
        pl.semaphore_signal(
            barrier, inc=1, device_id={"sp": sp, "tp": ((y + 1) * 2 + i) % 8},
            device_id_type=pl.DeviceIdType.MESH,
        )
        return carry

    lax.fori_loop(1, 32, greet_plane, 0)
    lax.fori_loop(0, 6, greet_column, 0)

    def project(m, n):
        r = jnp.dot(hid[m], wp[n], preferred_element_type=F32)
        return r.astype(BF16).astype(F32)

    def rotated(t, m, scale):
        cos, sin = cs_ref[0, m], cs_ref[1, m]
        if scale is not None:
            cos, sin = cos * scale, sin * scale
        parts = []
        for g in range(4):
            a, b = t[g * 64 : g * 64 + 32], t[g * 64 + 32 : g * 64 + 64]
            parts += [a * cos - b * sin, b * cos + a * sin]
        return jnp.concatenate(parts, axis=0)

    for e in range(2):
        lam_in[e] = jnp.full((8, 128), lam_ref[e], F32)

    loads[0].wait()
    for one in loads[4:6]:
        one.start()

    def key_rows(m, carry):
        pltpu.make_async_copy(hid_in.at[0:TQ], hid.at[m], h_sem.at[m]).wait()
        r = rotated(project(m, 0).T, m, None).T.astype(BF16)
        rows = pl.ds(pl.multiple_of(m * TQ, TQ), TQ)
        k_own[0, rows, :] = r[:, 0:128]
        k_own[1, rows, :] = r[:, 128:256]
        return carry

    lax.fori_loop(0, NT, key_rows, 0)
    for one in loads[6:]:
        one.start()
    pl.semaphore_wait(barrier, 37)
    for one in own_out + pair_out:
        one.start()

    pair_of_sp = jnp.where(sp < 8, sp, 15 - sp)
    slot_of_sp = jnp.where(sp < 8, 0, 1)

    def kv_same(e):
        return (2 * c + e == z) & (z % 2 == c)

    def q_same(e):
        return (2 * c + e == z) & (pair_of_sp % 4 == x) & (pair_of_sp // 4 == c)

    def key_first(e):
        return remote(k_own.at[e], k_all.at[sp], p1k_send.at[e], k_recv.at[sp], 2 * c + e, x, z % 2)

    def value_first(e):
        return remote(v_own.at[e], v_all.at[sp, pl.ds(0, 128)], p1v_send.at[e], v_recv.at[sp], 2 * c + e, x, z % 2)

    def query_first(e):
        return remote(q_src.at[e], q_own.at[slot_of_sp], q_send.at[e], q_recv.at[slot_of_sp], 2 * c + e, pair_of_sp % 4, pair_of_sp // 4)

    def lam_first(e):
        return remote(lam_in.at[e], lam_own.at[slot_of_sp], l_send.at[e], l_recv.at[slot_of_sp], 2 * c + e, pair_of_sp % 4, pair_of_sp // 4)

    def unless(same, action):
        @pl.when(jnp.logical_not(same))
        def _():
            action()

    def k_copy(blk, sems, n, xx, cc):
        return remote(k_all.at[blk], k_all.at[blk], sems.at[n], k_recv.at[blk], z, xx, cc)

    def v_copy(blk, sems, n, xx, cc):
        part = v_all.at[blk, pl.ds(0, 128)]
        return remote(part, part, sems.at[n], v_recv.at[blk], z, xx, cc)

    def block_of(w, u):
        side = jnp.where(u < 2, left, right)
        col = jnp.where(w == 0, x, jnp.where(w == 3, (x + 2) % 4, side))
        row = jnp.where(w == 2, (u + 2) % 4, u)
        return row * 4 + col

    def k_arrived(blk):
        k_copy(blk, dk_send, 0, x, 1 - c).wait_recv()

    def v_arrived(blk):
        v_copy(blk, dv_send, 0, x, 1 - c).wait_recv()

    def arrived(blk):
        k_arrived(blk)
        v_arrived(blk)

    def pass_right(blk, n):
        k_copy(blk, rk_send, n, right, c).start()
        v_copy(blk, rv_send, n, right, c).start()

    def pass_left(blk, n):
        k_copy(blk, lk_send, n, left, c).start()
        v_copy(blk, lv_send, n, left, c).start()

    def pass_partner(blk, n):
        k_copy(blk, dk_send, n, x, 1 - c).start()
        v_copy(blk, dv_send, n, x, 1 - c).start()

    low, high = c * 4 + x, (c + 2) * 4 + x
    near = z % 2 == c

    def send_low(copy, rights, lefts, partners):
        copy(low, rights, 0, right, c).start()
        copy(low, lefts, 1, left, c).start()
        copy(low, partners, 0, x, 1 - c).start()

    def send_high(copy, rights, lefts, partners):
        copy(high, lefts, 0, left, c).start()
        copy(high, rights, 1, right, c).start()
        copy(high, partners, 1, x, 1 - c).start()

    def start_own(copy, here, rights, lefts, partners):
        @pl.when(near)
        def _():
            unless(z // 2 == c, lambda: here(sp))

            @pl.when(z < 2)
            def _():
                send_low(copy, rights, lefts, partners)

            @pl.when(z >= 2)
            def _():
                send_high(copy, rights, lefts, partners)

    def start_rest(copy, here, rights, lefts, partners):
        @pl.when(jnp.logical_not(near & (z < 2)))
        def _():
            here(low)
            send_low(copy, rights, lefts, partners)

        @pl.when(jnp.logical_not(near & (z >= 2)))
        def _():
            here(high)
            send_high(copy, rights, lefts, partners)

    k_ring = (k_copy, k_arrived, rk_send, lk_send, dk_send)
    v_ring = (v_copy, v_arrived, rv_send, lv_send, dv_send)

    for e in range(2):
        unless(kv_same(e), lambda: key_first(e).start())

        @pl.when(kv_same(e))
        def _():
            k_all[sp] = k_own[e]

    def column(m):
        return pl.ds(pl.multiple_of(m * TQ, TQ), TQ)

    loads[4].wait()

    def value_rows(m, carry):
        r = project(m, 1).T.astype(BF16)
        v_own[0, :, column(m)] = r[0:128]
        v_own[1, :, column(m)] = r[128:256]
        return carry

    lax.fori_loop(0, NT, value_rows, 0)
    for e in range(2):
        unless(kv_same(e), lambda: value_first(e).start())

        @pl.when(kv_same(e))
        def _():
            v_all[sp, 0:128, :] = v_own[e]

    start_own(*k_ring)

    loads[5].wait()

    def query_rows(m, carry):
        r = rotated(project(m, 2).T, m, LOG2E * QK ** (-0.5)).astype(BF16)
        q_src[0, :, column(m)] = r[0:128]
        q_src[1, :, column(m)] = r[128:256]
        return carry

    lax.fori_loop(0, NT, query_rows, 0)
    for e in range(2):
        unless(q_same(e), lambda: query_first(e).start())
        unless(q_same(e), lambda: lam_first(e).start())

        @pl.when(q_same(e))
        def _():
            q_own[slot_of_sp] = q_src[e]
            lam_own[slot_of_sp] = lam_in[e]

    start_own(*v_ring)

    for n in (6, 7, 8):
        loads[n].wait()

    def gated_rows(m, carry):
        gated[pl.ds(pl.multiple_of(8 + m * TQ, 8), TQ), :] = project(m, 3) * project(m, 4)
        return carry

    lax.fori_loop(0, NT, gated_rows, 0)
    start_rest(*k_ring)

    def gate_rows(m, carry):
        u_b[m] = jnp.dot(hid[m], wp[5], preferred_element_type=F32).astype(BF16)
        return carry

    lax.fori_loop(0, NT, gate_rows, 0)

    rim_copy = copy_to(
        gated.at[pl.ds(TB, 8)], rim, rim_send, rim_recv, (sp + 1) % 16, tp
    )

    @pl.when(sp < 15)
    def _():
        rim_copy.start()

    def ones(j, carry):
        v_all[j, 128:VA, :] = jnp.ones((VA - 128, TB), BF16)
        return carry

    lax.fori_loop(0, NB, ones, 0)
    acc[...] = jnp.zeros(acc.shape, F32)
    m_ref[...] = jnp.full(m_ref.shape, NEG_LARGE, F32)
    start_rest(*v_ring)

    zero = jnp.zeros((QK, TQ), BF16)
    for qb in range(2):
        q_blk = own_pair if qb == 0 else 15 - own_pair
        same = (q_blk == sp) & (z // 2 == c)
        unless(same, lambda: remote(q_src.at[0], q_own.at[qb], q_send.at[0], q_recv.at[qb], z, x, 1 - c).wait_recv())
        unless(same, lambda: remote(lam_in.at[0], lam_own.at[qb], l_send.at[0], l_recv.at[qb], z, x, 1 - c).wait_recv())
        for t in range(NT):
            qt = q_own[qb, :, t * TQ : (t + 1) * TQ]
            qa[qb * NT + t, 0:QK, 0:TQ] = qt[0:QK]
            qa[qb * NT + t, QK:128, 0:TQ] = zero
            qa[qb * NT + t, 0:QK, TQ : 2 * TQ] = zero
            qa[qb * NT + t, QK:128, TQ : 2 * TQ] = qt[QK:128]

    scores = (s0, s1, s2)

    def unit(qb, j, diagonal):
        tops = [None] * NT

        def produce(t):
            rows = TQ * (t + 1) if diagonal else TB
            s = jnp.dot(k_all[j, 0:rows, :], qa[qb * NT + t], preferred_element_type=F32)
            if diagonal:
                key = lax.broadcasted_iota(jnp.int32, (rows, 2 * TQ), 0)
                query = lax.broadcasted_iota(jnp.int32, (rows, 2 * TQ), 1)
                query = jnp.where(query >= TQ, query - TQ, query) + t * TQ
                s = jnp.where(key <= query, s, NEG_LARGE)
            scores[t][0:rows, :] = s
            tops[t] = jnp.max(s, axis=0, keepdims=True)

        def consume(t):
            rows = TQ * (t + 1) if diagonal else TB
            at = qb * NT + t
            before = m_ref[at]
            after = jnp.maximum(before, tops[t])
            w = jnp.exp2(scores[t][0:rows, :] - after).astype(BF16)
            factor = jnp.exp2(before - after)
            acc[at] = acc[at] * factor + jnp.dot(
                v_all[j, :, 0:rows], w, preferred_element_type=F32
            )
            m_ref[at] = after

        produce(0)
        produce(1)
        consume(0)
        produce(2)
        consume(1)
        consume(2)

    def exchange(w):
        from_left, from_right = block_of(w, c), block_of(w, c + 2)
        arrived(from_left)

        @pl.when(w == 1)
        def _():
            pass_right(from_left, 2)

        pass_partner(from_left, 2 * w)
        arrived(from_right)

        @pl.when(w == 1)
        def _():
            pass_left(from_right, 2)

        pass_partner(from_right, 2 * w + 1)

    def out_same(q_blk):
        return (q_blk == sp) & (z // 2 == c)

    def out_copy(qb, q_blk):
        return remote(
            o_stage.at[qb], act.at[4 + z], o_send.at[qb], o_recv.at[z % 2],
            q_blk // 4, q_blk % 4, z // 2,
        )

    q_blks = (own_pair, 15 - own_pair)

    def finish(qb):
        hgain = jnp.broadcast_to(hgain_ref[...].astype(F32).reshape(1, 128), (8, 128)).T[:, 0:1]
        lam = lam_own[qb, 0:1, 0:1]
        for t in range(NT):
            at = qb * NT + t
            n1 = acc[at, 0:128, 0:TQ] / acc[at, 128:129, 0:TQ]
            n2 = acc[at, 0:128, TQ : 2 * TQ] / acc[at, 128:129, TQ : 2 * TQ]
            diff = n1 - lam * n2
            mean = jnp.mean(diff * diff, axis=0, keepdims=True)
            normed = diff * lax.rsqrt(mean + 1e-05) * hgain
            o_stage[qb, t * TQ : (t + 1) * TQ, :] = normed.T.astype(BF16)
        unless(out_same(q_blks[qb]), lambda: out_copy(qb, q_blks[qb]).start())

        @pl.when(out_same(q_blks[qb]))
        def _():
            act[4 + z] = o_stage[qb]

    conv_sends = []
    for n in range(2):
        piece = act.at[2 * c + n]
        conv_sends.append(partner(piece, piece, c_send.at[n], c_recv.at[n]))

    def convolve():
        @pl.when(sp > 0)
        def _():
            rim_copy.wait_recv()
            gated[0:8, :] = rim[...]

        @pl.when(sp == 0)
        def _():
            gated[0:8, :] = jnp.zeros((8, 256), F32)

        taps = taps_ref[...].astype(F32)
        for m in range(NT):
            total = jnp.zeros((TQ, 256), F32)
            for tap in range(TAPS):
                first = 8 + m * TQ - (TAPS - 1) + tap
                total = total + taps[tap : tap + 1, :] * gated[first : first + TQ, :]
            conv = (u_b[m].astype(F32) * total).astype(BF16)
            act[2 * c, m * TQ : (m + 1) * TQ, :] = conv[:, 0:128]
            act[2 * c + 1, m * TQ : (m + 1) * TQ, :] = conv[:, 128:256]
        for one in conv_sends:
            one.start()

    def step(i, carry):
        w, k = i // 4, i % 4
        plain = jnp.where(k < 2, c + 2 * k, 1 - c + 2 * (k - 2))
        last = jnp.where(k % 2 == 0, c, 1 - c) + 2 * (k // 2)
        u = jnp.where(w == 3, last, plain)
        blk = block_of(w, u)

        @pl.when((k == 3) & (w < 3))
        def _():
            exchange(w + 1)

        @pl.when(u % 2 != c)
        def _():
            arrived(blk)

        @pl.when(i == 9)
        def _():
            convolve()

        @pl.when(i == NB - 2)
        def _():
            finish(0)

        def for_queries(qb, carry):
            q_blk = jnp.where(qb == 0, own_pair, 15 - own_pair)

            @pl.when(blk < q_blk)
            def _():
                unit(qb, blk, False)

            @pl.when(blk == q_blk)
            def _():
                unit(qb, blk, True)

            return carry

        lax.fori_loop(0, 2, for_queries, 0)
        return carry

    lax.fori_loop(0, NB, step, 0)

    finish(1)

    forwards = []
    for e in range(2):
        head = 2 * c + e
        made_here = (head == z) & ((sp == own_pair) | (sp == 15 - own_pair))
        piece = act.at[4 + head]
        unless(made_here, lambda: remote(o_stage.at[0], piece, o_send.at[0], o_recv.at[e], z, x, 1 - c).wait_recv())
        forwards.append(partner(piece, piece, f_send.at[e], f_recv.at[e]))
        forwards[e].start()
    for one in own_out:
        one.wait()
    for one in pair_out + conv_sends + forwards:
        one.wait_recv()

    up, down = ((y + 1) % 4) * 2 + c, ((y + 3) % 4) * 2 + c

    def ring(s, d, u):
        return copy_to(
            sbuf.at[s, d, u], rbuf.at[s, d, u], r_send.at[s, d, u], r_recv.at[s, d, u],
            sp, up if d == 0 else down,
        )

    for s in range(4):
        for u in range(SUB):
            for d in range(2):
                chunk = (y + 3 - s) % 4 if d == 0 else (y + 1 + s) % 4
                first = d * HALF + u * PR
                rows = jnp.concatenate([act[n, first : first + PR, :] for n in range(8)], axis=1)
                part = jnp.dot(rows, wts[chunk], preferred_element_type=F32)
                if s > 0:
                    ring(s - 1, d, u).wait_recv()
                    part = part + rbuf[s - 1, d, u].astype(F32)
                if s < 3:
                    sbuf[s, d, u] = part.astype(BF16)
                    ring(s, d, u).start()
                else:
                    mix[first : first + PR, :] = part.astype(BF16)

    ones_row = jnp.ones((8, 512), BF16)
    dims = (((1,), (1,)), ((), ()))
    m = mix[...]
    square = m.astype(F32) * m.astype(F32)
    high = square.astype(BF16)
    low = (square - high.astype(F32)).astype(BF16)
    total = lax.dot_general(ones_row, m, dims, preferred_element_type=F32)
    squares = lax.dot_general(ones_row, high, dims, preferred_element_type=F32)
    squares = squares + lax.dot_general(ones_row, low, dims, preferred_element_type=F32)
    row = lax.broadcasted_iota(jnp.int32, (8, TB), 0)
    stats[tp] = jnp.where(row == 0, total, squares)

    def tell(i):
        return copy_to(stats.at[tp], stats.at[tp], t_send.at[i - 1], t_recv.at[i - 1], sp, (tp + i) % 8)

    for i in range(1, 8):
        tell(i).start()
    for i in range(1, 8):
        tell(i).wait_recv()
    everything = stats[0]
    for n in range(1, 8):
        everything = everything + stats[n]
    columns = everything.T
    ogain = ogain_ref[pl.ds(pl.multiple_of(tp * 512, 512), 512)].astype(F32).reshape(1, 512)
    mean = columns[:, 0:1] * (1.0 / D)
    variance = columns[:, 1:2] * (1.0 / D) - mean * mean
    out_ref[...] = (
        (mix[...].astype(F32) - mean) * lax.rsqrt(variance + 1e-05) * ogain
    ).astype(BF16)


    for e in range(2):
        unless(kv_same(e), lambda: key_first(e).wait_send())
        unless(kv_same(e), lambda: value_first(e).wait_send())
        unless(q_same(e), lambda: query_first(e).wait_send())
        unless(q_same(e), lambda: lam_first(e).wait_send())
        unless(out_same(q_blks[e]), lambda: out_copy(e, q_blks[e]).wait_send())

    @pl.when(sp < 15)
    def _():
        rim_copy.wait_send()

    for n in range(3):
        k_copy(0, rk_send, n, right, c).wait_send()
        v_copy(0, rv_send, n, right, c).wait_send()
        k_copy(0, lk_send, n, left, c).wait_send()
        v_copy(0, lv_send, n, left, c).wait_send()
    for n in range(8):
        k_copy(0, dk_send, n, x, 1 - c).wait_send()
        v_copy(0, dv_send, n, x, 1 - c).wait_send()
    for one in pair_out + conv_sends + forwards:
        one.wait_send()
    for s in range(3):
        for d in range(2):
            for u in range(SUB):
                ring(s, d, u).wait_send()
    for i in range(1, 8):
        tell(i).wait_send()


def mixer(*arrays):
    dma = pltpu.SemaphoreType.DMA
    hbm = pl.BlockSpec(memory_space=pl.ANY)
    vmem = pl.BlockSpec(memory_space=pltpu.VMEM)
    return pl.pallas_call(
        mixer_kernel,
        out_shape=jax.ShapeDtypeStruct((TB, 512), BF16),
        in_specs=[hbm] * 9 + [pl.BlockSpec(memory_space=pltpu.SMEM)] + [vmem] * 4,
        out_specs=vmem,
        scratch_shapes=[
            pltpu.VMEM((NT, TQ, D), BF16),
            pltpu.VMEM((6, D, 256), BF16),
            pltpu.VMEM((2, TB, 128), BF16),
            pltpu.VMEM((2, 128, TB), BF16),
            pltpu.VMEM((2, 128, TB), BF16),
            pltpu.VMEM((2, 8, 128), F32),
            pltpu.VMEM((TB + 8, 256), F32),
            pltpu.VMEM((8, 256), F32),
            pltpu.VMEM((NT, TQ, 256), BF16),
            pltpu.VMEM((NB, TB, 128), BF16),
            pltpu.VMEM((NB, VA, TB), BF16),
            pltpu.VMEM((2, 128, TB), BF16),
            pltpu.VMEM((2 * NT, 128, 2 * TQ), BF16),
            pltpu.VMEM((2, 8, 128), F32),
            pltpu.VMEM((TB, 2 * TQ), F32),
            pltpu.VMEM((TB, 2 * TQ), F32),
            pltpu.VMEM((TB, 2 * TQ), F32),
            pltpu.VMEM((2 * NT, VA, 2 * TQ), F32),
            pltpu.VMEM((2 * NT, 1, 2 * TQ), F32),
            pltpu.VMEM((2, TB, 128), BF16),
            pltpu.VMEM((8, TB, 128), BF16),
            pltpu.VMEM((4, 1024, 512), BF16),
            pltpu.VMEM((3, 2, SUB, PR, 512), BF16),
            pltpu.VMEM((3, 2, SUB, PR, 512), BF16),
            pltpu.VMEM((TB, 512), BF16),
            pltpu.VMEM((8, 8, TB), F32),
            dma((NT,)), dma((6,)), dma((8,)), dma((8,)), dma((8,)), dma, dma,
            dma((NB,)), dma((NB,)), dma((2,)), dma((2,)), dma((2,)),
            dma((2,)), dma((2,)), dma((2,)), dma((2,)),
            dma((3,)), dma((3,)), dma((3,)), dma((3,)),
            dma((8,)), dma((8,)), dma((2,)),
            dma((2,)), dma((2,)), dma((2,)), dma((2,)),
            dma((3, 2, SUB)), dma((3, 2, SUB)), dma((7,)), dma((7,)),
        ],
        compiler_params=pltpu.CompilerParams(
            collective_id=0, has_side_effects=True, vmem_limit_bytes=67043328
        ),
        name="mixer",
    )(*arrays)


def per_device(
    hidden_states,
    w_conv_b,
    w_conv_c,
    w_conv_h,
    conv_taps,
    w_query,
    w_key,
    w_value,
    lambdas,
    head_gain,
    w_out_conv,
    w_out_attn,
    out_gain,
):
    first = lax.axis_index("sp") * TB
    positions = (first + jnp.arange(TB, dtype=jnp.int32)).astype(F32).reshape(NT, 1, TQ)
    inverse = 1.0 / 10000.0 ** (jnp.arange(0, QK, 2, dtype=F32) / QK)
    angles = positions * inverse[None, :, None]
    table = jnp.stack([jnp.cos(angles), jnp.sin(angles)])
    return mixer(
        hidden_states, w_key, w_value, w_query, w_conv_b, w_conv_c, w_conv_h,
        w_out_conv, w_out_attn,
        lambdas,
        head_gain,
        table,
        conv_taps,
        out_gain,
    )


def solution(mesh):
    return jax.shard_map(
        per_device,
        mesh=mesh,
        in_specs=(
            P("sp", None),
            P(None, "tp"),
            P(None, "tp"),
            P(None, "tp"),
            P(None, "tp"),
            P(None, "tp"),
            P(None, "tp"),
            P(None, "tp"),
            P("tp"),
            P(),
            P("tp", None),
            P("tp", None),
            P(),
        ),
        out_specs=P("sp", "tp"),
        check_vma=False,
    )
```

```python
import jax
import jax.numpy as jnp
from jax import lax
from jax.experimental import pallas as pl
from jax.experimental.pallas import tpu as pltpu
from jax.sharding import PartitionSpec as P

D = 4096
QK = 64
TAPS = 3
TB = 768
NB = 16
TQ = 256
NT = TB // TQ
VA = 144
HALF = TB // 2
PR = HALF // 2
LOG2E = 1.4426950408889634
NEG_LARGE = -1e30
BF16 = jnp.bfloat16
F32 = jnp.float32


def mixer_kernel(
    hid_in, wk_in, wv_in, wq_in, wb_in, wc_in, wh_in, oc_in, oa_in,
    lam_ref, hgain_ref, cs_ref, taps_ref, ogain_ref,
    out_ref,
    hid, wp, k_own, v_own, q_src, lam_in, gated, halo, u_b,
    k_all, v_all, q_own, qa, lam_own, s0, s1, s2, acc, m_ref, o_stage,
    act, wtc, wta, sbuf, rbuf, mixc, mix, stats,
    h_sem, w_sem, ow_sem, ow_send, ow_recv, aw_sem, aw_send, aw_recv, halo_send, halo_recv,
    k_recv, v_recv, q_recv, l_recv, o_recv,
    q_send, l_send, p1k_send, p1v_send, rk_send, rv_send, lk_send, lv_send,
    dk_send, dv_send, o_send,
    c_send, c_recv, f_send, r_send, r_recv, t_send, t_recv,
):
    sp = lax.axis_index("sp")
    tp = lax.axis_index("tp")
    z, x = sp // 4, sp % 4
    y, c = tp // 2, tp % 2
    own_pair = jnp.where(z < 2, x, 3 - x) + 4 * c
    left, right = (x + 3) % 4, (x + 1) % 4

    def copy_to(src, dst, send_sem, recv_sem, at_sp, at_tp):
        return pltpu.make_async_remote_copy(
            src_ref=src, dst_ref=dst, send_sem=send_sem, recv_sem=recv_sem,
            device_id={"sp": at_sp, "tp": at_tp}, device_id_type=pl.DeviceIdType.MESH,
        )

    def remote(src, dst, send_sem, recv_sem, zz, xx, cc):
        return copy_to(src, dst, send_sem, recv_sem, zz * 4 + xx, y * 2 + cc)

    def partner(src, dst, send_sem, recv_sem):
        return copy_to(src, dst, send_sem, recv_sem, sp, y * 2 + (1 - c))

    loads = [pltpu.make_async_copy(wk_in, wp.at[0], w_sem.at[0])]
    for m in range(NT):
        loads.append(pltpu.make_async_copy(hid_in.at[m * TQ : (m + 1) * TQ], hid.at[m], h_sem.at[m]))
    for n, w_in in enumerate((wv_in, wq_in, wc_in, wh_in, wb_in)):
        loads.append(pltpu.make_async_copy(w_in, wp.at[n + 1], w_sem.at[n + 1]))
    own_out, pair_out = [], []
    for chunk in range(4):
        dst = wtc.at[chunk, pl.ds(c * 256, 256)]
        own = oc_in.at[:, pl.ds(chunk * 1024 + c * 512, 512)]
        theirs = oc_in.at[:, pl.ds(chunk * 1024 + (1 - c) * 512, 512)]
        own_out.append(pltpu.make_async_copy(own, dst, ow_sem.at[chunk]))
        pair_out.append(partner(theirs, dst, ow_send.at[chunk], ow_recv.at[chunk]))
    own_out.append(pltpu.make_async_copy(oa_in.at[:, pl.ds(tp * 512, 512)], wta.at[tp], aw_sem))
    for i in range(1, 8):
        other = (tp + i) % 8
        pair_out.append(copy_to(
            oa_in.at[:, pl.ds(other * 512, 512)], wta.at[tp], aw_send.at[i - 1], aw_recv.at[i - 1], sp, other
        ))
    halo_copy = copy_to(
        hid_in.at[pl.ds(TB - 16, 16)], halo, halo_send, halo_recv, (sp + 1) % 16, tp
    )
    for one in loads[:4]:
        one.start()

    barrier = pltpu.get_barrier_semaphore()
    me = sp * 2 + c

    def greet_plane(i, carry):
        other = (me + i) % 32
        pl.semaphore_signal(
            barrier, inc=1, device_id={"sp": other // 2, "tp": y * 2 + other % 2},
            device_id_type=pl.DeviceIdType.MESH,
        )
        return carry

    def greet_column(i, carry):
        pl.semaphore_signal(
            barrier, inc=1, device_id={"sp": sp, "tp": ((y + 1) * 2 + i) % 8},
            device_id_type=pl.DeviceIdType.MESH,
        )
        return carry

    pair_of_sp = jnp.where(sp < 8, sp, 15 - sp)
    slot_of_sp = jnp.where(sp < 8, 0, 1)
    pair_col = jnp.where(c == 0, pair_of_sp % 4, 3 - pair_of_sp % 4)
    q_blks = (own_pair, 15 - own_pair)
    for up in range(1, 4):
        plane = ((y + up) % 4) * 2
        for e in range(2):
            for at_sp, at_tp in (
                (q_blks[e], plane + z // 2),
                ((2 * c + e) * 4 + pair_col, plane + pair_of_sp // 4),
            ):
                pl.semaphore_signal(
                    barrier, inc=1, device_id={"sp": at_sp, "tp": at_tp},
                    device_id_type=pl.DeviceIdType.MESH,
                )
    lax.fori_loop(1, 32, greet_plane, 0)
    lax.fori_loop(0, 6, greet_column, 0)

    def project(m, n):
        r = jnp.dot(hid[m], wp[n], preferred_element_type=F32)
        return r.astype(BF16).astype(F32)

    def rotated(t, m, scale):
        cos, sin = cs_ref[0, m], cs_ref[1, m]
        if scale is not None:
            cos, sin = cos * scale, sin * scale
        parts = []
        for g in range(4):
            a, b = t[g * 64 : g * 64 + 32], t[g * 64 + 32 : g * 64 + 64]
            parts += [a * cos - b * sin, b * cos + a * sin]
        return jnp.concatenate(parts, axis=0)

    for e in range(2):
        lam_in[e] = jnp.full((8, 128), lam_ref[e], F32)

    loads[0].wait()
    for one in loads[4:6]:
        one.start()

    def key_rows(m, carry):
        pltpu.make_async_copy(hid_in.at[0:TQ], hid.at[m], h_sem.at[m]).wait()
        r = rotated(project(m, 0).T, m, None).T.astype(BF16)
        rows = pl.ds(pl.multiple_of(m * TQ, TQ), TQ)
        k_own[0, rows, :] = r[:, 0:128]
        k_own[1, rows, :] = r[:, 128:256]
        return carry

    lax.fori_loop(0, NT, key_rows, 0)
    for one in loads[6:]:
        one.start()
    pl.semaphore_wait(barrier, 49)

    @pl.when(sp < 15)
    def _():
        halo_copy.start()


    def kv_same(e):
        return (2 * c + e == z) & (z % 2 == c)

    def q_same(e):
        return (2 * c + e == z) & (pair_col == x) & (pair_of_sp // 4 == c)

    def key_first(e):
        return remote(k_own.at[e], k_all.at[sp], p1k_send.at[e], k_recv.at[sp], 2 * c + e, x, z % 2)

    def value_first(e):
        return remote(v_own.at[e], v_all.at[sp, pl.ds(0, 128)], p1v_send.at[e], v_recv.at[sp], 2 * c + e, x, z % 2)

    def query_first(e):
        return remote(q_src.at[e], q_own.at[slot_of_sp], q_send.at[e], q_recv.at[slot_of_sp], 2 * c + e, pair_col, pair_of_sp // 4)

    def lam_first(e):
        return remote(lam_in.at[e], lam_own.at[slot_of_sp], l_send.at[e], l_recv.at[slot_of_sp], 2 * c + e, pair_col, pair_of_sp // 4)

    def unless(same, action):
        @pl.when(jnp.logical_not(same))
        def _():
            action()

    def k_copy(blk, sems, n, xx, cc):
        return remote(k_all.at[blk], k_all.at[blk], sems.at[n], k_recv.at[blk], z, xx, cc)

    def v_copy(blk, sems, n, xx, cc):
        part = v_all.at[blk, pl.ds(0, 128)]
        return remote(part, part, sems.at[n], v_recv.at[blk], z, xx, cc)

    def block_of(w, u):
        side = jnp.where(u < 2, left, right)
        col = jnp.where(w == 0, x, jnp.where(w == 3, (x + 2) % 4, side))
        row = jnp.where(w == 2, (u + 2) % 4, u)
        return row * 4 + col

    def k_arrived(blk):
        k_copy(blk, dk_send, 0, x, 1 - c).wait_recv()

    def v_arrived(blk):
        v_copy(blk, dv_send, 0, x, 1 - c).wait_recv()

    def arrived(blk):
        k_arrived(blk)
        v_arrived(blk)

    def pass_right(blk, n):
        k_copy(blk, rk_send, n, right, c).start()
        v_copy(blk, rv_send, n, right, c).start()

    def pass_left(blk, n):
        k_copy(blk, lk_send, n, left, c).start()
        v_copy(blk, lv_send, n, left, c).start()

    def pass_partner(blk, n):
        k_copy(blk, dk_send, n, x, 1 - c).start()
        v_copy(blk, dv_send, n, x, 1 - c).start()

    low, high = c * 4 + x, (c + 2) * 4 + x
    near = z % 2 == c

    def send_low(copy, rights, lefts, partners):
        copy(low, rights, 0, right, c).start()
        copy(low, lefts, 1, left, c).start()
        copy(low, partners, 0, x, 1 - c).start()

    def send_high(copy, rights, lefts, partners):
        copy(high, lefts, 0, left, c).start()
        copy(high, rights, 1, right, c).start()
        copy(high, partners, 1, x, 1 - c).start()

    def start_own(copy, here, rights, lefts, partners):
        @pl.when(near)
        def _():
            unless(z // 2 == c, lambda: here(sp))

            @pl.when(z < 2)
            def _():
                send_low(copy, rights, lefts, partners)

            @pl.when(z >= 2)
            def _():
                send_high(copy, rights, lefts, partners)

    def start_rest(copy, here, rights, lefts, partners):
        @pl.when(jnp.logical_not(near & (z < 2)))
        def _():
            here(low)
            send_low(copy, rights, lefts, partners)

        @pl.when(jnp.logical_not(near & (z >= 2)))
        def _():
            here(high)
            send_high(copy, rights, lefts, partners)

    k_ring = (k_copy, k_arrived, rk_send, lk_send, dk_send)
    v_ring = (v_copy, v_arrived, rv_send, lv_send, dv_send)

    for e in range(2):
        unless(kv_same(e), lambda: key_first(e).start())

        @pl.when(kv_same(e))
        def _():
            k_all[sp] = k_own[e]

    for one in own_out + pair_out:
        one.start()

    def column(m):
        return pl.ds(pl.multiple_of(m * TQ, TQ), TQ)

    loads[4].wait()

    def value_rows(m, carry):
        r = project(m, 1).T.astype(BF16)
        v_own[0, :, column(m)] = r[0:128]
        v_own[1, :, column(m)] = r[128:256]
        return carry

    lax.fori_loop(0, NT, value_rows, 0)
    for e in range(2):
        unless(kv_same(e), lambda: value_first(e).start())

        @pl.when(kv_same(e))
        def _():
            v_all[sp, 0:128, :] = v_own[e]

    start_own(*k_ring)

    loads[5].wait()

    def query_rows(m, carry):
        r = rotated(project(m, 2).T, m, LOG2E * QK ** (-0.5)).astype(BF16)
        q_src[0, :, column(m)] = r[0:128]
        q_src[1, :, column(m)] = r[128:256]
        return carry

    lax.fori_loop(0, NT, query_rows, 0)
    for e in range(2):
        unless(q_same(e), lambda: query_first(e).start())
        unless(q_same(e), lambda: lam_first(e).start())

        @pl.when(q_same(e))
        def _():
            q_own[slot_of_sp] = q_src[e]
            lam_own[slot_of_sp] = lam_in[e]

    start_own(*v_ring)

    loads[6].wait()

    def gated_rows(m, carry):
        rows = pl.ds(pl.multiple_of(8 + m * TQ, 8), TQ)
        gated[rows, :] = gated[rows, :] * project(m, 4)
        return carry

    def inner_rows(m, carry):
        gated[pl.ds(pl.multiple_of(8 + m * TQ, 8), TQ), :] = project(m, 3)
        return carry

    lax.fori_loop(0, NT, inner_rows, 0)
    start_rest(*k_ring)
    loads[7].wait()
    lax.fori_loop(0, NT, gated_rows, 0)
    loads[8].wait()

    def gate_rows(m, carry):
        u_b[m] = jnp.dot(hid[m], wp[5], preferred_element_type=F32).astype(BF16)
        return carry

    lax.fori_loop(0, NT, gate_rows, 0)

    def ones(j, carry):
        v_all[j, 128:VA, :] = jnp.ones((VA - 128, TB), BF16)
        return carry

    lax.fori_loop(0, NB, ones, 0)
    acc[...] = jnp.zeros(acc.shape, F32)
    m_ref[...] = jnp.full(m_ref.shape, NEG_LARGE, F32)
    start_rest(*v_ring)

    zero = jnp.zeros((QK, TQ), BF16)
    for qb in range(2):
        q_blk = own_pair if qb == 0 else 15 - own_pair
        same = (q_blk == sp) & (z // 2 == c)
        unless(same, lambda: remote(q_src.at[0], q_own.at[qb], q_send.at[0], q_recv.at[qb], z, x, 1 - c).wait_recv())
        unless(same, lambda: remote(lam_in.at[0], lam_own.at[qb], l_send.at[0], l_recv.at[qb], z, x, 1 - c).wait_recv())
        for t in range(NT):
            qt = q_own[qb, :, t * TQ : (t + 1) * TQ]
            qa[qb * NT + t, 0:QK, 0:TQ] = qt[0:QK]
            qa[qb * NT + t, QK:128, 0:TQ] = zero
            qa[qb * NT + t, 0:QK, TQ : 2 * TQ] = zero
            qa[qb * NT + t, QK:128, TQ : 2 * TQ] = qt[QK:128]

    scores = (s0, s1, s2)

    def unit(qb, j, diagonal):
        tops = [None] * NT

        def produce(t):
            rows = TQ * (t + 1) if diagonal else TB
            s = jnp.dot(k_all[j, 0:rows, :], qa[qb * NT + t], preferred_element_type=F32)
            if diagonal:
                key = lax.broadcasted_iota(jnp.int32, (rows, 2 * TQ), 0)
                query = lax.broadcasted_iota(jnp.int32, (rows, 2 * TQ), 1)
                query = jnp.where(query >= TQ, query - TQ, query) + t * TQ
                s = jnp.where(key <= query, s, NEG_LARGE)
            scores[t][0:rows, :] = s
            tops[t] = jnp.max(s, axis=0, keepdims=True)

        def consume(t):
            rows = TQ * (t + 1) if diagonal else TB
            at = qb * NT + t
            before = m_ref[at]
            after = jnp.maximum(before, tops[t])
            w = jnp.exp2(scores[t][0:rows, :] - after).astype(BF16)
            factor = jnp.exp2(before - after)
            acc[at] = acc[at] * factor + jnp.dot(
                v_all[j, :, 0:rows], w, preferred_element_type=F32
            )
            m_ref[at] = after

        produce(0)
        produce(1)
        consume(0)
        produce(2)
        consume(1)
        consume(2)

    def exchange(w):
        from_left, from_right = block_of(w, c), block_of(w, c + 2)
        arrived(from_left)

        @pl.when(w == 1)
        def _():
            pass_right(from_left, 2)

        pass_partner(from_left, 2 * w)
        arrived(from_right)

        @pl.when(w == 1)
        def _():
            pass_left(from_right, 2)

        pass_partner(from_right, 2 * w + 1)

    def out_same(q_blk):
        return (q_blk == sp) & (z // 2 == c)

    def out_copies(qb):
        for n in range(4):
            plane = (y + n) % 4
            yield n, copy_to(
                o_stage.at[qb], act.at[4 + y * 4 + z], o_send.at[qb, n], o_recv.at[y * 4 + z],
                q_blks[qb], plane * 2 + z // 2,
            )

    def finish(qb):
        hgain = jnp.broadcast_to(hgain_ref[...].astype(F32).reshape(1, 128), (8, 128)).T[:, 0:1]
        lam = lam_own[qb, 0:1, 0:1]
        for t in range(NT):
            at = qb * NT + t
            n1 = acc[at, 0:128, 0:TQ] / acc[at, 128:129, 0:TQ]
            n2 = acc[at, 0:128, TQ : 2 * TQ] / acc[at, 128:129, TQ : 2 * TQ]
            diff = n1 - lam * n2
            mean = jnp.mean(diff * diff, axis=0, keepdims=True)
            normed = diff * lax.rsqrt(mean + 1e-05) * hgain
            o_stage[qb, t * TQ : (t + 1) * TQ, :] = normed.T.astype(BF16)
        for n, one in out_copies(qb):
            if n == 0:
                unless(out_same(q_blks[qb]), lambda: one.start())
            else:
                one.start()

        @pl.when(out_same(q_blks[qb]))
        def _():
            act[4 + y * 4 + z] = o_stage[qb]

    conv_sends = []
    for n in range(2):
        piece = act.at[2 * c + n]
        conv_sends.append(partner(piece, piece, c_send.at[n], c_recv.at[n]))

    def convolve():
        @pl.when(sp > 0)
        def _():
            halo_copy.wait_recv()
            inner = jnp.dot(halo[...], wp[3], preferred_element_type=F32).astype(BF16)
            outer = jnp.dot(halo[...], wp[4], preferred_element_type=F32).astype(BF16)
            gated[0:8, :] = inner[8:16].astype(F32) * outer[8:16].astype(F32)

        @pl.when(sp == 0)
        def _():
            gated[0:8, :] = jnp.zeros((8, 256), F32)

        taps = taps_ref[...].astype(F32)
        for m in range(NT):
            total = jnp.zeros((TQ, 256), F32)
            for tap in range(TAPS):
                first = 8 + m * TQ - (TAPS - 1) + tap
                total = total + taps[tap : tap + 1, :] * gated[first : first + TQ, :]
            conv = (u_b[m].astype(F32) * total).astype(BF16)
            act[2 * c, m * TQ : (m + 1) * TQ, :] = conv[:, 0:128]
            act[2 * c + 1, m * TQ : (m + 1) * TQ, :] = conv[:, 128:256]
        for one in conv_sends:
            one.start()

    convolve()

    up, down = ((y + 1) % 4) * 2 + c, ((y + 3) % 4) * 2 + c

    def ring(s, d):
        return copy_to(
            sbuf.at[s, d], rbuf.at[s, d], r_send.at[s, d], r_recv.at[s, d],
            sp, up if d == 0 else down,
        )

    def conv_ring(s):
        for d in range(2):
            chunk = (y + 3 - s) % 4 if d == 0 else (y + 1 + s) % 4
            first = d * HALF
            rows = jnp.concatenate([act[n, first : first + HALF, :] for n in range(4)], axis=1)
            part = jnp.dot(rows, wtc[chunk], preferred_element_type=F32)
            if s > 0:
                ring(s - 1, d).wait_recv()
                part = part + rbuf[s - 1, d].astype(F32)
            if s < 3:
                sbuf[s, d] = part.astype(BF16)
                ring(s, d).start()
            else:
                mixc[first : first + HALF, :] = part

    def step(i, carry):
        w, k = i // 4, i % 4
        plain = jnp.where(k < 2, c + 2 * k, 1 - c + 2 * (k - 2))
        last = jnp.where(k % 2 == 0, c, 1 - c) + 2 * (k // 2)
        u = jnp.where(w == 3, last, plain)
        blk = block_of(w, u)

        @pl.when((k == 3) & (w < 3))
        def _():
            exchange(w + 1)

        @pl.when(u % 2 != c)
        def _():
            arrived(blk)

        for s, when in enumerate((2, 8, 14)):

            @pl.when(i == when)
            def _():
                if s == 0:
                    for one in own_out:
                        one.wait()
                    for one in pair_out[:4] + conv_sends:
                        one.wait_recv()
                conv_ring(s)

        @pl.when(i == NB - 2)
        def _():
            finish(0)

        def for_queries(qb, carry):
            q_blk = jnp.where(qb == 0, own_pair, 15 - own_pair)

            @pl.when(blk < q_blk)
            def _():
                unit(qb, blk, False)

            @pl.when(blk == q_blk)
            def _():
                unit(qb, blk, True)

            return carry

        lax.fori_loop(0, 2, for_queries, 0)
        return carry

    lax.fori_loop(0, NB, step, 0)

    finish(1)

    conv_ring(3)

    def piece(head):
        return act.at[4 + head]

    def o_arrived(head):
        partner(piece(head), piece(head), f_send.at[0], o_recv.at[head]).wait_recv()

    forwards = []
    for n in (0, 1, 3, 2):
        for e in range(2):
            head = ((y + n) % 4) * 4 + 2 * c + e
            if n == 0:
                made_here = (2 * c + e == z) & ((sp == own_pair) | (sp == 15 - own_pair))
                unless(made_here, lambda: o_arrived(head))
            else:
                o_arrived(head)
            forwards.append(partner(piece(head), piece(head), f_send.at[len(forwards)], o_recv.at[head]))
            forwards[-1].start()
    for one in pair_out[4:]:
        one.wait_recv()
    for n in (0, 1, 3, 2):
        for e in range(2):
            o_arrived(((y + n) % 4) * 4 + 2 * (1 - c) + e)
    for n in range(4):
        first = n * PR
        rows = jnp.concatenate([act[4 + h, first : first + PR, :] for h in range(16)], axis=1)
        part = jnp.dot(rows, wta[...].reshape(2048, 512), preferred_element_type=F32)
        mix[first : first + PR, :] = (part + mixc[first : first + PR, :]).astype(BF16)

    ones_row = jnp.ones((8, 512), BF16)
    dims = (((1,), (1,)), ((), ()))
    m = mix[...]
    square = m.astype(F32) * m.astype(F32)
    high = square.astype(BF16)
    low = (square - high.astype(F32)).astype(BF16)
    total = lax.dot_general(ones_row, m, dims, preferred_element_type=F32)
    squares = lax.dot_general(ones_row, high, dims, preferred_element_type=F32)
    squares = squares + lax.dot_general(ones_row, low, dims, preferred_element_type=F32)
    row = lax.broadcasted_iota(jnp.int32, (8, TB), 0)
    stats[tp] = jnp.where(row == 0, total, squares)

    def tell(i):
        return copy_to(stats.at[tp], stats.at[tp], t_send.at[i - 1], t_recv.at[i - 1], sp, (tp + i) % 8)

    for i in range(1, 8):
        tell(i).start()
    for i in range(1, 8):
        tell(i).wait_recv()
    everything = stats[0]
    for n in range(1, 8):
        everything = everything + stats[n]
    columns = everything.T
    ogain = ogain_ref[pl.ds(pl.multiple_of(tp * 512, 512), 512)].astype(F32).reshape(1, 512)
    mean = columns[:, 0:1] * (1.0 / D)
    variance = columns[:, 1:2] * (1.0 / D) - mean * mean
    out_ref[...] = (
        (mix[...].astype(F32) - mean) * lax.rsqrt(variance + 1e-05) * ogain
    ).astype(BF16)


    for e in range(2):
        unless(kv_same(e), lambda: key_first(e).wait_send())
        unless(kv_same(e), lambda: value_first(e).wait_send())
        unless(q_same(e), lambda: query_first(e).wait_send())
        unless(q_same(e), lambda: lam_first(e).wait_send())
        for n, one in out_copies(e):
            if n == 0:
                unless(out_same(q_blks[e]), lambda: one.wait_send())
            else:
                one.wait_send()

    @pl.when(sp < 15)
    def _():
        halo_copy.wait_send()

    for n in range(3):
        k_copy(0, rk_send, n, right, c).wait_send()
        v_copy(0, rv_send, n, right, c).wait_send()
        k_copy(0, lk_send, n, left, c).wait_send()
        v_copy(0, lv_send, n, left, c).wait_send()
    for n in range(8):
        k_copy(0, dk_send, n, x, 1 - c).wait_send()
        v_copy(0, dv_send, n, x, 1 - c).wait_send()
    for one in pair_out + conv_sends + forwards:
        one.wait_send()
    for s in range(3):
        for d in range(2):
            ring(s, d).wait_send()
    for i in range(1, 8):
        tell(i).wait_send()


def mixer(*arrays):
    dma = pltpu.SemaphoreType.DMA
    hbm = pl.BlockSpec(memory_space=pl.ANY)
    vmem = pl.BlockSpec(memory_space=pltpu.VMEM)
    return pl.pallas_call(
        mixer_kernel,
        out_shape=jax.ShapeDtypeStruct((TB, 512), BF16),
        in_specs=[hbm] * 9 + [pl.BlockSpec(memory_space=pltpu.SMEM)] + [vmem] * 4,
        out_specs=vmem,
        scratch_shapes=[
            pltpu.VMEM((NT, TQ, D), BF16),
            pltpu.VMEM((6, D, 256), BF16),
            pltpu.VMEM((2, TB, 128), BF16),
            pltpu.VMEM((2, 128, TB), BF16),
            pltpu.VMEM((2, 128, TB), BF16),
            pltpu.VMEM((2, 8, 128), F32),
            pltpu.VMEM((TB + 8, 256), F32),
            pltpu.VMEM((16, D), BF16),
            pltpu.VMEM((NT, TQ, 256), BF16),
            pltpu.VMEM((NB, TB, 128), BF16),
            pltpu.VMEM((NB, VA, TB), BF16),
            pltpu.VMEM((2, 128, TB), BF16),
            pltpu.VMEM((2 * NT, 128, 2 * TQ), BF16),
            pltpu.VMEM((2, 8, 128), F32),
            pltpu.VMEM((TB, 2 * TQ), F32),
            pltpu.VMEM((TB, 2 * TQ), F32),
            pltpu.VMEM((TB, 2 * TQ), F32),
            pltpu.VMEM((2 * NT, VA, 2 * TQ), F32),
            pltpu.VMEM((2 * NT, 1, 2 * TQ), F32),
            pltpu.VMEM((2, TB, 128), BF16),
            pltpu.VMEM((20, TB, 128), BF16),
            pltpu.VMEM((4, 512, 512), BF16),
            pltpu.VMEM((8, 256, 512), BF16),
            pltpu.VMEM((3, 2, HALF, 512), BF16),
            pltpu.VMEM((3, 2, HALF, 512), BF16),
            pltpu.VMEM((TB, 512), F32),
            pltpu.VMEM((TB, 512), BF16),
            pltpu.VMEM((8, 8, TB), F32),
            dma((NT,)), dma((6,)), dma((4,)), dma((4,)), dma((4,)), dma, dma((7,)), dma((7,)), dma, dma,
            dma((NB,)), dma((NB,)), dma((2,)), dma((2,)), dma((16,)),
            dma((2,)), dma((2,)), dma((2,)), dma((2,)),
            dma((3,)), dma((3,)), dma((3,)), dma((3,)),
            dma((8,)), dma((8,)), dma((2, 4)),
            dma((2,)), dma((2,)), dma((8,)),
            dma((3, 2)), dma((3, 2)), dma((7,)), dma((7,)),
        ],
        compiler_params=pltpu.CompilerParams(
            collective_id=0, has_side_effects=True, vmem_limit_bytes=67043328
        ),
        name="mixer",
    )(*arrays)


def per_device(
    hidden_states,
    w_conv_b,
    w_conv_c,
    w_conv_h,
    conv_taps,
    w_query,
    w_key,
    w_value,
    lambdas,
    head_gain,
    w_out_conv,
    w_out_attn,
    out_gain,
):
    first = lax.axis_index("sp") * TB
    positions = (first + jnp.arange(TB, dtype=jnp.int32)).astype(F32).reshape(NT, 1, TQ)
    inverse = 1.0 / 10000.0 ** (jnp.arange(0, QK, 2, dtype=F32) / QK)
    angles = positions * inverse[None, :, None]
    table = jnp.stack([jnp.cos(angles), jnp.sin(angles)])
    return mixer(
        hidden_states, w_key, w_value, w_query, w_conv_b, w_conv_c, w_conv_h,
        w_out_conv, w_out_attn,
        lambdas,
        head_gain,
        table,
        conv_taps,
        out_gain,
    )


def solution(mesh):
    return jax.shard_map(
        per_device,
        mesh=mesh,
        in_specs=(
            P("sp", None),
            P(None, "tp"),
            P(None, "tp"),
            P(None, "tp"),
            P(None, "tp"),
            P(None, "tp"),
            P(None, "tp"),
            P(None, "tp"),
            P("tp"),
            P(),
            P("tp", None),
            P("tp", None),
            P(),
        ),
        out_specs=P("sp", "tp"),
        check_vma=False,
    )
```

```python
import jax
import jax.numpy as jnp
from jax import lax
from jax.experimental import pallas as pl
from jax.experimental.pallas import tpu as pltpu
from jax.sharding import PartitionSpec as P

D = 4096
QK = 64
TAPS = 3
TB = 768
NB = 16
TQ = 256
NT = TB // TQ
VA = 144
HALF = TB // 2
PR = HALF // 2
LOG2E = 1.4426950408889634
NEG_LARGE = -1e30
BF16 = jnp.bfloat16
F32 = jnp.float32


def mixer_kernel(
    hid_in, wk_in, wv_in, wq_in, wb_in, wc_in, wh_in, oc_in, oa_in,
    lam_ref, hgain_ref, cs_ref, taps_ref, ogain_ref,
    out_ref,
    hid, wp, k_own, v_own, q_src, lam_in, gated, halo, u_b,
    k_all, v_all, q_own, qa, lam_own, s0, s1, s2, acc, m_ref, o_stage,
    act, wtc, wta, sbuf, rbuf, mixc, mix, stats,
    h_sem, w_sem, ow_sem, ow_send, ow_recv, aw_sem, aw_send, aw_recv, zw_send, zw_recv, halo_send, halo_recv,
    k_recv, v_recv, q_recv, l_recv, o_recv,
    q_send, l_send, p1k_send, p1v_send, rk_send, rv_send, lk_send, lv_send,
    dk_send, dv_send, o_send,
    c_send, c_recv, f_send, r_send, r_recv, t_send, t_recv,
):
    sp = lax.axis_index("sp")
    tp = lax.axis_index("tp")
    z, x = sp // 4, sp % 4
    y, c = tp // 2, tp % 2
    own_pair = jnp.where(z < 2, x, 3 - x) + 4 * c
    left, right = (x + 3) % 4, (x + 1) % 4

    def copy_to(src, dst, send_sem, recv_sem, at_sp, at_tp):
        return pltpu.make_async_remote_copy(
            src_ref=src, dst_ref=dst, send_sem=send_sem, recv_sem=recv_sem,
            device_id={"sp": at_sp, "tp": at_tp}, device_id_type=pl.DeviceIdType.MESH,
        )

    def remote(src, dst, send_sem, recv_sem, zz, xx, cc):
        return copy_to(src, dst, send_sem, recv_sem, zz * 4 + xx, y * 2 + cc)

    def partner(src, dst, send_sem, recv_sem):
        return copy_to(src, dst, send_sem, recv_sem, sp, y * 2 + (1 - c))

    loads = [pltpu.make_async_copy(wk_in, wp.at[0], w_sem.at[0])]
    for m in range(NT):
        loads.append(pltpu.make_async_copy(hid_in.at[m * TQ : (m + 1) * TQ], hid.at[m], h_sem.at[m]))
    for n, w_in in enumerate((wv_in, wq_in, wc_in, wh_in, wb_in)):
        loads.append(pltpu.make_async_copy(w_in, wp.at[n + 1], w_sem.at[n + 1]))
    own_out, pair_out = [], []
    for chunk in range(4):
        dst = wtc.at[chunk, pl.ds(c * 256, 256)]
        own = oc_in.at[:, pl.ds(chunk * 1024 + c * 512, 512)]
        theirs = oc_in.at[:, pl.ds(chunk * 1024 + (1 - c) * 512, 512)]
        own_out.append(pltpu.make_async_copy(own, dst, ow_sem.at[chunk]))
        pair_out.append(partner(theirs, dst, ow_send.at[chunk], ow_recv.at[chunk]))
    own_out.append(pltpu.make_async_copy(oa_in.at[:, pl.ds(tp * 512, 512)], wta.at[tp], aw_sem))
    half = pl.ds((z % 2) * 128, 128)
    near_z = z + 1 - 2 * (z % 2)
    zcopies = []
    for i in range(1, 8):
        other = (tp + i) % 8
        pair_out.append(copy_to(
            oa_in.at[half, pl.ds(other * 512, 512)], wta.at[tp, half], aw_send.at[i - 1], aw_recv.at[i - 1], sp, other
        ))
        piece_of = wta.at[(tp + 8 - i) % 8, half]
        zcopies.append(remote(piece_of, piece_of, zw_send.at[i - 1], zw_recv.at[i - 1], near_z, x, c))
    halo_copy = copy_to(
        hid_in.at[pl.ds(TB - 16, 16)], halo, halo_send, halo_recv, (sp + 1) % 16, tp
    )
    for one in loads[:4]:
        one.start()

    barrier = pltpu.get_barrier_semaphore()
    me = sp * 2 + c

    def greet_plane(i, carry):
        other = (me + i) % 32
        pl.semaphore_signal(
            barrier, inc=1, device_id={"sp": other // 2, "tp": y * 2 + other % 2},
            device_id_type=pl.DeviceIdType.MESH,
        )
        return carry

    def greet_column(i, carry):
        pl.semaphore_signal(
            barrier, inc=1, device_id={"sp": sp, "tp": ((y + 1) * 2 + i) % 8},
            device_id_type=pl.DeviceIdType.MESH,
        )
        return carry

    pair_of_sp = jnp.where(sp < 8, sp, 15 - sp)
    slot_of_sp = jnp.where(sp < 8, 0, 1)
    pair_col = jnp.where(c == 0, pair_of_sp % 4, 3 - pair_of_sp % 4)
    q_blks = (own_pair, 15 - own_pair)
    lax.fori_loop(1, 32, greet_plane, 0)
    lax.fori_loop(0, 6, greet_column, 0)

    def project(m, n):
        r = jnp.dot(hid[m], wp[n], preferred_element_type=F32)
        return r.astype(BF16).astype(F32)

    def rotated(t, m, scale):
        cos, sin = cs_ref[0, m], cs_ref[1, m]
        if scale is not None:
            cos, sin = cos * scale, sin * scale
        parts = []
        for g in range(4):
            a, b = t[g * 64 : g * 64 + 32], t[g * 64 + 32 : g * 64 + 64]
            parts += [a * cos - b * sin, b * cos + a * sin]
        return jnp.concatenate(parts, axis=0)

    for e in range(2):
        lam_in[e] = jnp.full((8, 128), lam_ref[e], F32)

    loads[0].wait()
    for one in loads[4:6]:
        one.start()

    def key_rows(m, carry):
        pltpu.make_async_copy(hid_in.at[0:TQ], hid.at[m], h_sem.at[m]).wait()
        r = rotated(project(m, 0).T, m, None).T.astype(BF16)
        rows = pl.ds(pl.multiple_of(m * TQ, TQ), TQ)
        k_own[0, rows, :] = r[:, 0:128]
        k_own[1, rows, :] = r[:, 128:256]
        return carry

    lax.fori_loop(0, NT, key_rows, 0)
    for one in loads[6:]:
        one.start()
    pl.semaphore_wait(barrier, 37)

    @pl.when(sp < 15)
    def _():
        halo_copy.start()


    def kv_same(e):
        return (2 * c + e == z) & (z % 2 == c)

    def q_same(e):
        return (2 * c + e == z) & (pair_col == x) & (pair_of_sp // 4 == c)

    def key_first(e):
        return remote(k_own.at[e], k_all.at[sp], p1k_send.at[e], k_recv.at[sp], 2 * c + e, x, z % 2)

    def value_first(e):
        return remote(v_own.at[e], v_all.at[sp, pl.ds(0, 128)], p1v_send.at[e], v_recv.at[sp], 2 * c + e, x, z % 2)

    def query_first(e):
        return remote(q_src.at[e], q_own.at[slot_of_sp], q_send.at[e], q_recv.at[slot_of_sp], 2 * c + e, pair_col, pair_of_sp // 4)

    def lam_first(e):
        return remote(lam_in.at[e], lam_own.at[slot_of_sp], l_send.at[e], l_recv.at[slot_of_sp], 2 * c + e, pair_col, pair_of_sp // 4)

    def unless(same, action):
        @pl.when(jnp.logical_not(same))
        def _():
            action()

    def k_copy(blk, sems, n, xx, cc):
        return remote(k_all.at[blk], k_all.at[blk], sems.at[n], k_recv.at[blk], z, xx, cc)

    def v_copy(blk, sems, n, xx, cc):
        part = v_all.at[blk, pl.ds(0, 128)]
        return remote(part, part, sems.at[n], v_recv.at[blk], z, xx, cc)

    def block_of(w, u):
        side = jnp.where(u < 2, left, right)
        col = jnp.where(w == 0, x, jnp.where(w == 3, (x + 2) % 4, side))
        row = jnp.where(w == 2, (u + 2) % 4, u)
        return row * 4 + col

    def k_arrived(blk):
        k_copy(blk, dk_send, 0, x, 1 - c).wait_recv()

    def v_arrived(blk):
        v_copy(blk, dv_send, 0, x, 1 - c).wait_recv()

    def arrived(blk):
        k_arrived(blk)
        v_arrived(blk)

    def pass_right(blk, n):
        k_copy(blk, rk_send, n, right, c).start()
        v_copy(blk, rv_send, n, right, c).start()

    def pass_left(blk, n):
        k_copy(blk, lk_send, n, left, c).start()
        v_copy(blk, lv_send, n, left, c).start()

    def pass_partner(blk, n):
        k_copy(blk, dk_send, n, x, 1 - c).start()
        v_copy(blk, dv_send, n, x, 1 - c).start()

    low, high = c * 4 + x, (c + 2) * 4 + x
    near = z % 2 == c

    def send_low(copy, rights, lefts, partners):
        copy(low, rights, 0, right, c).start()
        copy(low, lefts, 1, left, c).start()
        copy(low, partners, 0, x, 1 - c).start()

    def send_high(copy, rights, lefts, partners):
        copy(high, lefts, 0, left, c).start()
        copy(high, rights, 1, right, c).start()
        copy(high, partners, 1, x, 1 - c).start()

    def start_own(copy, here, rights, lefts, partners):
        @pl.when(near)
        def _():
            unless(z // 2 == c, lambda: here(sp))

            @pl.when(z < 2)
            def _():
                send_low(copy, rights, lefts, partners)

            @pl.when(z >= 2)
            def _():
                send_high(copy, rights, lefts, partners)

    def start_rest(copy, here, rights, lefts, partners):
        @pl.when(jnp.logical_not(near & (z < 2)))
        def _():
            here(low)
            send_low(copy, rights, lefts, partners)

        @pl.when(jnp.logical_not(near & (z >= 2)))
        def _():
            here(high)
            send_high(copy, rights, lefts, partners)

    k_ring = (k_copy, k_arrived, rk_send, lk_send, dk_send)
    v_ring = (v_copy, v_arrived, rv_send, lv_send, dv_send)

    for e in range(2):
        unless(kv_same(e), lambda: key_first(e).start())

        @pl.when(kv_same(e))
        def _():
            k_all[sp] = k_own[e]

    for one in own_out + pair_out:
        one.start()

    def column(m):
        return pl.ds(pl.multiple_of(m * TQ, TQ), TQ)

    loads[4].wait()

    def value_rows(m, carry):
        r = project(m, 1).T.astype(BF16)
        v_own[0, :, column(m)] = r[0:128]
        v_own[1, :, column(m)] = r[128:256]
        return carry

    lax.fori_loop(0, NT, value_rows, 0)
    for e in range(2):
        unless(kv_same(e), lambda: value_first(e).start())

        @pl.when(kv_same(e))
        def _():
            v_all[sp, 0:128, :] = v_own[e]

    start_own(*k_ring)

    loads[5].wait()

    def query_rows(m, carry):
        r = rotated(project(m, 2).T, m, LOG2E * QK ** (-0.5)).astype(BF16)
        q_src[0, :, column(m)] = r[0:128]
        q_src[1, :, column(m)] = r[128:256]
        return carry

    lax.fori_loop(0, NT, query_rows, 0)
    for e in range(2):
        unless(q_same(e), lambda: query_first(e).start())
        unless(q_same(e), lambda: lam_first(e).start())

        @pl.when(q_same(e))
        def _():
            q_own[slot_of_sp] = q_src[e]
            lam_own[slot_of_sp] = lam_in[e]

    start_own(*v_ring)

    loads[6].wait()

    def gated_rows(m, carry):
        rows = pl.ds(pl.multiple_of(8 + m * TQ, 8), TQ)
        gated[rows, :] = gated[rows, :] * project(m, 4)
        return carry

    def inner_rows(m, carry):
        gated[pl.ds(pl.multiple_of(8 + m * TQ, 8), TQ), :] = project(m, 3)
        return carry

    lax.fori_loop(0, NT, inner_rows, 0)
    start_rest(*k_ring)
    loads[7].wait()
    lax.fori_loop(0, NT, gated_rows, 0)
    loads[8].wait()

    def gate_rows(m, carry):
        u_b[m] = jnp.dot(hid[m], wp[5], preferred_element_type=F32).astype(BF16)
        return carry

    lax.fori_loop(0, NT, gate_rows, 0)

    def ones(j, carry):
        v_all[j, 128:VA, :] = jnp.ones((VA - 128, TB), BF16)
        return carry

    lax.fori_loop(0, NB, ones, 0)
    acc[...] = jnp.zeros(acc.shape, F32)
    m_ref[...] = jnp.full(m_ref.shape, NEG_LARGE, F32)
    start_rest(*v_ring)

    zero = jnp.zeros((QK, TQ), BF16)
    for qb in range(2):
        q_blk = own_pair if qb == 0 else 15 - own_pair
        same = (q_blk == sp) & (z // 2 == c)
        unless(same, lambda: remote(q_src.at[0], q_own.at[qb], q_send.at[0], q_recv.at[qb], z, x, 1 - c).wait_recv())
        unless(same, lambda: remote(lam_in.at[0], lam_own.at[qb], l_send.at[0], l_recv.at[qb], z, x, 1 - c).wait_recv())
        for t in range(NT):
            qt = q_own[qb, :, t * TQ : (t + 1) * TQ]
            qa[qb * NT + t, 0:QK, 0:TQ] = qt[0:QK]
            qa[qb * NT + t, QK:128, 0:TQ] = zero
            qa[qb * NT + t, 0:QK, TQ : 2 * TQ] = zero
            qa[qb * NT + t, QK:128, TQ : 2 * TQ] = qt[QK:128]

    scores = (s0, s1, s2)

    def unit(qb, j, diagonal):
        tops = [None] * NT

        def produce(t):
            rows = TQ * (t + 1) if diagonal else TB
            s = jnp.dot(k_all[j, 0:rows, :], qa[qb * NT + t], preferred_element_type=F32)
            if diagonal:
                key = lax.broadcasted_iota(jnp.int32, (rows, 2 * TQ), 0)
                query = lax.broadcasted_iota(jnp.int32, (rows, 2 * TQ), 1)
                query = jnp.where(query >= TQ, query - TQ, query) + t * TQ
                s = jnp.where(key <= query, s, NEG_LARGE)
            scores[t][0:rows, :] = s
            tops[t] = jnp.max(s, axis=0, keepdims=True)

        def consume(t):
            rows = TQ * (t + 1) if diagonal else TB
            at = qb * NT + t
            before = m_ref[at]
            after = jnp.maximum(before, tops[t])
            w = jnp.exp2(scores[t][0:rows, :] - after).astype(BF16)
            factor = jnp.exp2(before - after)
            acc[at] = acc[at] * factor + jnp.dot(
                v_all[j, :, 0:rows], w, preferred_element_type=F32
            )
            m_ref[at] = after

        produce(0)
        produce(1)
        consume(0)
        produce(2)
        consume(1)
        consume(2)

    def exchange(w):
        from_left, from_right = block_of(w, c), block_of(w, c + 2)
        arrived(from_left)

        @pl.when(w == 1)
        def _():
            pass_right(from_left, 2)

        pass_partner(from_left, 2 * w)
        arrived(from_right)

        @pl.when(w == 1)
        def _():
            pass_left(from_right, 2)

        pass_partner(from_right, 2 * w + 1)

    def out_same(q_blk):
        return (q_blk == sp) & (z // 2 == c)

    def out_copy(qb):
        return remote(
            o_stage.at[qb], act.at[4 + y * 4 + z], o_send.at[qb], o_recv.at[y * 4 + z],
            q_blks[qb] // 4, q_blks[qb] % 4, z // 2,
        )

    def finish(qb):
        hgain = jnp.broadcast_to(hgain_ref[...].astype(F32).reshape(1, 128), (8, 128)).T[:, 0:1]
        lam = lam_own[qb, 0:1, 0:1]
        for t in range(NT):
            at = qb * NT + t
            n1 = acc[at, 0:128, 0:TQ] / acc[at, 128:129, 0:TQ]
            n2 = acc[at, 0:128, TQ : 2 * TQ] / acc[at, 128:129, TQ : 2 * TQ]
            diff = n1 - lam * n2
            mean = jnp.mean(diff * diff, axis=0, keepdims=True)
            normed = diff * lax.rsqrt(mean + 1e-05) * hgain
            o_stage[qb, t * TQ : (t + 1) * TQ, :] = normed.T.astype(BF16)
        unless(out_same(q_blks[qb]), lambda: out_copy(qb).start())

        @pl.when(out_same(q_blks[qb]))
        def _():
            act[4 + y * 4 + z] = o_stage[qb]

    conv_sends = []
    for n in range(2):
        piece = act.at[2 * c + n]
        conv_sends.append(partner(piece, piece, c_send.at[n], c_recv.at[n]))

    def convolve():
        @pl.when(sp > 0)
        def _():
            halo_copy.wait_recv()
            inner = jnp.dot(halo[...], wp[3], preferred_element_type=F32).astype(BF16)
            outer = jnp.dot(halo[...], wp[4], preferred_element_type=F32).astype(BF16)
            gated[0:8, :] = inner[8:16].astype(F32) * outer[8:16].astype(F32)

        @pl.when(sp == 0)
        def _():
            gated[0:8, :] = jnp.zeros((8, 256), F32)

        taps = taps_ref[...].astype(F32)
        for m in range(NT):
            total = jnp.zeros((TQ, 256), F32)
            for tap in range(TAPS):
                first = 8 + m * TQ - (TAPS - 1) + tap
                total = total + taps[tap : tap + 1, :] * gated[first : first + TQ, :]
            conv = (u_b[m].astype(F32) * total).astype(BF16)
            act[2 * c, m * TQ : (m + 1) * TQ, :] = conv[:, 0:128]
            act[2 * c + 1, m * TQ : (m + 1) * TQ, :] = conv[:, 128:256]
        for one in conv_sends:
            one.start()

    convolve()

    up, down = ((y + 1) % 4) * 2 + c, ((y + 3) % 4) * 2 + c

    def ring(s, d):
        return copy_to(
            sbuf.at[s, d], rbuf.at[s, d], r_send.at[s, d], r_recv.at[s, d],
            sp, up if d == 0 else down,
        )

    def conv_ring(s):
        for d in range(2):
            chunk = (y + 3 - s) % 4 if d == 0 else (y + 1 + s) % 4
            first = d * HALF
            rows = jnp.concatenate([act[n, first : first + HALF, :] for n in range(4)], axis=1)
            part = jnp.dot(rows, wtc[chunk], preferred_element_type=F32)
            if s > 0:
                ring(s - 1, d).wait_recv()
                part = part + rbuf[s - 1, d].astype(F32)
            if s < 3:
                sbuf[s, d] = part.astype(BF16)
                ring(s, d).start()
            else:
                mixc[first : first + HALF, :] = part

    def step(i, carry):
        w, k = i // 4, i % 4
        plain = jnp.where(k < 2, c + 2 * k, 1 - c + 2 * (k - 2))
        last = jnp.where(k % 2 == 0, c, 1 - c) + 2 * (k // 2)
        u = jnp.where(w == 3, last, plain)
        blk = block_of(w, u)

        @pl.when((k == 3) & (w < 3))
        def _():
            exchange(w + 1)

        @pl.when(u % 2 != c)
        def _():
            arrived(blk)

        @pl.when(i == 3)
        def _():
            for n in range(7):
                pair_out[4 + n].wait_recv()
                zcopies[n].start()

        for s, when in enumerate((1, 7, 12)):

            @pl.when(i == when)
            def _():
                if s == 0:
                    for one in own_out:
                        one.wait()
                    for one in pair_out[:4] + conv_sends:
                        one.wait_recv()
                conv_ring(s)

        @pl.when(i == NB - 2)
        def _():
            finish(0)

        def for_queries(qb, carry):
            q_blk = jnp.where(qb == 0, own_pair, 15 - own_pair)

            @pl.when(blk < q_blk)
            def _():
                unit(qb, blk, False)

            @pl.when(blk == q_blk)
            def _():
                unit(qb, blk, True)

            return carry

        lax.fori_loop(0, 2, for_queries, 0)
        return carry

    lax.fori_loop(0, NB, step, 0)

    finish(1)

    conv_ring(3)

    def piece(head):
        return act.at[4 + head]

    def o_arrived(head):
        partner(piece(head), piece(head), f_send.at[0], o_recv.at[head]).wait_recv()

    forwards = []

    def pass_on(head, target):
        one = copy_to(piece(head), piece(head), f_send.at[len(forwards)], o_recv.at[head], sp, target)
        one.start()
        forwards.append(one)

    beside = y * 2 + (1 - c)
    mine = [y * 4 + 2 * c + e for e in range(2)]
    below = [((y + 3) % 4) * 4 + 2 * c + e for e in range(2)]
    above = [((y + 1) % 4) * 4 + 2 * c + e for e in range(2)]
    across = [((y + 2) % 4) * 4 + 2 * c + e for e in range(2)]
    here = (sp == own_pair) | (sp == 15 - own_pair)
    unless((2 * c == z) & here, lambda: o_arrived(mine[0]))
    pass_on(mine[0], up)
    unless((2 * c + 1 == z) & here, lambda: o_arrived(mine[1]))
    pass_on(mine[1], down)
    pass_on(mine[1], up)
    pass_on(mine[0], down)
    pass_on(mine[0], beside)
    pass_on(mine[1], beside)
    o_arrived(below[0])
    pass_on(below[0], up)
    o_arrived(above[1])
    pass_on(above[1], down)
    pass_on(below[0], beside)
    pass_on(above[1], beside)
    for head in (below[1], above[0], across[0], across[1]):
        o_arrived(head)
        pass_on(head, beside)
    for one in zcopies:
        one.wait_recv()
    for n in (0, 1, 3, 2):
        for e in range(2):
            o_arrived(((y + n) % 4) * 4 + 2 * (1 - c) + e)
    for n in range(4):
        first = n * PR
        rows = jnp.concatenate([act[4 + h, first : first + PR, :] for h in range(16)], axis=1)
        part = jnp.dot(rows, wta[...].reshape(2048, 512), preferred_element_type=F32)
        mix[first : first + PR, :] = (part + mixc[first : first + PR, :]).astype(BF16)

    ones_row = jnp.ones((8, 512), BF16)
    dims = (((1,), (1,)), ((), ()))
    m = mix[...]
    square = m.astype(F32) * m.astype(F32)
    high = square.astype(BF16)
    low = (square - high.astype(F32)).astype(BF16)
    total = lax.dot_general(ones_row, m, dims, preferred_element_type=F32)
    squares = lax.dot_general(ones_row, high, dims, preferred_element_type=F32)
    squares = squares + lax.dot_general(ones_row, low, dims, preferred_element_type=F32)
    row = lax.broadcasted_iota(jnp.int32, (8, TB), 0)
    stats[tp] = jnp.where(row == 0, total, squares)

    def tell(i):
        return copy_to(stats.at[tp], stats.at[tp], t_send.at[i - 1], t_recv.at[i - 1], sp, (tp + i) % 8)

    for i in range(1, 8):
        tell(i).start()
    for i in range(1, 8):
        tell(i).wait_recv()
    everything = stats[0]
    for n in range(1, 8):
        everything = everything + stats[n]
    columns = everything.T
    ogain = ogain_ref[pl.ds(pl.multiple_of(tp * 512, 512), 512)].astype(F32).reshape(1, 512)
    mean = columns[:, 0:1] * (1.0 / D)
    variance = columns[:, 1:2] * (1.0 / D) - mean * mean
    out_ref[...] = (
        (mix[...].astype(F32) - mean) * lax.rsqrt(variance + 1e-05) * ogain
    ).astype(BF16)


    for e in range(2):
        unless(kv_same(e), lambda: key_first(e).wait_send())
        unless(kv_same(e), lambda: value_first(e).wait_send())
        unless(q_same(e), lambda: query_first(e).wait_send())
        unless(q_same(e), lambda: lam_first(e).wait_send())
        unless(out_same(q_blks[e]), lambda: out_copy(e).wait_send())

    @pl.when(sp < 15)
    def _():
        halo_copy.wait_send()

    for n in range(3):
        k_copy(0, rk_send, n, right, c).wait_send()
        v_copy(0, rv_send, n, right, c).wait_send()
        k_copy(0, lk_send, n, left, c).wait_send()
        v_copy(0, lv_send, n, left, c).wait_send()
    for n in range(8):
        k_copy(0, dk_send, n, x, 1 - c).wait_send()
        v_copy(0, dv_send, n, x, 1 - c).wait_send()
    for one in pair_out + zcopies + conv_sends + forwards:
        one.wait_send()
    for s in range(3):
        for d in range(2):
            ring(s, d).wait_send()
    for i in range(1, 8):
        tell(i).wait_send()


def mixer(*arrays):
    dma = pltpu.SemaphoreType.DMA
    hbm = pl.BlockSpec(memory_space=pl.ANY)
    vmem = pl.BlockSpec(memory_space=pltpu.VMEM)
    return pl.pallas_call(
        mixer_kernel,
        out_shape=jax.ShapeDtypeStruct((TB, 512), BF16),
        in_specs=[hbm] * 9 + [pl.BlockSpec(memory_space=pltpu.SMEM)] + [vmem] * 4,
        out_specs=vmem,
        scratch_shapes=[
            pltpu.VMEM((NT, TQ, D), BF16),
            pltpu.VMEM((6, D, 256), BF16),
            pltpu.VMEM((2, TB, 128), BF16),
            pltpu.VMEM((2, 128, TB), BF16),
            pltpu.VMEM((2, 128, TB), BF16),
            pltpu.VMEM((2, 8, 128), F32),
            pltpu.VMEM((TB + 8, 256), F32),
            pltpu.VMEM((16, D), BF16),
            pltpu.VMEM((NT, TQ, 256), BF16),
            pltpu.VMEM((NB, TB, 128), BF16),
            pltpu.VMEM((NB, VA, TB), BF16),
            pltpu.VMEM((2, 128, TB), BF16),
            pltpu.VMEM((2 * NT, 128, 2 * TQ), BF16),
            pltpu.VMEM((2, 8, 128), F32),
            pltpu.VMEM((TB, 2 * TQ), F32),
            pltpu.VMEM((TB, 2 * TQ), F32),
            pltpu.VMEM((TB, 2 * TQ), F32),
            pltpu.VMEM((2 * NT, VA, 2 * TQ), F32),
            pltpu.VMEM((2 * NT, 1, 2 * TQ), F32),
            pltpu.VMEM((2, TB, 128), BF16),
            pltpu.VMEM((20, TB, 128), BF16),
            pltpu.VMEM((4, 512, 512), BF16),
            pltpu.VMEM((8, 256, 512), BF16),
            pltpu.VMEM((3, 2, HALF, 512), BF16),
            pltpu.VMEM((3, 2, HALF, 512), BF16),
            pltpu.VMEM((TB, 512), F32),
            pltpu.VMEM((TB, 512), BF16),
            pltpu.VMEM((8, 8, TB), F32),
            dma((NT,)), dma((6,)), dma((4,)), dma((4,)), dma((4,)), dma, dma((7,)), dma((7,)), dma((7,)), dma((7,)), dma, dma,
            dma((NB,)), dma((NB,)), dma((2,)), dma((2,)), dma((16,)),
            dma((2,)), dma((2,)), dma((2,)), dma((2,)),
            dma((3,)), dma((3,)), dma((3,)), dma((3,)),
            dma((8,)), dma((8,)), dma((2,)),
            dma((2,)), dma((2,)), dma((14,)),
            dma((3, 2)), dma((3, 2)), dma((7,)), dma((7,)),
        ],
        compiler_params=pltpu.CompilerParams(
            collective_id=0, has_side_effects=True, vmem_limit_bytes=67043328
        ),
        name="mixer",
    )(*arrays)


def per_device(
    hidden_states,
    w_conv_b,
    w_conv_c,
    w_conv_h,
    conv_taps,
    w_query,
    w_key,
    w_value,
    lambdas,
    head_gain,
    w_out_conv,
    w_out_attn,
    out_gain,
):
    first = lax.axis_index("sp") * TB
    positions = (first + jnp.arange(TB, dtype=jnp.int32)).astype(F32).reshape(NT, 1, TQ)
    inverse = 1.0 / 10000.0 ** (jnp.arange(0, QK, 2, dtype=F32) / QK)
    angles = positions * inverse[None, :, None]
    table = jnp.stack([jnp.cos(angles), jnp.sin(angles)])
    return mixer(
        hidden_states, w_key, w_value, w_query, w_conv_b, w_conv_c, w_conv_h,
        w_out_conv, w_out_attn,
        lambdas,
        head_gain,
        table,
        conv_taps,
        out_gain,
    )


def solution(mesh):
    return jax.shard_map(
        per_device,
        mesh=mesh,
        in_specs=(
            P("sp", None),
            P(None, "tp"),
            P(None, "tp"),
            P(None, "tp"),
            P(None, "tp"),
            P(None, "tp"),
            P(None, "tp"),
            P(None, "tp"),
            P("tp"),
            P(),
            P("tp", None),
            P("tp", None),
            P(),
        ),
        out_specs=P("sp", "tp"),
        check_vma=False,
    )
```

```python
import jax
import jax.numpy as jnp
from jax import lax
from jax.experimental import pallas as pl
from jax.experimental.pallas import tpu as pltpu
from jax.sharding import PartitionSpec as P

D = 4096
QK = 64
TAPS = 3
TB = 768
NB = 16
TQ = 256
NT = TB // TQ
VA = 144
HALF = TB // 2
PR = HALF // 2
LOG2E = 1.4426950408889634
NEG_LARGE = -1e30
BF16 = jnp.bfloat16
F32 = jnp.float32


def mixer_kernel(
    hid_in, wk_in, wv_in, wq_in, wb_in, wc_in, wh_in, oc_in, oa_in,
    lam_ref, hgain_ref, cs_ref, taps_ref, ogain_ref,
    out_ref,
    hid, wp, k_own, v_own, q_src, lam_in, gated, halo, u_b,
    k_all, v_all, q_own, qa, lam_own, s0, s1, s2, acc, m_ref, o_stage,
    act, wtc, wta, sbuf, rbuf, mixc, total_mix, mix, stats,
    h_sem, w_sem, ow_sem, ow_send, ow_recv, aw_sem, aw_send, aw_recv, zw_send, zw_recv, halo_send, halo_recv,
    k_recv, v_recv, q_recv, l_recv, o_recv,
    q_send, l_send, p1k_send, p1v_send, rk_send, rv_send, lk_send, lv_send,
    dk_send, dv_send, o_send,
    c_send, c_recv, f_send, r_send, r_recv, t_send, t_recv,
):
    sp = lax.axis_index("sp")
    tp = lax.axis_index("tp")
    z, x = sp // 4, sp % 4
    y, c = tp // 2, tp % 2
    own_pair = jnp.where(z < 2, x, 3 - x) + 4 * c
    left, right = (x + 3) % 4, (x + 1) % 4

    def copy_to(src, dst, send_sem, recv_sem, at_sp, at_tp):
        return pltpu.make_async_remote_copy(
            src_ref=src, dst_ref=dst, send_sem=send_sem, recv_sem=recv_sem,
            device_id={"sp": at_sp, "tp": at_tp}, device_id_type=pl.DeviceIdType.MESH,
        )

    def remote(src, dst, send_sem, recv_sem, zz, xx, cc):
        return copy_to(src, dst, send_sem, recv_sem, zz * 4 + xx, y * 2 + cc)

    def partner(src, dst, send_sem, recv_sem):
        return copy_to(src, dst, send_sem, recv_sem, sp, y * 2 + (1 - c))

    loads = [pltpu.make_async_copy(wk_in, wp.at[0], w_sem.at[0])]
    for m in range(NT):
        loads.append(pltpu.make_async_copy(hid_in.at[m * TQ : (m + 1) * TQ], hid.at[m], h_sem.at[m]))
    for n, w_in in enumerate((wv_in, wq_in, wc_in, wh_in, wb_in)):
        loads.append(pltpu.make_async_copy(w_in, wp.at[n + 1], w_sem.at[n + 1]))
    own_out, pair_out = [], []
    for chunk in range(4):
        dst = wtc.at[chunk, pl.ds(c * 256, 256)]
        own = oc_in.at[:, pl.ds(chunk * 1024 + c * 512, 512)]
        theirs = oc_in.at[:, pl.ds(chunk * 1024 + (1 - c) * 512, 512)]
        own_out.append(pltpu.make_async_copy(own, dst, ow_sem.at[chunk]))
        pair_out.append(partner(theirs, dst, ow_send.at[chunk], ow_recv.at[chunk]))
    own_out.append(pltpu.make_async_copy(oa_in.at[:, pl.ds(tp * 512, 512)], wta.at[tp], aw_sem))
    half = pl.ds((z % 2) * 128, 128)
    near_z = z + 1 - 2 * (z % 2)
    zcopies = []
    for i in range(1, 8):
        other = (tp + i) % 8
        pair_out.append(copy_to(
            oa_in.at[half, pl.ds(other * 512, 512)], wta.at[tp, half], aw_send.at[i - 1], aw_recv.at[i - 1], sp, other
        ))
        piece_of = wta.at[(tp + 8 - i) % 8, half]
        zcopies.append(remote(piece_of, piece_of, zw_send.at[i - 1], zw_recv.at[i - 1], near_z, x, c))
    halo_copy = copy_to(
        hid_in.at[pl.ds(TB - 16, 16)], halo, halo_send, halo_recv, (sp + 1) % 16, tp
    )
    for one in loads[:4]:
        one.start()

    barrier = pltpu.get_barrier_semaphore()
    me = sp * 2 + c

    def greet_plane(i, carry):
        other = (me + i) % 32
        pl.semaphore_signal(
            barrier, inc=1, device_id={"sp": other // 2, "tp": y * 2 + other % 2},
            device_id_type=pl.DeviceIdType.MESH,
        )
        return carry

    def greet_column(i, carry):
        pl.semaphore_signal(
            barrier, inc=1, device_id={"sp": sp, "tp": ((y + 1) * 2 + i) % 8},
            device_id_type=pl.DeviceIdType.MESH,
        )
        return carry

    pair_of_sp = jnp.where(sp < 8, sp, 15 - sp)
    slot_of_sp = jnp.where(sp < 8, 0, 1)
    pair_col = jnp.where(c == 0, pair_of_sp % 4, 3 - pair_of_sp % 4)
    q_blks = (own_pair, 15 - own_pair)
    lax.fori_loop(1, 32, greet_plane, 0)
    lax.fori_loop(0, 6, greet_column, 0)

    def project(m, n):
        r = jnp.dot(hid[m], wp[n], preferred_element_type=F32)
        return r.astype(BF16).astype(F32)

    def rotated(t, m, scale):
        cos, sin = cs_ref[0, m], cs_ref[1, m]
        if scale is not None:
            cos, sin = cos * scale, sin * scale
        parts = []
        for g in range(4):
            a, b = t[g * 64 : g * 64 + 32], t[g * 64 + 32 : g * 64 + 64]
            parts += [a * cos - b * sin, b * cos + a * sin]
        return jnp.concatenate(parts, axis=0)

    for e in range(2):
        lam_in[e] = jnp.full((8, 128), lam_ref[e], F32)

    loads[0].wait()
    for one in loads[4:6]:
        one.start()

    def key_rows(m, carry):
        pltpu.make_async_copy(hid_in.at[0:TQ], hid.at[m], h_sem.at[m]).wait()
        r = rotated(project(m, 0).T, m, None).T.astype(BF16)
        rows = pl.ds(pl.multiple_of(m * TQ, TQ), TQ)
        k_own[0, rows, :] = r[:, 0:128]
        k_own[1, rows, :] = r[:, 128:256]
        return carry

    lax.fori_loop(0, NT, key_rows, 0)
    for one in loads[6:]:
        one.start()
    pl.semaphore_wait(barrier, 37)

    @pl.when(sp < 15)
    def _():
        halo_copy.start()


    def kv_same(e):
        return (2 * c + e == z) & (z % 2 == c)

    def q_same(e):
        return (2 * c + e == z) & (pair_col == x) & (pair_of_sp // 4 == c)

    def key_first(e):
        return remote(k_own.at[e], k_all.at[sp], p1k_send.at[e], k_recv.at[sp], 2 * c + e, x, z % 2)

    def value_first(e):
        return remote(v_own.at[e], v_all.at[sp, pl.ds(0, 128)], p1v_send.at[e], v_recv.at[sp], 2 * c + e, x, z % 2)

    def query_first(e):
        return remote(q_src.at[e], q_own.at[slot_of_sp], q_send.at[e], q_recv.at[slot_of_sp], 2 * c + e, pair_col, pair_of_sp // 4)

    def lam_first(e):
        return remote(lam_in.at[e], lam_own.at[slot_of_sp], l_send.at[e], l_recv.at[slot_of_sp], 2 * c + e, pair_col, pair_of_sp // 4)

    def unless(same, action):
        @pl.when(jnp.logical_not(same))
        def _():
            action()

    def k_copy(blk, sems, n, xx, cc):
        return remote(k_all.at[blk], k_all.at[blk], sems.at[n], k_recv.at[blk], z, xx, cc)

    def v_copy(blk, sems, n, xx, cc):
        part = v_all.at[blk, pl.ds(0, 128)]
        return remote(part, part, sems.at[n], v_recv.at[blk], z, xx, cc)

    def block_of(w, u):
        side = jnp.where(u < 2, left, right)
        col = jnp.where(w == 0, x, jnp.where(w == 3, (x + 2) % 4, side))
        row = jnp.where(w == 2, (u + 2) % 4, u)
        return row * 4 + col

    def k_arrived(blk):
        k_copy(blk, dk_send, 0, x, 1 - c).wait_recv()

    def v_arrived(blk):
        v_copy(blk, dv_send, 0, x, 1 - c).wait_recv()

    def arrived(blk):
        k_arrived(blk)
        v_arrived(blk)

    def pass_right(blk, n):
        k_copy(blk, rk_send, n, right, c).start()
        v_copy(blk, rv_send, n, right, c).start()

    def pass_left(blk, n):
        k_copy(blk, lk_send, n, left, c).start()
        v_copy(blk, lv_send, n, left, c).start()

    def pass_partner(blk, n):
        k_copy(blk, dk_send, n, x, 1 - c).start()
        v_copy(blk, dv_send, n, x, 1 - c).start()

    low, high = c * 4 + x, (c + 2) * 4 + x
    near = z % 2 == c

    def send_low(copy, rights, lefts, partners):
        copy(low, rights, 0, right, c).start()
        copy(low, lefts, 1, left, c).start()
        copy(low, partners, 0, x, 1 - c).start()

    def send_high(copy, rights, lefts, partners):
        copy(high, lefts, 0, left, c).start()
        copy(high, rights, 1, right, c).start()
        copy(high, partners, 1, x, 1 - c).start()

    def start_own(copy, here, rights, lefts, partners):
        @pl.when(near)
        def _():
            unless(z // 2 == c, lambda: here(sp))

            @pl.when(z < 2)
            def _():
                send_low(copy, rights, lefts, partners)

            @pl.when(z >= 2)
            def _():
                send_high(copy, rights, lefts, partners)

    def start_rest(copy, here, rights, lefts, partners):
        @pl.when(jnp.logical_not(near & (z < 2)))
        def _():
            here(low)
            send_low(copy, rights, lefts, partners)

        @pl.when(jnp.logical_not(near & (z >= 2)))
        def _():
            here(high)
            send_high(copy, rights, lefts, partners)

    k_ring = (k_copy, k_arrived, rk_send, lk_send, dk_send)
    v_ring = (v_copy, v_arrived, rv_send, lv_send, dv_send)

    for e in range(2):
        unless(kv_same(e), lambda: key_first(e).start())

        @pl.when(kv_same(e))
        def _():
            k_all[sp] = k_own[e]

    for one in own_out + pair_out:
        one.start()

    def column(m):
        return pl.ds(pl.multiple_of(m * TQ, TQ), TQ)

    loads[4].wait()

    def value_rows(m, carry):
        r = project(m, 1).T.astype(BF16)
        v_own[0, :, column(m)] = r[0:128]
        v_own[1, :, column(m)] = r[128:256]
        return carry

    lax.fori_loop(0, NT, value_rows, 0)
    for e in range(2):
        unless(kv_same(e), lambda: value_first(e).start())

        @pl.when(kv_same(e))
        def _():
            v_all[sp, 0:128, :] = v_own[e]

    start_own(*k_ring)

    loads[5].wait()

    def query_rows(m, carry):
        r = rotated(project(m, 2).T, m, LOG2E * QK ** (-0.5)).astype(BF16)
        q_src[0, :, column(m)] = r[0:128]
        q_src[1, :, column(m)] = r[128:256]
        return carry

    lax.fori_loop(0, NT, query_rows, 0)
    for e in range(2):
        unless(q_same(e), lambda: query_first(e).start())
        unless(q_same(e), lambda: lam_first(e).start())

        @pl.when(q_same(e))
        def _():
            q_own[slot_of_sp] = q_src[e]
            lam_own[slot_of_sp] = lam_in[e]

    start_own(*v_ring)

    loads[6].wait()

    def gated_rows(m, carry):
        rows = pl.ds(pl.multiple_of(8 + m * TQ, 8), TQ)
        gated[rows, :] = gated[rows, :] * project(m, 4)
        return carry

    def inner_rows(m, carry):
        gated[pl.ds(pl.multiple_of(8 + m * TQ, 8), TQ), :] = project(m, 3)
        return carry

    lax.fori_loop(0, NT, inner_rows, 0)
    loads[7].wait()
    lax.fori_loop(0, NT, gated_rows, 0)
    start_rest(*k_ring)
    loads[8].wait()

    def gate_rows(m, carry):
        u_b[m] = jnp.dot(hid[m], wp[5], preferred_element_type=F32).astype(BF16)
        return carry

    lax.fori_loop(0, NT, gate_rows, 0)

    def ones(j, carry):
        v_all[j, 128:VA, :] = jnp.ones((VA - 128, TB), BF16)
        return carry

    lax.fori_loop(0, NB, ones, 0)
    acc[...] = jnp.zeros(acc.shape, F32)
    m_ref[...] = jnp.full(m_ref.shape, NEG_LARGE, F32)
    start_rest(*v_ring)

    zero = jnp.zeros((QK, TQ), BF16)
    for qb in range(2):
        q_blk = own_pair if qb == 0 else 15 - own_pair
        same = (q_blk == sp) & (z // 2 == c)
        unless(same, lambda: remote(q_src.at[0], q_own.at[qb], q_send.at[0], q_recv.at[qb], z, x, 1 - c).wait_recv())
        unless(same, lambda: remote(lam_in.at[0], lam_own.at[qb], l_send.at[0], l_recv.at[qb], z, x, 1 - c).wait_recv())
        for t in range(NT):
            qt = q_own[qb, :, t * TQ : (t + 1) * TQ]
            qa[qb * NT + t, 0:QK, 0:TQ] = qt[0:QK]
            qa[qb * NT + t, QK:128, 0:TQ] = zero
            qa[qb * NT + t, 0:QK, TQ : 2 * TQ] = zero
            qa[qb * NT + t, QK:128, TQ : 2 * TQ] = qt[QK:128]

    scores = (s0, s1, s2)

    def unit(qb, j, diagonal):
        tops = [None] * NT

        def produce(t):
            rows = TQ * (t + 1) if diagonal else TB
            s = jnp.dot(k_all[j, 0:rows, :], qa[qb * NT + t], preferred_element_type=F32)
            if diagonal:
                key = lax.broadcasted_iota(jnp.int32, (rows, 2 * TQ), 0)
                query = lax.broadcasted_iota(jnp.int32, (rows, 2 * TQ), 1)
                query = jnp.where(query >= TQ, query - TQ, query) + t * TQ
                s = jnp.where(key <= query, s, NEG_LARGE)
            scores[t][0:rows, :] = s
            tops[t] = jnp.max(s, axis=0, keepdims=True)

        def consume(t):
            rows = TQ * (t + 1) if diagonal else TB
            at = qb * NT + t
            before = m_ref[at]
            after = jnp.maximum(before, tops[t])
            w = jnp.exp2(scores[t][0:rows, :] - after).astype(BF16)
            factor = jnp.exp2(before - after)
            acc[at] = acc[at] * factor + jnp.dot(
                v_all[j, :, 0:rows], w, preferred_element_type=F32
            )
            m_ref[at] = after

        produce(0)
        produce(1)
        consume(0)
        produce(2)
        consume(1)
        consume(2)

    def exchange(w):
        from_left, from_right = block_of(w, c), block_of(w, c + 2)
        arrived(from_left)

        @pl.when(w == 1)
        def _():
            pass_right(from_left, 2)

        pass_partner(from_left, 2 * w)
        arrived(from_right)

        @pl.when(w == 1)
        def _():
            pass_left(from_right, 2)

        pass_partner(from_right, 2 * w + 1)

    def out_same(q_blk):
        return (q_blk == sp) & (z // 2 == c)

    def out_copy(qb):
        return remote(
            o_stage.at[qb], act.at[4 + y * 4 + z], o_send.at[qb], o_recv.at[y * 4 + z],
            q_blks[qb] // 4, q_blks[qb] % 4, z // 2,
        )

    def finish(qb):
        hgain = jnp.broadcast_to(hgain_ref[...].astype(F32).reshape(1, 128), (8, 128)).T[:, 0:1]
        lam = lam_own[qb, 0:1, 0:1]
        for t in range(NT):
            at = qb * NT + t
            n1 = acc[at, 0:128, 0:TQ] / acc[at, 128:129, 0:TQ]
            n2 = acc[at, 0:128, TQ : 2 * TQ] / acc[at, 128:129, TQ : 2 * TQ]
            diff = n1 - lam * n2
            mean = jnp.mean(diff * diff, axis=0, keepdims=True)
            normed = diff * lax.rsqrt(mean + 1e-05) * hgain
            o_stage[qb, t * TQ : (t + 1) * TQ, :] = normed.T.astype(BF16)
        unless(out_same(q_blks[qb]), lambda: out_copy(qb).start())

        @pl.when(out_same(q_blks[qb]))
        def _():
            act[4 + y * 4 + z] = o_stage[qb]

    conv_sends = []
    for n in range(2):
        piece = act.at[2 * c + n]
        conv_sends.append(partner(piece, piece, c_send.at[n], c_recv.at[n]))

    def convolve():
        @pl.when(sp > 0)
        def _():
            halo_copy.wait_recv()
            inner = jnp.dot(halo[...], wp[3], preferred_element_type=F32).astype(BF16)
            outer = jnp.dot(halo[...], wp[4], preferred_element_type=F32).astype(BF16)
            gated[0:8, :] = inner[8:16].astype(F32) * outer[8:16].astype(F32)

        @pl.when(sp == 0)
        def _():
            gated[0:8, :] = jnp.zeros((8, 256), F32)

        taps = taps_ref[...].astype(F32)
        for m in range(NT):
            total = jnp.zeros((TQ, 256), F32)
            for tap in range(TAPS):
                first = 8 + m * TQ - (TAPS - 1) + tap
                total = total + taps[tap : tap + 1, :] * gated[first : first + TQ, :]
            conv = (u_b[m].astype(F32) * total).astype(BF16)
            act[2 * c, m * TQ : (m + 1) * TQ, :] = conv[:, 0:128]
            act[2 * c + 1, m * TQ : (m + 1) * TQ, :] = conv[:, 128:256]
        for one in conv_sends:
            one.start()

    convolve()

    up, down = ((y + 1) % 4) * 2 + c, ((y + 3) % 4) * 2 + c

    def ring(s, d):
        return copy_to(
            sbuf.at[s, d], rbuf.at[s, d], r_send.at[s, d], r_recv.at[s, d],
            sp, up if d == 0 else down,
        )

    def conv_ring(s):
        for d in range(2):
            chunk = (y + 3 - s) % 4 if d == 0 else (y + 1 + s) % 4
            first = d * HALF
            rows = jnp.concatenate([act[n, first : first + HALF, :] for n in range(4)], axis=1)
            part = jnp.dot(rows, wtc[chunk], preferred_element_type=F32)
            if s > 0:
                ring(s - 1, d).wait_recv()
                part = part + rbuf[s - 1, d].astype(F32)
            if s < 3:
                sbuf[s, d] = part.astype(BF16)
                ring(s, d).start()
            else:
                mixc[first : first + HALF, :] = part

    def step(i, carry):
        w, k = i // 4, i % 4
        plain = jnp.where(k < 2, c + 2 * k, 1 - c + 2 * (k - 2))
        last = jnp.where(k % 2 == 0, c, 1 - c) + 2 * (k // 2)
        u = jnp.where(w == 3, last, plain)
        blk = block_of(w, u)

        @pl.when(i == 4)
        def _():
            exchange(1)

        @pl.when((k == 3) & (0 < w) & (w < 3))
        def _():
            exchange(w + 1)

        @pl.when(u % 2 != c)
        def _():
            arrived(blk)

        @pl.when(i == 3)
        def _():
            for n in range(7):
                pair_out[4 + n].wait_recv()
                zcopies[n].start()

        for s, when in enumerate((1, 8, 14)):

            @pl.when(i == when)
            def _():
                if s == 0:
                    for one in own_out:
                        one.wait()
                    for one in pair_out[:4] + conv_sends:
                        one.wait_recv()
                conv_ring(s)

        @pl.when(i == NB - 2)
        def _():
            finish(0)

        def for_queries(qb, carry):
            q_blk = jnp.where(qb == 0, own_pair, 15 - own_pair)

            @pl.when(blk < q_blk)
            def _():
                unit(qb, blk, False)

            @pl.when(blk == q_blk)
            def _():
                unit(qb, blk, True)

            return carry

        lax.fori_loop(0, 2, for_queries, 0)
        return carry

    lax.fori_loop(0, NB, step, 0)

    finish(1)

    def piece(head):
        return act.at[4 + head]

    def o_arrived(head):
        partner(piece(head), piece(head), f_send.at[0], o_recv.at[head]).wait_recv()

    forwards = []

    def pass_on(head, target):
        one = copy_to(piece(head), piece(head), f_send.at[len(forwards)], o_recv.at[head], sp, target)
        one.start()
        forwards.append(one)

    beside = y * 2 + (1 - c)
    mine = [y * 4 + 2 * c + e for e in range(2)]
    below = [((y + 3) % 4) * 4 + 2 * c + e for e in range(2)]
    above = [((y + 1) % 4) * 4 + 2 * c + e for e in range(2)]
    across = [((y + 2) % 4) * 4 + 2 * c + e for e in range(2)]
    here = (sp == own_pair) | (sp == 15 - own_pair)
    unless((2 * c == z) & here, lambda: o_arrived(mine[0]))
    pass_on(mine[0], up)
    unless((2 * c + 1 == z) & here, lambda: o_arrived(mine[1]))
    pass_on(mine[1], down)
    pass_on(mine[1], up)
    pass_on(mine[0], down)
    pass_on(mine[0], beside)
    pass_on(mine[1], beside)

    for one in zcopies:
        one.wait_recv()

    def add_plane(n):
        plane = (y + n) % 4
        weights = wta[pl.ds(plane * 2, 2)].reshape(512, 512)
        for r in range(3):
            at = slice(r * TQ, (r + 1) * TQ)
            rows = jnp.concatenate([act[4 + plane * 4 + h, at, :] for h in range(4)], axis=1)
            part = jnp.dot(rows, weights, preferred_element_type=F32)
            if n == 0:
                total_mix[at, :] = part
            elif n != 2:
                total_mix[at, :] += part
            else:
                part = part + total_mix[at, :] + mixc[at, :]
                mix[at, :] = part.astype(BF16)

    def from_partner(n):
        for e in range(2):
            o_arrived(((y + n) % 4) * 4 + 2 * (1 - c) + e)

    from_partner(0)
    add_plane(0)
    o_arrived(below[0])
    pass_on(below[0], up)
    o_arrived(above[1])
    pass_on(above[1], down)
    pass_on(below[0], beside)
    pass_on(above[1], beside)
    conv_ring(3)
    for head in (below[1], above[0]):
        o_arrived(head)
        pass_on(head, beside)
    for n in (3, 1):
        from_partner(n)
        add_plane(n)
    for head in across:
        o_arrived(head)
        pass_on(head, beside)
    from_partner(2)
    add_plane(2)

    ones_row = jnp.ones((8, 512), BF16)
    dims = (((1,), (1,)), ((), ()))
    m = mix[...]
    square = m.astype(F32) * m.astype(F32)
    high = square.astype(BF16)
    low = (square - high.astype(F32)).astype(BF16)
    total = lax.dot_general(ones_row, m, dims, preferred_element_type=F32)
    squares = lax.dot_general(ones_row, high, dims, preferred_element_type=F32)
    squares = squares + lax.dot_general(ones_row, low, dims, preferred_element_type=F32)
    row = lax.broadcasted_iota(jnp.int32, (8, TB), 0)
    stats[tp] = jnp.where(row == 0, total, squares)

    def tell(i):
        return copy_to(stats.at[tp], stats.at[tp], t_send.at[i - 1], t_recv.at[i - 1], sp, (tp + i) % 8)

    for i in range(1, 8):
        tell(i).start()
    for i in range(1, 8):
        tell(i).wait_recv()
    everything = stats[0]
    for n in range(1, 8):
        everything = everything + stats[n]
    columns = everything.T
    ogain = ogain_ref[pl.ds(pl.multiple_of(tp * 512, 512), 512)].astype(F32).reshape(1, 512)
    mean = columns[:, 0:1] * (1.0 / D)
    variance = columns[:, 1:2] * (1.0 / D) - mean * mean
    out_ref[...] = (
        (mix[...].astype(F32) - mean) * lax.rsqrt(variance + 1e-05) * ogain
    ).astype(BF16)


    for e in range(2):
        unless(kv_same(e), lambda: key_first(e).wait_send())
        unless(kv_same(e), lambda: value_first(e).wait_send())
        unless(q_same(e), lambda: query_first(e).wait_send())
        unless(q_same(e), lambda: lam_first(e).wait_send())
        unless(out_same(q_blks[e]), lambda: out_copy(e).wait_send())

    @pl.when(sp < 15)
    def _():
        halo_copy.wait_send()

    for n in range(3):
        k_copy(0, rk_send, n, right, c).wait_send()
        v_copy(0, rv_send, n, right, c).wait_send()
        k_copy(0, lk_send, n, left, c).wait_send()
        v_copy(0, lv_send, n, left, c).wait_send()
    for n in range(8):
        k_copy(0, dk_send, n, x, 1 - c).wait_send()
        v_copy(0, dv_send, n, x, 1 - c).wait_send()
    for one in pair_out + zcopies + conv_sends + forwards:
        one.wait_send()
    for s in range(3):
        for d in range(2):
            ring(s, d).wait_send()
    for i in range(1, 8):
        tell(i).wait_send()


def mixer(*arrays):
    dma = pltpu.SemaphoreType.DMA
    hbm = pl.BlockSpec(memory_space=pl.ANY)
    vmem = pl.BlockSpec(memory_space=pltpu.VMEM)
    return pl.pallas_call(
        mixer_kernel,
        out_shape=jax.ShapeDtypeStruct((TB, 512), BF16),
        in_specs=[hbm] * 9 + [pl.BlockSpec(memory_space=pltpu.SMEM)] + [vmem] * 4,
        out_specs=vmem,
        scratch_shapes=[
            pltpu.VMEM((NT, TQ, D), BF16),
            pltpu.VMEM((6, D, 256), BF16),
            pltpu.VMEM((2, TB, 128), BF16),
            pltpu.VMEM((2, 128, TB), BF16),
            pltpu.VMEM((2, 128, TB), BF16),
            pltpu.VMEM((2, 8, 128), F32),
            pltpu.VMEM((TB + 8, 256), F32),
            pltpu.VMEM((16, D), BF16),
            pltpu.VMEM((NT, TQ, 256), BF16),
            pltpu.VMEM((NB, TB, 128), BF16),
            pltpu.VMEM((NB, VA, TB), BF16),
            pltpu.VMEM((2, 128, TB), BF16),
            pltpu.VMEM((2 * NT, 128, 2 * TQ), BF16),
            pltpu.VMEM((2, 8, 128), F32),
            pltpu.VMEM((TB, 2 * TQ), F32),
            pltpu.VMEM((TB, 2 * TQ), F32),
            pltpu.VMEM((TB, 2 * TQ), F32),
            pltpu.VMEM((2 * NT, VA, 2 * TQ), F32),
            pltpu.VMEM((2 * NT, 1, 2 * TQ), F32),
            pltpu.VMEM((2, TB, 128), BF16),
            pltpu.VMEM((20, TB, 128), BF16),
            pltpu.VMEM((4, 512, 512), BF16),
            pltpu.VMEM((8, 256, 512), BF16),
            pltpu.VMEM((3, 2, HALF, 512), BF16),
            pltpu.VMEM((3, 2, HALF, 512), BF16),
            pltpu.VMEM((TB, 512), F32),
            pltpu.VMEM((TB, 512), F32),
            pltpu.VMEM((TB, 512), BF16),
            pltpu.VMEM((8, 8, TB), F32),
            dma((NT,)), dma((6,)), dma((4,)), dma((4,)), dma((4,)), dma, dma((7,)), dma((7,)), dma((7,)), dma((7,)), dma, dma,
            dma((NB,)), dma((NB,)), dma((2,)), dma((2,)), dma((16,)),
            dma((2,)), dma((2,)), dma((2,)), dma((2,)),
            dma((3,)), dma((3,)), dma((3,)), dma((3,)),
            dma((8,)), dma((8,)), dma((2,)),
            dma((2,)), dma((2,)), dma((14,)),
            dma((3, 2)), dma((3, 2)), dma((7,)), dma((7,)),
        ],
        compiler_params=pltpu.CompilerParams(
            collective_id=0, has_side_effects=True, vmem_limit_bytes=67043328
        ),
        name="mixer",
    )(*arrays)


def per_device(
    hidden_states,
    w_conv_b,
    w_conv_c,
    w_conv_h,
    conv_taps,
    w_query,
    w_key,
    w_value,
    lambdas,
    head_gain,
    w_out_conv,
    w_out_attn,
    out_gain,
):
    first = lax.axis_index("sp") * TB
    positions = (first + jnp.arange(TB, dtype=jnp.int32)).astype(F32).reshape(NT, 1, TQ)
    inverse = 1.0 / 10000.0 ** (jnp.arange(0, QK, 2, dtype=F32) / QK)
    angles = positions * inverse[None, :, None]
    table = jnp.stack([jnp.cos(angles), jnp.sin(angles)])
    return mixer(
        hidden_states, w_key, w_value, w_query, w_conv_b, w_conv_c, w_conv_h,
        w_out_conv, w_out_attn,
        lambdas,
        head_gain,
        table,
        conv_taps,
        out_gain,
    )


def solution(mesh):
    return jax.shard_map(
        per_device,
        mesh=mesh,
        in_specs=(
            P("sp", None),
            P(None, "tp"),
            P(None, "tp"),
            P(None, "tp"),
            P(None, "tp"),
            P(None, "tp"),
            P(None, "tp"),
            P(None, "tp"),
            P("tp"),
            P(),
            P("tp", None),
            P("tp", None),
            P(),
        ),
        out_specs=P("sp", "tp"),
        check_vma=False,
    )
```

```python
import jax
import jax.numpy as jnp
from jax import lax
from jax.experimental import pallas as pl
from jax.experimental.pallas import tpu as pltpu
from jax.sharding import PartitionSpec as P

D = 4096
QK = 64
TAPS = 3
TB = 768
NB = 16
TQ = 256
NT = TB // TQ
VA = 144
HALF = TB // 2
PR = HALF // 2
LOG2E = 1.4426950408889634
NEG_LARGE = -1e30
BF16 = jnp.bfloat16
F32 = jnp.float32


def mixer_kernel(
    hid_in, wk_in, wv_in, wq_in, wb_in, wc_in, wh_in, oc_in, oa_in,
    lam_ref, hgain_ref, cs_ref, taps_ref, ogain_ref,
    out_ref,
    hid, wp, k_own, v_own, q_src, lam_in, gated, halo, u_b,
    k_all, v_all, q_own, qa, lam_own, s0, s1, s2, acc, m_ref, o_stage,
    act, wtc, wta, sbuf, rbuf, mixc, total_mix, mix, stats,
    h_sem, w_sem, ow_sem, ow_send, ow_recv, aw_sem, aw_send, aw_recv, zw_send, zw_recv, halo_send, halo_recv,
    k_recv, v_recv, q_recv, l_recv, o_recv,
    q_send, l_send, p1k_send, p1v_send, rk_send, rv_send, lk_send, lv_send,
    dk_send, dv_send, o_send,
    c_send, c_recv, f_send, r_send, r_recv, t_send, t_recv,
):
    sp = lax.axis_index("sp")
    tp = lax.axis_index("tp")
    z, x = sp // 4, sp % 4
    y, c = tp // 2, tp % 2
    own_pair = jnp.where(z < 2, x, 3 - x) + 4 * c
    left, right = (x + 3) % 4, (x + 1) % 4

    def copy_to(src, dst, send_sem, recv_sem, at_sp, at_tp):
        return pltpu.make_async_remote_copy(
            src_ref=src, dst_ref=dst, send_sem=send_sem, recv_sem=recv_sem,
            device_id={"sp": at_sp, "tp": at_tp}, device_id_type=pl.DeviceIdType.MESH,
        )

    def remote(src, dst, send_sem, recv_sem, zz, xx, cc):
        return copy_to(src, dst, send_sem, recv_sem, zz * 4 + xx, y * 2 + cc)

    def partner(src, dst, send_sem, recv_sem):
        return copy_to(src, dst, send_sem, recv_sem, sp, y * 2 + (1 - c))

    loads = [pltpu.make_async_copy(wk_in, wp.at[0], w_sem.at[0])]
    for m in range(NT):
        loads.append(pltpu.make_async_copy(hid_in.at[m * TQ : (m + 1) * TQ], hid.at[m], h_sem.at[m]))
    for n, w_in in enumerate((wv_in, wq_in, wc_in, wh_in, wb_in)):
        loads.append(pltpu.make_async_copy(w_in, wp.at[n + 1], w_sem.at[n + 1]))
    own_out, pair_out = [], []
    for chunk in range(4):
        dst = wtc.at[chunk, pl.ds(c * 256, 256)]
        own = oc_in.at[:, pl.ds(chunk * 1024 + c * 512, 512)]
        theirs = oc_in.at[:, pl.ds(chunk * 1024 + (1 - c) * 512, 512)]
        own_out.append(pltpu.make_async_copy(own, dst, ow_sem.at[chunk]))
        pair_out.append(partner(theirs, dst, ow_send.at[chunk], ow_recv.at[chunk]))
    own_out.append(pltpu.make_async_copy(oa_in.at[:, pl.ds(tp * 512, 512)], wta.at[tp], aw_sem))
    half = pl.ds((z % 2) * 128, 128)
    near_z = z + 1 - 2 * (z % 2)
    zcopies = []
    for i in range(1, 8):
        other = (tp + i) % 8
        pair_out.append(copy_to(
            oa_in.at[half, pl.ds(other * 512, 512)], wta.at[tp, half], aw_send.at[i - 1], aw_recv.at[i - 1], sp, other
        ))
        piece_of = wta.at[(tp + 8 - i) % 8, half]
        zcopies.append(remote(piece_of, piece_of, zw_send.at[i - 1], zw_recv.at[i - 1], near_z, x, c))
    halo_copy = copy_to(
        hid_in.at[pl.ds(TB - 16, 16)], halo, halo_send, halo_recv, (sp + 1) % 16, tp
    )
    for one in loads[:4]:
        one.start()

    barrier = pltpu.get_barrier_semaphore()
    me = sp * 2 + c

    def greet_plane(i, carry):
        other = (me + i) % 32
        pl.semaphore_signal(
            barrier, inc=1, device_id={"sp": other // 2, "tp": y * 2 + other % 2},
            device_id_type=pl.DeviceIdType.MESH,
        )
        return carry

    def greet_column(i, carry):
        pl.semaphore_signal(
            barrier, inc=1, device_id={"sp": sp, "tp": ((y + 1) * 2 + i) % 8},
            device_id_type=pl.DeviceIdType.MESH,
        )
        return carry

    pair_of_sp = jnp.where(sp < 8, sp, 15 - sp)
    slot_of_sp = jnp.where(sp < 8, 0, 1)
    pair_col = jnp.where(c == 0, pair_of_sp % 4, 3 - pair_of_sp % 4)
    q_blks = (own_pair, 15 - own_pair)
    lax.fori_loop(1, 32, greet_plane, 0)
    lax.fori_loop(0, 6, greet_column, 0)

    def project(m, n):
        r = jnp.dot(hid[m], wp[n], preferred_element_type=F32)
        return r.astype(BF16).astype(F32)

    def rotated(t, m, scale):
        cos, sin = cs_ref[0, m], cs_ref[1, m]
        if scale is not None:
            cos, sin = cos * scale, sin * scale
        parts = []
        for g in range(4):
            a, b = t[g * 64 : g * 64 + 32], t[g * 64 + 32 : g * 64 + 64]
            parts += [a * cos - b * sin, b * cos + a * sin]
        return jnp.concatenate(parts, axis=0)

    for e in range(2):
        lam_in[e] = jnp.full((8, 128), lam_ref[e], F32)

    loads[0].wait()
    for one in loads[4:6]:
        one.start()

    def key_rows(m, carry):
        pltpu.make_async_copy(hid_in.at[0:TQ], hid.at[m], h_sem.at[m]).wait()
        r = rotated(project(m, 0).T, m, None).T.astype(BF16)
        rows = pl.ds(pl.multiple_of(m * TQ, TQ), TQ)
        k_own[0, rows, :] = r[:, 0:128]
        k_own[1, rows, :] = r[:, 128:256]
        return carry

    lax.fori_loop(0, NT, key_rows, 0)
    for one in loads[6:]:
        one.start()
    pl.semaphore_wait(barrier, 37)

    @pl.when(sp < 15)
    def _():
        halo_copy.start()


    def kv_same(e):
        return (2 * c + e == z) & (z % 2 == c)

    def q_same(e):
        return (2 * c + e == z) & (pair_col == x) & (pair_of_sp // 4 == c)

    def key_first(e):
        return remote(k_own.at[e], k_all.at[sp], p1k_send.at[e], k_recv.at[sp], 2 * c + e, x, z % 2)

    def value_first(e):
        return remote(v_own.at[e], v_all.at[sp, pl.ds(0, 128)], p1v_send.at[e], v_recv.at[sp], 2 * c + e, x, z % 2)

    def query_first(e):
        return remote(q_src.at[e], q_own.at[slot_of_sp], q_send.at[e], q_recv.at[slot_of_sp], 2 * c + e, pair_col, pair_of_sp // 4)

    def lam_first(e):
        return remote(lam_in.at[e], lam_own.at[slot_of_sp], l_send.at[e], l_recv.at[slot_of_sp], 2 * c + e, pair_col, pair_of_sp // 4)

    def unless(same, action):
        @pl.when(jnp.logical_not(same))
        def _():
            action()

    def k_copy(blk, sems, n, xx, cc):
        return remote(k_all.at[blk], k_all.at[blk], sems.at[n], k_recv.at[blk], z, xx, cc)

    def v_copy(blk, sems, n, xx, cc):
        part = v_all.at[blk, pl.ds(0, 128)]
        return remote(part, part, sems.at[n], v_recv.at[blk], z, xx, cc)

    def block_of(w, u):
        side = jnp.where(u < 2, left, right)
        col = jnp.where(w == 0, x, jnp.where(w == 3, (x + 2) % 4, side))
        row = jnp.where(w == 2, (u + 2) % 4, u)
        return row * 4 + col

    def k_arrived(blk):
        k_copy(blk, dk_send, 0, x, 1 - c).wait_recv()

    def v_arrived(blk):
        v_copy(blk, dv_send, 0, x, 1 - c).wait_recv()

    def arrived(blk):
        k_arrived(blk)
        v_arrived(blk)

    def pass_right(blk, n):
        k_copy(blk, rk_send, n, right, c).start()
        v_copy(blk, rv_send, n, right, c).start()

    def pass_left(blk, n):
        k_copy(blk, lk_send, n, left, c).start()
        v_copy(blk, lv_send, n, left, c).start()

    def pass_partner(blk, n):
        k_copy(blk, dk_send, n, x, 1 - c).start()
        v_copy(blk, dv_send, n, x, 1 - c).start()

    low, high = c * 4 + x, (c + 2) * 4 + x
    near = z % 2 == c

    def send_low(copy, rights, lefts, partners):
        copy(low, rights, 0, right, c).start()
        copy(low, lefts, 1, left, c).start()
        copy(low, partners, 0, x, 1 - c).start()

    def send_high(copy, rights, lefts, partners):
        copy(high, lefts, 0, left, c).start()
        copy(high, rights, 1, right, c).start()
        copy(high, partners, 1, x, 1 - c).start()

    def start_own(copy, here, rights, lefts, partners):
        @pl.when(near)
        def _():
            unless(z // 2 == c, lambda: here(sp))

            @pl.when(z < 2)
            def _():
                send_low(copy, rights, lefts, partners)

            @pl.when(z >= 2)
            def _():
                send_high(copy, rights, lefts, partners)

    def start_rest(copy, here, rights, lefts, partners):
        @pl.when(jnp.logical_not(near & (z < 2)))
        def _():
            here(low)
            send_low(copy, rights, lefts, partners)

        @pl.when(jnp.logical_not(near & (z >= 2)))
        def _():
            here(high)
            send_high(copy, rights, lefts, partners)

    k_ring = (k_copy, k_arrived, rk_send, lk_send, dk_send)
    v_ring = (v_copy, v_arrived, rv_send, lv_send, dv_send)

    for e in range(2):
        unless(kv_same(e), lambda: key_first(e).start())

        @pl.when(kv_same(e))
        def _():
            k_all[sp] = k_own[e]

    for one in own_out + pair_out:
        one.start()

    def column(m):
        return pl.ds(pl.multiple_of(m * TQ, TQ), TQ)

    loads[4].wait()

    def value_rows(m, carry):
        r = project(m, 1).T.astype(BF16)
        v_own[0, :, column(m)] = r[0:128]
        v_own[1, :, column(m)] = r[128:256]
        return carry

    lax.fori_loop(0, NT, value_rows, 0)
    for e in range(2):
        unless(kv_same(e), lambda: value_first(e).start())

        @pl.when(kv_same(e))
        def _():
            v_all[sp, 0:128, :] = v_own[e]

    start_own(*k_ring)

    loads[5].wait()

    def query_rows(m, carry):
        r = rotated(project(m, 2).T, m, LOG2E * QK ** (-0.5)).astype(BF16)
        q_src[0, :, column(m)] = r[0:128]
        q_src[1, :, column(m)] = r[128:256]
        return carry

    lax.fori_loop(0, NT, query_rows, 0)
    for e in range(2):
        unless(q_same(e), lambda: query_first(e).start())
        unless(q_same(e), lambda: lam_first(e).start())

        @pl.when(q_same(e))
        def _():
            q_own[slot_of_sp] = q_src[e]
            lam_own[slot_of_sp] = lam_in[e]

    start_own(*v_ring)

    loads[6].wait()

    def gated_rows(m, carry):
        rows = pl.ds(pl.multiple_of(8 + m * TQ, 8), TQ)
        gated[rows, :] = gated[rows, :] * project(m, 4)
        return carry

    def inner_rows(m, carry):
        gated[pl.ds(pl.multiple_of(8 + m * TQ, 8), TQ), :] = project(m, 3)
        return carry

    lax.fori_loop(0, NT, inner_rows, 0)
    loads[7].wait()
    lax.fori_loop(0, NT, gated_rows, 0)
    start_rest(*k_ring)
    loads[8].wait()

    def gate_rows(m, carry):
        u_b[m] = jnp.dot(hid[m], wp[5], preferred_element_type=F32).astype(BF16)
        return carry

    lax.fori_loop(0, NT, gate_rows, 0)

    def ones(j, carry):
        v_all[j, 128:VA, :] = jnp.ones((VA - 128, TB), BF16)
        return carry

    lax.fori_loop(0, NB, ones, 0)
    acc[...] = jnp.zeros(acc.shape, F32)
    m_ref[...] = jnp.full(m_ref.shape, NEG_LARGE, F32)
    start_rest(*v_ring)

    zero = jnp.zeros((QK, TQ), BF16)
    for qb in range(2):
        q_blk = own_pair if qb == 0 else 15 - own_pair
        same = (q_blk == sp) & (z // 2 == c)
        unless(same, lambda: remote(q_src.at[0], q_own.at[qb], q_send.at[0], q_recv.at[qb], z, x, 1 - c).wait_recv())
        unless(same, lambda: remote(lam_in.at[0], lam_own.at[qb], l_send.at[0], l_recv.at[qb], z, x, 1 - c).wait_recv())
        for t in range(NT):
            qt = q_own[qb, :, t * TQ : (t + 1) * TQ]
            qa[qb * NT + t, 0:QK, 0:TQ] = qt[0:QK]
            qa[qb * NT + t, QK:128, 0:TQ] = zero
            qa[qb * NT + t, 0:QK, TQ : 2 * TQ] = zero
            qa[qb * NT + t, QK:128, TQ : 2 * TQ] = qt[QK:128]

    scores = (s0, s1, s2)

    def unit(qb, j, diagonal):
        tops = [None] * NT

        def produce(t):
            rows = TQ * (t + 1) if diagonal else TB
            s = jnp.dot(k_all[j, 0:rows, :], qa[qb * NT + t], preferred_element_type=F32)
            if diagonal:
                key = lax.broadcasted_iota(jnp.int32, (rows, 2 * TQ), 0)
                query = lax.broadcasted_iota(jnp.int32, (rows, 2 * TQ), 1)
                query = jnp.where(query >= TQ, query - TQ, query) + t * TQ
                s = jnp.where(key <= query, s, NEG_LARGE)
            scores[t][0:rows, :] = s
            tops[t] = jnp.max(s, axis=0, keepdims=True)

        def consume(t):
            rows = TQ * (t + 1) if diagonal else TB
            at = qb * NT + t
            before = m_ref[at]
            after = jnp.maximum(before, tops[t])
            w = jnp.exp2(scores[t][0:rows, :] - after).astype(BF16)
            factor = jnp.exp2(before - after)
            acc[at] = acc[at] * factor + jnp.dot(
                v_all[j, :, 0:rows], w, preferred_element_type=F32
            )
            m_ref[at] = after

        for t in range(NT):
            produce(t)
        for t in range(NT):
            consume(t)

    def exchange(w):
        from_left, from_right = block_of(w, c), block_of(w, c + 2)
        arrived(from_left)

        @pl.when(w == 1)
        def _():
            pass_right(from_left, 2)

        pass_partner(from_left, 2 * w)
        arrived(from_right)

        @pl.when(w == 1)
        def _():
            pass_left(from_right, 2)

        pass_partner(from_right, 2 * w + 1)

    def out_same(q_blk):
        return (q_blk == sp) & (z // 2 == c)

    def out_copy(qb):
        return remote(
            o_stage.at[qb], act.at[4 + y * 4 + z], o_send.at[qb], o_recv.at[y * 4 + z],
            q_blks[qb] // 4, q_blks[qb] % 4, z // 2,
        )

    def finish(qb):
        hgain = jnp.broadcast_to(hgain_ref[...].astype(F32).reshape(1, 128), (8, 128)).T[:, 0:1]
        lam = lam_own[qb, 0:1, 0:1]
        for t in range(NT):
            at = qb * NT + t
            n1 = acc[at, 0:128, 0:TQ] / acc[at, 128:129, 0:TQ]
            n2 = acc[at, 0:128, TQ : 2 * TQ] / acc[at, 128:129, TQ : 2 * TQ]
            diff = n1 - lam * n2
            mean = jnp.mean(diff * diff, axis=0, keepdims=True)
            normed = diff * lax.rsqrt(mean + 1e-05) * hgain
            o_stage[qb, t * TQ : (t + 1) * TQ, :] = normed.T.astype(BF16)
        unless(out_same(q_blks[qb]), lambda: out_copy(qb).start())

        @pl.when(out_same(q_blks[qb]))
        def _():
            act[4 + y * 4 + z] = o_stage[qb]

    conv_sends = []
    for n in range(2):
        piece = act.at[2 * c + n]
        conv_sends.append(partner(piece, piece, c_send.at[n], c_recv.at[n]))

    def convolve():
        @pl.when(sp > 0)
        def _():
            halo_copy.wait_recv()
            inner = jnp.dot(halo[...], wp[3], preferred_element_type=F32).astype(BF16)
            outer = jnp.dot(halo[...], wp[4], preferred_element_type=F32).astype(BF16)
            gated[0:8, :] = inner[8:16].astype(F32) * outer[8:16].astype(F32)

        @pl.when(sp == 0)
        def _():
            gated[0:8, :] = jnp.zeros((8, 256), F32)

        taps = taps_ref[...].astype(F32)
        for m in range(NT):
            total = jnp.zeros((TQ, 256), F32)
            for tap in range(TAPS):
                first = 8 + m * TQ - (TAPS - 1) + tap
                total = total + taps[tap : tap + 1, :] * gated[first : first + TQ, :]
            conv = (u_b[m].astype(F32) * total).astype(BF16)
            act[2 * c, m * TQ : (m + 1) * TQ, :] = conv[:, 0:128]
            act[2 * c + 1, m * TQ : (m + 1) * TQ, :] = conv[:, 128:256]
        for one in conv_sends:
            one.start()

    convolve()

    up, down = ((y + 1) % 4) * 2 + c, ((y + 3) % 4) * 2 + c

    def ring(s, d):
        return copy_to(
            sbuf.at[s, d], rbuf.at[s, d], r_send.at[s, d], r_recv.at[s, d],
            sp, up if d == 0 else down,
        )

    def conv_ring(s):
        for d in range(2):
            chunk = (y + 3 - s) % 4 if d == 0 else (y + 1 + s) % 4
            first = d * HALF
            rows = jnp.concatenate([act[n, first : first + HALF, :] for n in range(4)], axis=1)
            part = jnp.dot(rows, wtc[chunk], preferred_element_type=F32)
            if s > 0:
                ring(s - 1, d).wait_recv()
                part = part + rbuf[s - 1, d].astype(F32)
            if s < 3:
                sbuf[s, d] = part.astype(BF16)
                ring(s, d).start()
            else:
                mixc[first : first + HALF, :] = part

    def step(i, carry):
        w, k = i // 4, i % 4
        plain = jnp.where(k < 2, c + 2 * k, 1 - c + 2 * (k - 2))
        last = jnp.where(k % 2 == 0, c, 1 - c) + 2 * (k // 2)
        u = jnp.where(w == 3, last, plain)
        blk = block_of(w, u)

        @pl.when(i == 4)
        def _():
            exchange(1)

        @pl.when((k == 3) & (0 < w) & (w < 3))
        def _():
            exchange(w + 1)

        @pl.when(u % 2 != c)
        def _():
            arrived(blk)

        @pl.when(i == 3)
        def _():
            for n in range(7):
                pair_out[4 + n].wait_recv()
                zcopies[n].start()

        for s, when in enumerate((1, 8, 14)):

            @pl.when(i == when)
            def _():
                if s == 0:
                    for one in own_out:
                        one.wait()
                    for one in pair_out[:4] + conv_sends:
                        one.wait_recv()
                conv_ring(s)

        @pl.when(i == NB - 2)
        def _():
            finish(0)

        def for_queries(qb, carry):
            q_blk = jnp.where(qb == 0, own_pair, 15 - own_pair)

            @pl.when(blk < q_blk)
            def _():
                unit(qb, blk, False)

            @pl.when(blk == q_blk)
            def _():
                unit(qb, blk, True)

            return carry

        lax.fori_loop(0, 2, for_queries, 0)
        return carry

    lax.fori_loop(0, NB, step, 0)

    finish(1)

    def piece(head):
        return act.at[4 + head]

    def o_arrived(head):
        partner(piece(head), piece(head), f_send.at[0], o_recv.at[head]).wait_recv()

    forwards = []

    def pass_on(head, target):
        one = copy_to(piece(head), piece(head), f_send.at[len(forwards)], o_recv.at[head], sp, target)
        one.start()
        forwards.append(one)

    beside = y * 2 + (1 - c)
    mine = [y * 4 + 2 * c + e for e in range(2)]
    below = [((y + 3) % 4) * 4 + 2 * c + e for e in range(2)]
    above = [((y + 1) % 4) * 4 + 2 * c + e for e in range(2)]
    across = [((y + 2) % 4) * 4 + 2 * c + e for e in range(2)]
    here = (sp == own_pair) | (sp == 15 - own_pair)
    unless((2 * c == z) & here, lambda: o_arrived(mine[0]))
    pass_on(mine[0], up)
    unless((2 * c + 1 == z) & here, lambda: o_arrived(mine[1]))
    pass_on(mine[1], down)
    pass_on(mine[1], up)
    pass_on(mine[0], down)
    pass_on(mine[0], beside)
    pass_on(mine[1], beside)

    for one in zcopies:
        one.wait_recv()

    def add_plane(n):
        plane = (y + n) % 4
        weights = wta[pl.ds(plane * 2, 2)].reshape(512, 512)
        for r in range(3):
            at = slice(r * TQ, (r + 1) * TQ)
            rows = jnp.concatenate([act[4 + plane * 4 + h, at, :] for h in range(4)], axis=1)
            part = jnp.dot(rows, weights, preferred_element_type=F32)
            if n == 0:
                total_mix[at, :] = part
            elif n != 2:
                total_mix[at, :] += part
            else:
                part = part + total_mix[at, :] + mixc[at, :]
                mix[at, :] = part.astype(BF16)

    def from_partner(n):
        for e in range(2):
            o_arrived(((y + n) % 4) * 4 + 2 * (1 - c) + e)

    from_partner(0)
    add_plane(0)
    o_arrived(below[0])
    pass_on(below[0], up)
    o_arrived(above[1])
    pass_on(above[1], down)
    pass_on(below[0], beside)
    pass_on(above[1], beside)
    conv_ring(3)
    for head in (below[1], above[0]):
        o_arrived(head)
        pass_on(head, beside)
    for n in (3, 1):
        from_partner(n)
        add_plane(n)
    for head in across:
        o_arrived(head)
        pass_on(head, beside)
    from_partner(2)
    add_plane(2)

    ones_row = jnp.ones((8, 512), BF16)
    dims = (((1,), (1,)), ((), ()))
    m = mix[...]
    square = m.astype(F32) * m.astype(F32)
    high = square.astype(BF16)
    low = (square - high.astype(F32)).astype(BF16)
    total = lax.dot_general(ones_row, m, dims, preferred_element_type=F32)
    squares = lax.dot_general(ones_row, high, dims, preferred_element_type=F32)
    squares = squares + lax.dot_general(ones_row, low, dims, preferred_element_type=F32)
    row = lax.broadcasted_iota(jnp.int32, (8, TB), 0)
    stats[tp] = jnp.where(row == 0, total, squares)

    def tell(i):
        return copy_to(stats.at[tp], stats.at[tp], t_send.at[i - 1], t_recv.at[i - 1], sp, (tp + i) % 8)

    for i in range(1, 8):
        tell(i).start()
    for i in range(1, 8):
        tell(i).wait_recv()
    everything = stats[0]
    for n in range(1, 8):
        everything = everything + stats[n]
    columns = everything.T
    ogain = ogain_ref[pl.ds(pl.multiple_of(tp * 512, 512), 512)].astype(F32).reshape(1, 512)
    mean = columns[:, 0:1] * (1.0 / D)
    variance = columns[:, 1:2] * (1.0 / D) - mean * mean
    out_ref[...] = (
        (mix[...].astype(F32) - mean) * lax.rsqrt(variance + 1e-05) * ogain
    ).astype(BF16)


    for e in range(2):
        unless(kv_same(e), lambda: key_first(e).wait_send())
        unless(kv_same(e), lambda: value_first(e).wait_send())
        unless(q_same(e), lambda: query_first(e).wait_send())
        unless(q_same(e), lambda: lam_first(e).wait_send())
        unless(out_same(q_blks[e]), lambda: out_copy(e).wait_send())

    @pl.when(sp < 15)
    def _():
        halo_copy.wait_send()

    for n in range(3):
        k_copy(0, rk_send, n, right, c).wait_send()
        v_copy(0, rv_send, n, right, c).wait_send()
        k_copy(0, lk_send, n, left, c).wait_send()
        v_copy(0, lv_send, n, left, c).wait_send()
    for n in range(8):
        k_copy(0, dk_send, n, x, 1 - c).wait_send()
        v_copy(0, dv_send, n, x, 1 - c).wait_send()
    for one in pair_out + zcopies + conv_sends + forwards:
        one.wait_send()
    for s in range(3):
        for d in range(2):
            ring(s, d).wait_send()
    for i in range(1, 8):
        tell(i).wait_send()


def mixer(*arrays):
    dma = pltpu.SemaphoreType.DMA
    hbm = pl.BlockSpec(memory_space=pl.ANY)
    vmem = pl.BlockSpec(memory_space=pltpu.VMEM)
    return pl.pallas_call(
        mixer_kernel,
        out_shape=jax.ShapeDtypeStruct((TB, 512), BF16),
        in_specs=[hbm] * 9 + [pl.BlockSpec(memory_space=pltpu.SMEM)] + [vmem] * 4,
        out_specs=vmem,
        scratch_shapes=[
            pltpu.VMEM((NT, TQ, D), BF16),
            pltpu.VMEM((6, D, 256), BF16),
            pltpu.VMEM((2, TB, 128), BF16),
            pltpu.VMEM((2, 128, TB), BF16),
            pltpu.VMEM((2, 128, TB), BF16),
            pltpu.VMEM((2, 8, 128), F32),
            pltpu.VMEM((TB + 8, 256), F32),
            pltpu.VMEM((16, D), BF16),
            pltpu.VMEM((NT, TQ, 256), BF16),
            pltpu.VMEM((NB, TB, 128), BF16),
            pltpu.VMEM((NB, VA, TB), BF16),
            pltpu.VMEM((2, 128, TB), BF16),
            pltpu.VMEM((2 * NT, 128, 2 * TQ), BF16),
            pltpu.VMEM((2, 8, 128), F32),
            pltpu.VMEM((TB, 2 * TQ), F32),
            pltpu.VMEM((TB, 2 * TQ), F32),
            pltpu.VMEM((TB, 2 * TQ), F32),
            pltpu.VMEM((2 * NT, VA, 2 * TQ), F32),
            pltpu.VMEM((2 * NT, 1, 2 * TQ), F32),
            pltpu.VMEM((2, TB, 128), BF16),
            pltpu.VMEM((20, TB, 128), BF16),
            pltpu.VMEM((4, 512, 512), BF16),
            pltpu.VMEM((8, 256, 512), BF16),
            pltpu.VMEM((3, 2, HALF, 512), BF16),
            pltpu.VMEM((3, 2, HALF, 512), BF16),
            pltpu.VMEM((TB, 512), F32),
            pltpu.VMEM((TB, 512), F32),
            pltpu.VMEM((TB, 512), BF16),
            pltpu.VMEM((8, 8, TB), F32),
            dma((NT,)), dma((6,)), dma((4,)), dma((4,)), dma((4,)), dma, dma((7,)), dma((7,)), dma((7,)), dma((7,)), dma, dma,
            dma((NB,)), dma((NB,)), dma((2,)), dma((2,)), dma((16,)),
            dma((2,)), dma((2,)), dma((2,)), dma((2,)),
            dma((3,)), dma((3,)), dma((3,)), dma((3,)),
            dma((8,)), dma((8,)), dma((2,)),
            dma((2,)), dma((2,)), dma((14,)),
            dma((3, 2)), dma((3, 2)), dma((7,)), dma((7,)),
        ],
        compiler_params=pltpu.CompilerParams(
            collective_id=0, has_side_effects=True, vmem_limit_bytes=67043328
        ),
        name="mixer",
    )(*arrays)


def per_device(
    hidden_states,
    w_conv_b,
    w_conv_c,
    w_conv_h,
    conv_taps,
    w_query,
    w_key,
    w_value,
    lambdas,
    head_gain,
    w_out_conv,
    w_out_attn,
    out_gain,
):
    first = lax.axis_index("sp") * TB
    positions = (first + jnp.arange(TB, dtype=jnp.int32)).astype(F32).reshape(NT, 1, TQ)
    inverse = 1.0 / 10000.0 ** (jnp.arange(0, QK, 2, dtype=F32) / QK)
    angles = positions * inverse[None, :, None]
    table = jnp.stack([jnp.cos(angles), jnp.sin(angles)])
    return mixer(
        hidden_states, w_key, w_value, w_query, w_conv_b, w_conv_c, w_conv_h,
        w_out_conv, w_out_attn,
        lambdas,
        head_gain,
        table,
        conv_taps,
        out_gain,
    )


def solution(mesh):
    return jax.shard_map(
        per_device,
        mesh=mesh,
        in_specs=(
            P("sp", None),
            P(None, "tp"),
            P(None, "tp"),
            P(None, "tp"),
            P(None, "tp"),
            P(None, "tp"),
            P(None, "tp"),
            P(None, "tp"),
            P("tp"),
            P(),
            P("tp", None),
            P("tp", None),
            P(),
        ),
        out_specs=P("sp", "tp"),
        check_vma=False,
    )
```
